32 devices in a mesh: sp: 8 (over z, x), tp: 4 (over y, core).
Axes of the slice: x: 2, y: 2, z: 4, core: 2. Of those that a mesh axis runs over, the one named last changes fastest.
Arguments:
- resid: bfloat16 [3072, 2048], P(('sp', 'tp')), may hold values from -6 to 6
- queries: bfloat16 [3072, 1024], P('sp', 'tp'), may hold values from -6 to 6
- keys: bfloat16 [3072, 1024], P('sp', 'tp'), may hold values from -6 to 6
- values: bfloat16 [3072, 1024], P('sp', 'tp'), may hold values from -6 to 6
- decay_input_part: bfloat16 [3072, 1024], P('sp', 'tp'), may hold values from -4 to 4
- decay_channel_offset: float32 [1024], P('tp'), may hold values from -16 to -2
- decay_head_extra: float32 [3072, 16], P('sp', 'tp'), may hold values from 0 to 0.7
- correction_rate_input: bfloat16 [3072, 1024], P('sp', 'tp'), may hold values from -6 to 6
- correction_rate_offset: float32 [1024], P('tp'), may hold values from -0.4 to 1
- head_norm_gain: float32 [1024], P('tp'), may hold values from 0.1 to 1.9
- mixer_output_weight: bfloat16 [1024, 2048], replicated, may hold values from -0.1875 to 0.1875
- feedforward_norm_gain: float32 [2048], replicated, may hold values from 0.1 to 1.9
- gate_weight: bfloat16 [2048, 5632], P('sp', 'tp'), may hold values from -0.125 to 0.125
- up_weight: bfloat16 [2048, 5632], P('sp', 'tp'), may hold values from -0.125 to 0.125
- down_weight: bfloat16 [5632, 2048], P('tp', 'sp'), may hold values from -0.078125 to 0.078125
Outputs:
- result: bfloat16 [3072, 2048], P(('sp', 'tp'))
The draws below stay inside these ranges and needn't reach their ends.
All inputs are finite; a program needn't handle non-finite values.
Results may differ from the reference program's by a relative error of at most 0.014.
Values may be sent and summed in bfloat16 or wider, within the bound.
A program may use at most 64 MiB of HBM per device.

```python
import math
import jax
import jax.numpy as jnp
from jax import lax

D = 2048
HEADS = 16
HEAD = 64
FF = 5632
TOK_DEV = 384
HW = 1024
TOKENS = 3072
N_SP = 8
N_TP = 4


def head_kinds(key, share):
    chosen = jax.random.uniform(jax.random.fold_in(key, 11), (HEADS,))
    return jnp.repeat(chosen < share, HEAD)


def draw_keys(key, part):
    flips = jax.random.bernoulli(jax.random.fold_in(key, 21), 0.5, (HEADS, HEAD))
    sizes = jax.random.uniform(jax.random.fold_in(key, 22), (HEADS, HEAD), jnp.float32, 0.5, 1.5)
    direction = jnp.where(flips, 1.0, -1.0) * sizes
    turns = jax.random.bernoulli(jax.random.fold_in(key, 23), 0.5, (TOKENS, HEADS))
    amounts = jax.random.uniform(jax.random.fold_in(key, 24), (TOKENS, HEADS), jnp.float32, 1.5, 3.0)
    amplitude = jnp.where(turns, 1.0, -1.0) * amounts
    spread = math.sqrt(6.0 * HEAD / TOKENS)
    noise = spread * jax.random.normal(jax.random.fold_in(key, 25), (TOKENS, HEADS, HEAD), jnp.float32)
    rows = amplitude[:, :, None] * direction[None] + noise
    return jnp.clip(rows, -6.0, 6.0).reshape(TOKENS, HEADS * HEAD).astype(jnp.bfloat16)


def draw_decay_channel_offset(key, part):
    share = 0.5
    slow = head_kinds(key, share)
    jitter = jax.random.uniform(jax.random.fold_in(key, 12), (HEADS * HEAD,), jnp.float32, -0.4, 0.4)
    quick = jax.random.uniform(jax.random.fold_in(key, 18), (HEADS * HEAD,), jnp.float32, -5.6, -2.4)
    return jnp.where(slow, math.log(0.3 / TOKENS) + 0.5 + jitter, quick)


def draw_correction_rate_offset(key, part):
    share = 0.5
    slow = head_kinds(key, share)
    jitter = jax.random.uniform(jax.random.fold_in(key, 13), (HEADS * HEAD,), jnp.float32, -0.4, 0.4)
    strong = jax.random.uniform(jax.random.fold_in(key, 19), (HEADS * HEAD,), jnp.float32, 0.2, 1.0)
    return jnp.where(slow, strong, jitter)


def draw_decay_head_extra(key, part):
    places = jax.random.randint(jax.random.fold_in(key, 14), (3, HEADS), 0, TOKENS)
    losses = jax.random.uniform(jax.random.fold_in(key, 15), (3, HEADS), jnp.float32, 0.22, 0.69)
    positions = jnp.arange(TOKENS, dtype=jnp.int32)[:, None, None]
    return jnp.sum(jnp.where(positions == places[None], losses[None], 0.0), axis=1)


def draw_decay_input_part(key, part):
    noise = 0.5 * jax.random.normal(jax.random.fold_in(key, 16), (TOKENS, HEADS * HEAD), jnp.float32)
    offset = jax.random.uniform(jax.random.fold_in(key, 17), (TOKENS // TOK_DEV, HEADS * HEAD), jnp.float32, -0.7, 0.7)
    return jnp.clip(noise + jnp.repeat(offset, TOK_DEV, axis=0), -4.0, 4.0).astype(jnp.bfloat16)


def steps_of(own_key, shape, split, low, top_value):
    factor_of = 1.0
    for dim, parts in split:
        draws = jax.random.uniform(jax.random.fold_in(jax.random.fold_in(own_key, 6), dim), (parts,), jnp.float32, low / len(split), top_value / len(split))
        factor_of = factor_of * jnp.repeat(jnp.exp(draws), shape[dim] // parts).reshape((-1,) + (1,) * (len(shape) - 1 - dim))
    return factor_of


def gaussian(rng, dims, deviation, reach, pieces=(), held_as=jnp.bfloat16):
    factor_of = steps_of(rng, dims, pieces, -0.22, 0.18) if pieces else 1.0
    array = jax.random.normal(rng, dims, jnp.float32) * deviation * factor_of
    return jnp.minimum(jnp.maximum(array, -reach), reach).astype(held_as)


def setup_inputs(seed: int = 0) -> dict:
    key_of = jax.random.split(jax.random.key(seed), 16)
    resid = gaussian(key_of[0], (TOKENS, D), 1.0, 6.0, ((0, 32),))
    queries = gaussian(key_of[1], (TOKENS, HW), 1.0, 6.0, ((0, 8), (1, 4)))
    keys = draw_keys(jax.random.fold_in(key_of[15], 71), 0)
    values = gaussian(key_of[3], (TOKENS, HW), 1.0, 6.0, ((0, 8), (1, 4)))
    decay_input_part = draw_decay_input_part(jax.random.fold_in(key_of[15], 71), 0)
    decay_channel_offset = draw_decay_channel_offset(jax.random.fold_in(key_of[15], 71), 0)
    decay_head_extra = draw_decay_head_extra(jax.random.fold_in(key_of[15], 71), 0)
    correction_rate_input = gaussian(key_of[7], (TOKENS, HW), 1.0, 6.0, ((0, 8), (1, 4)))
    correction_rate_offset = draw_correction_rate_offset(jax.random.fold_in(key_of[15], 71), 0)
    head_norm_gain = jnp.clip(1.0 + 0.18 * jax.random.normal(key_of[9], (HW,), jnp.float32), 0.1, 1.9)
    mixer_output_weight = gaussian(key_of[10], (HW, D), HW ** -0.5, 0.1875)
    feedforward_norm_gain = jnp.clip(1.0 + 0.18 * jax.random.normal(key_of[11], (D,), jnp.float32), 0.1, 1.9)
    gate_weight = gaussian(key_of[12], (D, FF), D ** -0.5, 0.125, ((0, 8), (1, 4)))
    up_weight = gaussian(key_of[13], (D, FF), D ** -0.5, 0.125, ((0, 8), (1, 4)))
    down_weight = gaussian(key_of[14], (FF, D), FF ** -0.5, 0.078125, ((0, 4), (1, 8)))
    return {"resid": resid, "queries": queries, "keys": keys, "values": values, "decay_input_part": decay_input_part, "decay_channel_offset": decay_channel_offset, "decay_head_extra": decay_head_extra, "correction_rate_input": correction_rate_input, "correction_rate_offset": correction_rate_offset, "head_norm_gain": head_norm_gain, "mixer_output_weight": mixer_output_weight, "feedforward_norm_gain": feedforward_norm_gain, "gate_weight": gate_weight, "up_weight": up_weight, "down_weight": down_weight}


def recurrence(carry_state, inputs):
    query_t, decay_t, key_t, value_t, unit_t, lrate_t = inputs
    lifted = jnp.einsum('hvk,hk->hv', carry_state, -unit_t, precision=lax.Precision.HIGHEST)
    carry_state = carry_state * decay_t[:, None, :] + lifted[:, :, None] * (unit_t * lrate_t)[:, None, :] + value_t[:, :, None] * key_t[:, None, :]
    return (carry_state, jnp.einsum('hvk,hk->hv', carry_state, query_t, precision=lax.Precision.HIGHEST))

def reference(resid, queries, keys, values, decay_input_part, decay_channel_offset, decay_head_extra, correction_rate_input, correction_rate_offset, head_norm_gain, mixer_output_weight, feedforward_norm_gain, gate_weight, up_weight, down_weight):

    def head_count(arr):
        return arr.astype(jnp.float32).reshape(TOKENS, HEADS, HEAD)
    correction_rate = jnp.exp(-jax.nn.softplus(-(decay_channel_offset + decay_input_part.astype(jnp.float32))) - 0.5)
    decay_factor = jnp.exp(-head_count(correction_rate) - decay_head_extra[:, :, None])
    key_f = head_count(keys)
    unit_keys = key_f * lax.rsqrt(lax.optimization_barrier(jnp.sum(key_f * key_f, axis=-1, keepdims=True)) + 1e-06)
    lrate = head_count(jax.nn.sigmoid(correction_rate_offset + correction_rate_input.astype(jnp.float32)))
    start = jnp.zeros((HEADS, HEAD, HEAD), jnp.float32)
    _, mixer_out = lax.scan(recurrence, start, (head_count(queries), decay_factor, key_f, head_count(values), unit_keys, lrate))
    center = mixer_out - lax.optimization_barrier(jnp.mean(mixer_out, axis=-1, keepdims=True))
    spread = lax.optimization_barrier(jnp.mean(center * center, axis=-1, keepdims=True))
    mixed = (center * lax.rsqrt(spread + 1e-05) * head_norm_gain.reshape(HEADS, HEAD)).reshape(TOKENS, HW).astype(jnp.bfloat16)

    def layer_block(pair):
        mixed_rows, resid_rows = pair
        proj = jnp.dot(mixed_rows, mixer_output_weight, preferred_element_type=jnp.float32)
        resid_mid = (resid_rows.astype(jnp.float32) + proj).astype(jnp.bfloat16)
        mid_f = resid_mid.astype(jnp.float32)
        normed = (mid_f * lax.rsqrt(lax.optimization_barrier(jnp.mean(mid_f * mid_f, axis=-1, keepdims=True)) + 1e-06) * feedforward_norm_gain).astype(jnp.bfloat16)
        gate = jnp.dot(normed, gate_weight, preferred_element_type=jnp.float32)
        upper = jnp.dot(normed, up_weight, preferred_element_type=jnp.float32)
        hidden = (jax.nn.silu(gate) * upper).astype(jnp.bfloat16)
        hid_parts = hidden.reshape(TOK_DEV, N_TP, FF // N_TP).astype(jnp.float32)
        down_parts = down_weight.reshape(N_TP, FF // N_TP, D).astype(jnp.float32)
        partial_value = jnp.einsum('tnf,nfd->ntd', hid_parts, down_parts).astype(jnp.bfloat16)
        partial_value = lax.optimization_barrier(partial_value).astype(jnp.float32)
        down_sum = lax.optimization_barrier(jnp.sum(partial_value, axis=0))
        return (mid_f + 0.5 * down_sum).astype(jnp.bfloat16)
    result = lax.map(layer_block, (mixed.reshape(N_SP, TOK_DEV, HW), resid.reshape(N_SP, TOK_DEV, D)))
    return result.reshape(TOKENS, D)
```

```python
import functools
import math

import jax
import jax.numpy as jnp
from jax import lax
from jax.experimental import pallas as pl
from jax.experimental.pallas import tpu as pltpu
from jax.sharding import Mesh, PartitionSpec as P

HEAD = 64
F32 = jnp.float32
BF16 = jnp.bfloat16


def split2(a):
    high = a.astype(BF16)
    return high, (a - high.astype(F32)).astype(BF16)


def dot3(a, b, dims):
    (ah, al), (bh, bl) = a, b
    dn = (dims, ((), ()))
    d = functools.partial(lax.dot_general, dimension_numbers=dn, preferred_element_type=F32)
    return d(ah, bh) + (d(ah, bl) + d(al, bh))


NN = ((1,), (0,))
NT = ((1,), (1,))
TN = ((0,), (0,))


def chunk_kernel(heads, chunk, q_ref, k_ref, v_ref, din_ref, doff_ref, extra_ref, rin_ref, roff_ref, reads_ref, total_ref, z_ref):
    rows = q_ref.shape[0]
    width = heads * HEAD
    wide = heads * chunk
    step = pl.program_id(0)

    @pl.when(step == 0)
    def _():
        r = lax.broadcasted_iota(jnp.int32, (width, 2 * HEAD), 0) % HEAD
        c = lax.broadcasted_iota(jnp.int32, (width, 2 * HEAD), 1)
        z_ref[...] = jnp.where(r == c, 1.0, 0.0).astype(F32)

    def load(ref):
        return ref[...].astype(F32)

    def stack(a):
        return jnp.concatenate([a[:, h * HEAD:(h + 1) * HEAD] for h in range(heads)], axis=0)

    spread_r = lax.broadcasted_iota(jnp.int32, (heads, width), 0)
    spread_c = lax.broadcasted_iota(jnp.int32, (heads, width), 1) // HEAD
    spread = jnp.where(spread_r == spread_c, 1.0, 0.0).astype(F32)
    extra = lax.dot_general(extra_ref[...], spread, ((((1,), (0,))), ((), ())), precision=lax.Precision.HIGHEST, preferred_element_type=F32)
    log_decay = -jax.nn.sigmoid(load(din_ref) + doff_ref[...]) * math.exp(-0.5) - extra
    tr = lax.broadcasted_iota(jnp.int32, (chunk, chunk), 0)
    tc = lax.broadcasted_iota(jnp.int32, (chunk, chunk), 1)
    lower = jnp.where(tr >= tc, 1.0, 0.0).astype(F32)
    cum = lax.dot_general(lower, log_decay, (((1,), (0,)), ((), ())), precision=lax.Precision.HIGHEST, preferred_element_type=F32)
    last = cum[chunk - 1:chunk, :]
    mid = cum[chunk // 2 - 1:chunk // 2, :]
    before = cum - log_decay
    rate = jax.nn.sigmoid(load(rin_ref) + roff_ref[...])

    key = stack(load(k_ref))
    unit = key * lax.rsqrt(jnp.sum(key * key, axis=-1, keepdims=True) + 1e-6)
    base = unit * stack(rate)
    query = stack(load(q_ref))
    value = split2(stack(load(v_ref)))
    to_mid = stack(jnp.exp(mid - cum))
    key_mid = split2(key * to_mid)
    base_mid = split2(base * to_mid)
    query_mid = split2(query * stack(jnp.exp(cum - mid)))
    unit_mid = split2(unit * stack(jnp.exp(before - mid)))
    to_last = stack(jnp.exp(last - cum))

    row = lax.broadcasted_iota(jnp.int32, (wide, wide), 0)
    col = lax.broadcasted_iota(jnp.int32, (wide, wide), 1)
    same = (row // chunk) == (col // chunk)
    strict = same & (row > col)
    upto = same & (row >= col)
    a_ub = jnp.where(strict, dot3(unit_mid, base_mid, NT), 0.0)
    a_uk = jnp.where(strict, dot3(unit_mid, key_mid, NT), 0.0)
    a_qb = jnp.where(upto, dot3(query_mid, base_mid, NT), 0.0)
    a_qk = jnp.where(upto, dot3(query_mid, key_mid, NT), 0.0)

    inverse = jnp.where(row == col, 1.0, 0.0).astype(F32)
    size = 1
    while size < chunk:
        pair = ((row // (2 * size)) == (col // (2 * size))) & ((row // size) > (col // size))
        part = jnp.where(pair, a_ub, 0.0)
        if size == 1:
            inverse = inverse - part
        else:
            inv = split2(inverse)
            inverse = inverse - dot3(split2(dot3(inv, split2(part), NN)), inv, NN)
        size *= 2
    inverse = split2(inverse)

    wr = lax.broadcasted_iota(jnp.int32, (wide, width), 0) // chunk
    wc = lax.broadcasted_iota(jnp.int32, (wide, width), 1) // HEAD

    def spread_wide(a):
        return jnp.where(wr == wc, jnp.concatenate([a] * heads, axis=1), 0.0)

    unit_wide = split2(spread_wide(unit * stack(jnp.exp(before))))
    query_wide = spread_wide(query * stack(jnp.exp(cum)))
    base_wide = split2(spread_wide(base * to_last))
    key_wide = split2(spread_wide(key * to_last))
    qb = split2(a_qb)
    trans = split2(dot3(inverse, unit_wide, NN))
    own = split2(dot3(inverse, split2(dot3(split2(a_uk), value, NN)), NN))
    read = split2(query_wide - dot3(qb, trans, NN))
    out_own = dot3(split2(a_qk), value, NN) - dot3(qb, own, NN)
    pr = lax.broadcasted_iota(jnp.int32, (width, width), 0)
    pc = lax.broadcasted_iota(jnp.int32, (width, width), 1)
    move = jnp.where(pr == pc, jnp.exp(last), 0.0) - dot3(base_wide, trans, TN)
    end = dot3(key_wide, value, TN) - dot3(base_wide, own, TN)

    z = split2(z_ref[...])
    x = dot3(read, z, NN) + jnp.concatenate([jnp.zeros_like(out_own), out_own], axis=1)
    for h in range(heads):
        reads_ref[h] = x[h * chunk:(h + 1) * chunk, :]
    z_new = dot3(split2(move), z, NN) + jnp.concatenate([jnp.zeros_like(end), end], axis=1)
    z_ref[...] = z_new
    total_ref[...] = z_new.astype(BF16)


def chunks(q, k, v, din, doff, extra, rin, roff):
    rows, width = q.shape
    heads = width // HEAD
    chunk = 64
    while rows % chunk:
        chunk //= 2
    tile = pl.BlockSpec((chunk, width), lambda i: (i, 0))
    vec = pl.BlockSpec((1, width), lambda i: (0, 0))
    n = rows // chunk
    return pl.pallas_call(
        functools.partial(chunk_kernel, heads, chunk),
        grid=(n,),
        in_specs=[tile, tile, tile, tile, vec, pl.BlockSpec((chunk, heads), lambda i: (i, 0)), tile, vec],
        out_specs=(
            pl.BlockSpec((heads, chunk, 2 * HEAD), lambda i: (0, i, 0)),
            pl.BlockSpec((width, 2 * HEAD), lambda i: (0, 0)),
        ),
        out_shape=(
            jax.ShapeDtypeStruct((heads, rows, 2 * HEAD), F32),
            jax.ShapeDtypeStruct((width, 2 * HEAD), BF16),
        ),
        scratch_shapes=[pltpu.VMEM((width, 2 * HEAD), F32)],
        compiler_params=pltpu.CompilerParams(dimension_semantics=("arbitrary",), vmem_limit_bytes=40 * 2**20),
    )(q, k, v, din, doff.reshape(1, width), extra, rin, roff.reshape(1, width))


def carry_kernel(nz, nx, total_ref, reads_ref, gain_ref, mixed_ref, held, send_sem, recv_sem):
    n = nz * nx
    me = lax.axis_index("z") * nx + lax.axis_index("x")
    heads = reads_ref.shape[0]

    def place(k):
        peer = lax.rem(me + k, n)
        return {"z": peer // nx, "x": lax.rem(peer, nx)}

    barrier = pltpu.get_barrier_semaphore()
    for k in range(1, n):
        pl.semaphore_signal(barrier, inc=1, device_id=place(k), device_id_type=pl.DeviceIdType.MESH)
    pl.semaphore_wait(barrier, n - 1)
    copies = []
    for k in range(1, n):
        c = pltpu.make_async_remote_copy(
            src_ref=total_ref, dst_ref=held.at[k], send_sem=send_sem.at[k], recv_sem=recv_sem.at[k],
            device_id=place(k), device_id_type=pl.DeviceIdType.MESH)
        c.start()
        copies.append(c)
    for c in copies:
        c.wait()
    state = [jnp.zeros((HEAD, HEAD), F32) for _ in range(heads)]
    for k in range(n - 1, 0, -1):
        there = k <= me
        for h in range(heads):
            block = held[k, h * HEAD:(h + 1) * HEAD, :].astype(F32)
            new = block[:, HEAD:] + jnp.dot(block[:, :HEAD], state[h], precision=lax.Precision.HIGHEST, preferred_element_type=F32)
            state[h] = jnp.where(there, new, state[h])
    outs = []
    for h in range(heads):
        x = reads_ref[h]
        o = x[:, HEAD:] + dot3(split2(x[:, :HEAD]), split2(state[h]), NN)
        center = o - jnp.mean(o, axis=-1, keepdims=True)
        var = jnp.mean(center * center, axis=-1, keepdims=True)
        outs.append(center * lax.rsqrt(var + 1e-5))
    mixed_ref[...] = (jnp.concatenate(outs, axis=1) * gain_ref[...]).astype(BF16)


def carry(total, reads, gain, nz, nx):
    heads, rows, _ = reads.shape
    width = heads * HEAD
    n = nz * nx
    vm = pl.BlockSpec(memory_space=pltpu.VMEM)
    return pl.pallas_call(
        functools.partial(carry_kernel, nz, nx),
        in_specs=[vm, vm, vm],
        out_specs=vm,
        out_shape=jax.ShapeDtypeStruct((rows, width), BF16),
        scratch_shapes=[
            pltpu.VMEM((n, width, 2 * HEAD), BF16),
            pltpu.SemaphoreType.DMA((n,)),
            pltpu.SemaphoreType.DMA((n,)),
        ],
        compiler_params=pltpu.CompilerParams(collective_id=1, has_side_effects=True, vmem_limit_bytes=24 * 2**20),
    )(total, reads, gain.reshape(1, width))


def send_z(block, nz):
    return [lax.ppermute(block, "z", [(s, (s + k) % nz) for s in range(nz)]) for k in range(1, nz)]


def in_order(block, came, nz, axis):
    z = lax.axis_index("z")
    size = block.shape[axis]
    shape = list(block.shape)
    shape[axis] = size * nz
    whole = jnp.zeros(shape, block.dtype)
    whole = lax.dynamic_update_slice_in_dim(whole, block, z * size, axis)
    for k in range(1, nz):
        whole = lax.dynamic_update_slice_in_dim(whole, came[k - 1], lax.rem(z - k + nz, nz) * size, axis)
    return whole


def per_device(
    nz, nx,
    resid, queries, keys, values, decay_input_part, decay_channel_offset, decay_head_extra,
    correction_rate_input, correction_rate_offset, head_norm_gain, mixer_output_weight,
    feedforward_norm_gain, gate_weight, up_weight, down_weight,
):
    ff = gate_weight.shape[1] // nx
    x = lax.axis_index("x")

    def exchange(weight, axis, join):
        pieces = weight.reshape(weight.shape[:axis] + (nx, ff) + weight.shape[axis + 1:])
        return lax.all_to_all(pieces, "x", split_axis=axis, concat_axis=join, tiled=False)

    def swap(weight, axis, join):
        if nx == 1:
            return weight
        if nx != 2:
            out = exchange(weight, axis, join)
            return out.reshape((-1, ff) if axis == 1 else (ff, -1))
        mine = lax.dynamic_slice_in_dim(weight, x * ff, ff, axis)
        other = lax.dynamic_slice_in_dim(weight, (1 - x) * ff, ff, axis)
        came = lax.ppermute(other, "x", [(0, 1), (1, 0)])
        first = jnp.where(x == 0, mine, came)
        second = jnp.where(x == 0, came, mine)
        return jnp.concatenate([first, second], axis=join)

    halves = (swap(gate_weight, 1, 0), swap(up_weight, 1, 0), swap(down_weight, 0, 1))
    halves, queries = lax.optimization_barrier((halves, queries))
    whole_gate = lax.all_gather(halves[0], "z", axis=0, tiled=True)
    up_came = send_z(halves[1], nz)
    down_came = send_z(halves[2], nz)

    reads, total = chunks(
        queries, keys, values, decay_input_part, decay_channel_offset, decay_head_extra,
        correction_rate_input, correction_rate_offset)
    total, up_came = lax.optimization_barrier((total, up_came))
    mixed = carry(total, reads, head_norm_gain, nz, nx)
    row_mixed = lax.all_to_all(mixed, "tp", split_axis=0, concat_axis=1, tiled=True)
    proj = jnp.dot(row_mixed, mixer_output_weight, preferred_element_type=F32)
    mid_f = (resid.astype(F32) + proj).astype(BF16).astype(F32)
    normed = (
        mid_f
        * lax.rsqrt(jnp.mean(mid_f * mid_f, axis=-1, keepdims=True) + 1e-06)
        * feedforward_norm_gain
    ).astype(BF16)
    normed, whole_gate = lax.optimization_barrier((normed, whole_gate))
    whole_up = in_order(halves[1], up_came, nz, 0)
    whole_down = in_order(halves[2], down_came, nz, 1)
    whole_rows = lax.all_gather(normed, ("x", "tp"), axis=0, tiled=True)
    gate = jnp.dot(whole_rows, whole_gate, preferred_element_type=F32)
    upper = jnp.dot(whole_rows, whole_up, preferred_element_type=F32)
    hidden = (jax.nn.silu(gate) * upper).astype(BF16)
    down_sum = lax.psum_scatter(
        jnp.dot(hidden, whole_down, preferred_element_type=F32).astype(BF16),
        ("x", "tp"), scatter_dimension=0, tiled=True,
    ).astype(F32)
    return (mid_f + 0.5 * down_sum).astype(BF16)


MESH = pl.DeviceIdType.MESH


def layer_kernel(
    total_ref, reads_ref, gain_ref, resid_ref, fgain_ref, wo_hbm, gate_hbm, up_hbm, down_hbm, out_ref,
    held, mixed, mixrow, wo, mid, tok, gate, up, down, hidden, near_sum, far_sum, y_out, y_in, z_out, z_in,
    wo_sem, w_send, w_recv, c_send, c_recv, a_send, a_recv, t_send, t_recv, y_send, y_recv, z_send, z_recv,
):
    z, x, y, c = (lax.axis_index(name) for name in ("z", "x", "y", "c"))
    half, low = z // 2, lax.rem(z, 2)
    sib = z + 1 - 2 * low
    pair = lax.rem(z + 2, 4)
    near = 1 + half
    mine = c == half
    me = 2 * z + x
    n = 8
    depth = gate_hbm.shape[0]
    heads = reads_ref.shape[0]
    width = heads * HEAD
    rows = resid_ref.shape[0]
    model = resid_ref.shape[1]
    sources = (gate_hbm, up_hbm, down_hbm)

    def at(index, size):
        return pl.ds(pl.multiple_of(index * size, size), size)

    def remote(src, dst, send, recv, **where):
        return pltpu.make_async_remote_copy(
            src_ref=src, dst_ref=dst, send_sem=send, recv_sem=recv, device_id=where, device_id_type=MESH)

    def piece(m, s):
        return down.at[:, at(s, depth)] if m == 2 else (gate, up)[m].at[at(s, depth), :]

    def to(src, m, s, slot, **where):
        return remote(src, piece(m, s), w_send.at[m, slot], w_recv.at[m, s], **where)

    def landed(m, s):
        to(piece(m, s), m, s, 0, c=1 - c).wait_recv()

    def own(m):
        return pltpu.make_async_copy(sources[m], piece(m, me), w_recv.at[m, me])

    def first_sends(m):
        src = sources[m]
        return (
            (mine, (to(src, m, me, 0, z=sib, c=1 - half), to(src, m, me, 1, x=1 - x), to(src, m, me, 2, c=1 - c))),
            (jnp.logical_not(mine), (to(src, m, me, 3, z=1 + c, c=low),)),
        )

    first = jnp.where(mine, z, sib)
    second = 2 * (1 - half) + c
    other_first = jnp.where(mine, sib, z)
    other_second = 2 * (1 - half) + 1 - c

    def relay(m, step):
        s = 2 * (first, second, first, second)[step] + (x, x, 1 - x, 1 - x)[step]
        p = piece(m, s)
        if step == 0:
            return s, ((jnp.logical_not(mine), (to(p, m, s, 4, x=1 - x), to(p, m, s, 5, c=1 - c))),)
        if step == 1:
            return s, (
                (z == near, (to(p, m, s, 6, z=3 * half),)),
                (None, (to(p, m, s, 7, x=1 - x), to(p, m, s, 8, c=1 - c))),
            )
        return s, ((None, (to(p, m, s, 7 + step, c=1 - c),)),)

    def each(groups, act):
        for when, copies in groups:
            if when is None:
                for copy in copies:
                    act(copy)
            else:
                @pl.when(when)
                def _():
                    for copy in copies:
                        act(copy)

    def start(copy):
        copy.start()

    def begin(m):
        @pl.when(mine)
        def _():
            own(m).start()
        each(first_sends(m), start)

    def pump(m, step):
        s, groups = relay(m, step)
        landed(m, s)
        each(groups, start)

    def gather_rest(m):
        for plane in (other_first, other_second):
            for column in (x, 1 - x):
                landed(m, 2 * plane + column)

    def drain(m):
        for groups in (first_sends(m), *(relay(m, step)[1] for step in range(4))):
            each(groups, lambda copy: copy.wait_send())

    barrier = pltpu.get_barrier_semaphore()
    for dz in range(4):
        for dx in range(2):
            for dy in range(2):
                for dc in range(2):
                    if dz or dx or dy or dc:
                        peer = {"z": lax.rem(z + dz, 4), "x": lax.rem(x + dx, 2), "y": lax.rem(y + dy, 2), "c": lax.rem(c + dc, 2)}
                        pl.semaphore_signal(barrier, inc=1, device_id=peer, device_id_type=MESH)
    pl.semaphore_wait(barrier, 31)

    load_wo = pltpu.make_async_copy(wo_hbm, wo, wo_sem)
    load_wo.start()

    def place(k):
        peer = lax.rem(me + k, n)
        return {"z": peer // 2, "x": lax.rem(peer, 2)}

    def carry_copy(k):
        return remote(total_ref, held.at[k], c_send.at[k], c_recv.at[k], **place(k))

    for k in range(1, n):
        @pl.when(me + k < n)
        def _():
            carry_copy(k).start()
    for m in range(3):
        begin(m)
    for k in range(1, n):
        @pl.when(me >= k)
        def _():
            carry_copy(k).wait_recv()
    state = [jnp.zeros((HEAD, HEAD), F32) for _ in range(heads)]
    for k in range(n - 1, 0, -1):
        there = k <= me
        for h in range(heads):
            block = held[k, h * HEAD:(h + 1) * HEAD, :].astype(F32)
            new = block[:, HEAD:] + jnp.dot(block[:, :HEAD], state[h], precision=lax.Precision.HIGHEST, preferred_element_type=F32)
            state[h] = jnp.where(there, new, state[h])
    outs = []
    for h in range(heads):
        r = reads_ref[h]
        o = r[:, HEAD:] + dot3(split2(r[:, :HEAD]), split2(state[h]), NN)
        center = o - jnp.mean(o, axis=-1, keepdims=True)
        var = jnp.mean(center * center, axis=-1, keepdims=True)
        outs.append(center * lax.rsqrt(var + 1e-5))
    mixed[...] = (jnp.concatenate(outs, axis=1) * gain_ref[...]).astype(BF16)

    t = 2 * y + c

    def exchange(dy, dc):
        ty, tc = lax.rem(y + dy, 2), lax.rem(c + dc, 2)
        slot = 2 * dy + dc
        return remote(
            mixed.at[at(2 * ty + tc, rows), :], mixrow.at[:, at(t, width)], a_send.at[slot], a_recv.at[slot], y=ty, c=tc)

    swaps = [exchange(1, 0), exchange(1, 1), exchange(0, 1)]
    for copy in swaps:
        copy.start()
    mixrow[:, at(t, width)] = mixed[at(t, rows), :]
    pump(0, 0)
    load_wo.wait()
    for copy in swaps:
        copy.wait()

    tile = 512
    square = jnp.zeros((rows, 1), F32)
    for j in range(0, model, tile):
        proj = jnp.dot(mixrow[...], wo[:, j:j + tile], preferred_element_type=F32)
        part = (resid_ref[:, j:j + tile].astype(F32) + proj).astype(BF16).astype(F32)
        mid[:, j:j + tile] = part
        square += jnp.sum(part * part, axis=-1, keepdims=True)
    g = 2 * half + y
    g_far = 2 * (1 - half) + y
    g_side = 2 * half + 1 - y
    g_diag = 2 * (1 - half) + 1 - y
    tok[at(g, rows), :] = (mid[...] * lax.rsqrt(square / model + 1e-06) * fgain_ref[...]).astype(BF16)

    def rows_to(block, slot, **where):
        r = tok.at[at(block, rows), :]
        return remote(r, r, t_send.at[slot], t_recv.at[slot], **where)

    def rows_from(block, slot):
        r = tok.at[at(block, rows), :]
        remote(r, r, t_send.at[slot], t_recv.at[slot], y=1 - y).wait_recv()

    ahead = rows_to(g, 0, z=pair)
    beside = rows_to(g, 1, y=1 - y)
    onward = rows_to(g_far, 2, y=1 - y)
    ahead.start()
    beside.start()
    for step in range(1, 4):
        pump(0, step)
    pump(1, 0)
    rows_from(g_far, 0)
    onward.start()
    for step in range(1, 4):
        pump(1, step)
    for step in range(4):
        pump(2, step)
    for m in range(3):
        gather_rest(m)
    rows_from(g_side, 1)
    rows_from(g_diag, 2)

    units = gate.shape[1]
    for j in range(0, units, 256):
        cols = slice(j, min(j + 256, units))
        gated = jnp.dot(tok[...], gate[:, cols], preferred_element_type=F32)
        upper = jnp.dot(tok[...], up[:, cols], preferred_element_type=F32)
        hidden[:, cols] = (gated * jax.nn.sigmoid(gated) * upper).astype(BF16)

    def side_copy(i):
        return remote(y_out.at[i], y_in.at[i], y_send.at[i], y_recv.at[i], y=1 - y)

    def far_copy(i):
        return remote(z_out.at[i], z_in.at[i], z_send.at[i], z_recv.at[i], z=pair)

    for i in range(n):
        cols = slice(i * depth, (i + 1) * depth)
        for place_of, dst in ((g_diag, y_out.at[i, 0]), (g_side, y_out.at[i, 1])):
            dst[...] = jnp.dot(hidden[at(place_of, rows), :], down[:, cols], preferred_element_type=F32).astype(BF16)
        far_sum[:, cols] = jnp.dot(hidden[at(g_far, rows), :], down[:, cols], preferred_element_type=F32)
        side_copy(i).start()
        near_sum[:, cols] = jnp.dot(hidden[at(g, rows), :], down[:, cols], preferred_element_type=F32)
    for i in range(n):
        cols = slice(i * depth, (i + 1) * depth)
        side_copy(i).wait_recv()
        z_out[i] = (far_sum[:, cols] + y_in[i, 0].astype(F32)).astype(BF16)
        far_copy(i).start()
    for i in range(n):
        cols = slice(i * depth, (i + 1) * depth)
        far_copy(i).wait_recv()
        total = near_sum[:, cols] + y_in[i, 1].astype(F32) + z_in[i].astype(F32)
        out_ref[:, cols] = (mid[:, cols] + 0.5 * total).astype(BF16)

    for k in range(1, n):
        @pl.when(me + k < n)
        def _():
            carry_copy(k).wait_send()
    for m in range(3):
        drain(m)
    for copy in (ahead, beside, onward):
        copy.wait_send()
    for i in range(n):
        side_copy(i).wait_send()
        far_copy(i).wait_send()


def layer(total, reads, gain, resid, fgain, wo, gate, up, down):
    heads, tokens, _ = reads.shape
    width = heads * HEAD
    rows, model = resid.shape
    depth, units = gate.shape
    n = 8
    vm = pl.BlockSpec(memory_space=pltpu.VMEM)
    hbm = pl.BlockSpec(memory_space=pl.ANY)
    dma = pltpu.SemaphoreType.DMA
    return pl.pallas_call(
        layer_kernel,
        in_specs=[vm, vm, vm, vm, vm, hbm, hbm, hbm, hbm],
        out_specs=vm,
        out_shape=jax.ShapeDtypeStruct((rows, model), BF16),
        scratch_shapes=[
            pltpu.VMEM((n, width, 2 * HEAD), BF16),
            pltpu.VMEM((tokens, width), BF16),
            pltpu.VMEM((rows, wo.shape[0]), BF16),
            pltpu.VMEM(wo.shape, BF16),
            pltpu.VMEM((rows, model), F32),
            pltpu.VMEM((4 * rows, model), BF16),
            pltpu.VMEM((n * depth, units), BF16),
            pltpu.VMEM((n * depth, units), BF16),
            pltpu.VMEM((units, n * depth), BF16),
            pltpu.VMEM((4 * rows, units), BF16),
            pltpu.VMEM((rows, model), F32),
            pltpu.VMEM((rows, model), F32),
            pltpu.VMEM((n, 2, rows, depth), BF16),
            pltpu.VMEM((n, 2, rows, depth), BF16),
            pltpu.VMEM((n, rows, depth), BF16),
            pltpu.VMEM((n, rows, depth), BF16),
            dma, dma((3, 11)), dma((3, n)), dma((n,)), dma((n,)), dma((4,)), dma((4,)), dma((3,)), dma((3,)),
            dma((n,)), dma((n,)), dma((n,)), dma((n,)),
        ],
        compiler_params=pltpu.CompilerParams(collective_id=2, has_side_effects=True, vmem_limit_bytes=56 * 2**20),
    )(total, reads, gain.reshape(1, width), resid, fgain.reshape(1, model), wo, gate, up, down)


def per_device_pairs(
    resid, queries, keys, values, decay_input_part, decay_channel_offset, decay_head_extra,
    correction_rate_input, correction_rate_offset, head_norm_gain, mixer_output_weight,
    feedforward_norm_gain, gate_weight, up_weight, down_weight,
):
    reads, total = chunks(
        queries, keys, values, decay_input_part, decay_channel_offset, decay_head_extra,
        correction_rate_input, correction_rate_offset)
    return layer(total, reads, head_norm_gain, resid, feedforward_norm_gain, mixer_output_weight, gate_weight, up_weight, down_weight)


def solution(mesh):
    n_sp, n_tp = mesh.shape["sp"], mesh.shape["tp"]
    if (n_sp, n_tp) == (8, 4):
        inner = Mesh(mesh.devices.reshape(4, 2, 2, 2), ("z", "x", "y", "c"))
        sp, tp = ("z", "x"), ("y", "c")
        body = per_device_pairs
    else:
        nx = 2 if n_sp % 2 == 0 else 1
        nz = n_sp // nx
        inner = Mesh(mesh.devices.reshape(nz, nx, n_tp), ("z", "x", "tp"))
        sp, tp = ("z", "x"), ("tp",)
        body = functools.partial(per_device, nz, nx)
    rows = P((*sp, *tp), None)
    placed = (
        rows, P(sp, tp), P(sp, tp), P(sp, tp), P(sp, tp), P(tp), P(sp, tp), P(sp, tp), P(tp), P(tp), P(), P(),
        P(sp, tp), P(sp, tp), P(tp, sp),
    )
    return jax.shard_map(body, mesh=inner, in_specs=placed, out_specs=rows, check_vma=False)
```

```python
import functools
import math

import jax
import jax.numpy as jnp
from jax import lax
from jax.experimental import pallas as pl
from jax.experimental.pallas import tpu as pltpu
from jax.sharding import Mesh, PartitionSpec as P

HEAD = 64
F32 = jnp.float32
BF16 = jnp.bfloat16


def split2(a):
    high = a.astype(BF16)
    return high, (a - high.astype(F32)).astype(BF16)


def dot3(a, b, dims):
    (ah, al), (bh, bl) = a, b
    dn = (dims, ((), ()))
    d = functools.partial(lax.dot_general, dimension_numbers=dn, preferred_element_type=F32)
    return d(ah, bh) + (d(ah, bl) + d(al, bh))


NN = ((1,), (0,))
NT = ((1,), (1,))
TN = ((0,), (0,))


def chunk_kernel(heads, chunk, *refs):
    chunk_step(heads, chunk, pl.program_id(0), *refs)


def chunk_step(heads, chunk, step, q_ref, k_ref, v_ref, din_ref, doff_ref, extra_ref, rin_ref, roff_ref, reads_ref, total_ref, z_ref):
    rows = q_ref.shape[0]
    width = heads * HEAD
    wide = heads * chunk

    @pl.when(step == 0)
    def _():
        r = lax.broadcasted_iota(jnp.int32, (width, 2 * HEAD), 0) % HEAD
        c = lax.broadcasted_iota(jnp.int32, (width, 2 * HEAD), 1)
        z_ref[...] = jnp.where(r == c, 1.0, 0.0).astype(F32)

    def load(ref):
        return ref[...].astype(F32)

    def stack(a):
        return jnp.concatenate([a[:, h * HEAD:(h + 1) * HEAD] for h in range(heads)], axis=0)

    spread_r = lax.broadcasted_iota(jnp.int32, (heads, width), 0)
    spread_c = lax.broadcasted_iota(jnp.int32, (heads, width), 1) // HEAD
    spread = jnp.where(spread_r == spread_c, 1.0, 0.0).astype(F32)
    extra = lax.dot_general(extra_ref[...], spread, ((((1,), (0,))), ((), ())), precision=lax.Precision.HIGHEST, preferred_element_type=F32)
    log_decay = -jax.nn.sigmoid(load(din_ref) + doff_ref[...]) * math.exp(-0.5) - extra
    tr = lax.broadcasted_iota(jnp.int32, (chunk, chunk), 0)
    tc = lax.broadcasted_iota(jnp.int32, (chunk, chunk), 1)
    lower = jnp.where(tr >= tc, 1.0, 0.0).astype(F32)
    cum = lax.dot_general(lower, log_decay, (((1,), (0,)), ((), ())), precision=lax.Precision.HIGHEST, preferred_element_type=F32)
    last = cum[chunk - 1:chunk, :]
    mid = cum[chunk // 2 - 1:chunk // 2, :]
    before = cum - log_decay
    rate = jax.nn.sigmoid(load(rin_ref) + roff_ref[...])

    key = stack(load(k_ref))
    unit = key * lax.rsqrt(jnp.sum(key * key, axis=-1, keepdims=True) + 1e-6)
    base = unit * stack(rate)
    query = stack(load(q_ref))
    value = split2(stack(load(v_ref)))
    to_mid = stack(jnp.exp(mid - cum))
    key_mid = split2(key * to_mid)
    base_mid = split2(base * to_mid)
    query_mid = split2(query * stack(jnp.exp(cum - mid)))
    unit_mid = split2(unit * stack(jnp.exp(before - mid)))
    to_last = stack(jnp.exp(last - cum))

    row = lax.broadcasted_iota(jnp.int32, (wide, wide), 0)
    col = lax.broadcasted_iota(jnp.int32, (wide, wide), 1)
    same = (row // chunk) == (col // chunk)
    strict = same & (row > col)
    upto = same & (row >= col)
    a_ub = jnp.where(strict, dot3(unit_mid, base_mid, NT), 0.0)
    a_uk = jnp.where(strict, dot3(unit_mid, key_mid, NT), 0.0)
    a_qb = jnp.where(upto, dot3(query_mid, base_mid, NT), 0.0)
    a_qk = jnp.where(upto, dot3(query_mid, key_mid, NT), 0.0)

    inverse = jnp.where(row == col, 1.0, 0.0).astype(F32)
    size = 1
    while size < chunk:
        pair = ((row // (2 * size)) == (col // (2 * size))) & ((row // size) > (col // size))
        part = jnp.where(pair, a_ub, 0.0)
        if size == 1:
            inverse = inverse - part
        else:
            inv = split2(inverse)
            inverse = inverse - dot3(split2(dot3(inv, split2(part), NN)), inv, NN)
        size *= 2
    inverse = split2(inverse)

    wr = lax.broadcasted_iota(jnp.int32, (wide, width), 0) // chunk
    wc = lax.broadcasted_iota(jnp.int32, (wide, width), 1) // HEAD

    def spread_wide(a):
        return jnp.where(wr == wc, jnp.concatenate([a] * heads, axis=1), 0.0)

    unit_wide = split2(spread_wide(unit * stack(jnp.exp(before))))
    query_wide = spread_wide(query * stack(jnp.exp(cum)))
    base_wide = split2(spread_wide(base * to_last))
    key_wide = split2(spread_wide(key * to_last))
    qb = split2(a_qb)
    trans = split2(dot3(inverse, unit_wide, NN))
    own = split2(dot3(inverse, split2(dot3(split2(a_uk), value, NN)), NN))
    read = split2(query_wide - dot3(qb, trans, NN))
    out_own = dot3(split2(a_qk), value, NN) - dot3(qb, own, NN)
    pr = lax.broadcasted_iota(jnp.int32, (width, width), 0)
    pc = lax.broadcasted_iota(jnp.int32, (width, width), 1)
    move = jnp.where(pr == pc, jnp.exp(last), 0.0) - dot3(base_wide, trans, TN)
    end = dot3(key_wide, value, TN) - dot3(base_wide, own, TN)

    z = split2(z_ref[...])
    x = dot3(read, z, NN) + jnp.concatenate([jnp.zeros_like(out_own), out_own], axis=1)
    for h in range(heads):
        reads_ref[h] = x[h * chunk:(h + 1) * chunk, :]
    z_new = dot3(split2(move), z, NN) + jnp.concatenate([jnp.zeros_like(end), end], axis=1)
    z_ref[...] = z_new
    total_ref[...] = z_new.astype(BF16)


def chunks(q, k, v, din, doff, extra, rin, roff):
    rows, width = q.shape
    heads = width // HEAD
    chunk = 64
    while rows % chunk:
        chunk //= 2
    tile = pl.BlockSpec((chunk, width), lambda i: (i, 0))
    vec = pl.BlockSpec((1, width), lambda i: (0, 0))
    n = rows // chunk
    return pl.pallas_call(
        functools.partial(chunk_kernel, heads, chunk),
        grid=(n,),
        in_specs=[tile, tile, tile, tile, vec, pl.BlockSpec((chunk, heads), lambda i: (i, 0)), tile, vec],
        out_specs=(
            pl.BlockSpec((heads, chunk, 2 * HEAD), lambda i: (0, i, 0)),
            pl.BlockSpec((width, 2 * HEAD), lambda i: (0, 0)),
        ),
        out_shape=(
            jax.ShapeDtypeStruct((heads, rows, 2 * HEAD), F32),
            jax.ShapeDtypeStruct((width, 2 * HEAD), BF16),
        ),
        scratch_shapes=[pltpu.VMEM((width, 2 * HEAD), F32)],
        compiler_params=pltpu.CompilerParams(dimension_semantics=("arbitrary",), vmem_limit_bytes=40 * 2**20),
    )(q, k, v, din, doff.reshape(1, width), extra, rin, roff.reshape(1, width))


def carry_kernel(nz, nx, total_ref, reads_ref, gain_ref, mixed_ref, held, send_sem, recv_sem):
    n = nz * nx
    me = lax.axis_index("z") * nx + lax.axis_index("x")
    heads = reads_ref.shape[0]

    def place(k):
        peer = lax.rem(me + k, n)
        return {"z": peer // nx, "x": lax.rem(peer, nx)}

    barrier = pltpu.get_barrier_semaphore()
    for k in range(1, n):
        pl.semaphore_signal(barrier, inc=1, device_id=place(k), device_id_type=pl.DeviceIdType.MESH)
    pl.semaphore_wait(barrier, n - 1)
    copies = []
    for k in range(1, n):
        c = pltpu.make_async_remote_copy(
            src_ref=total_ref, dst_ref=held.at[k], send_sem=send_sem.at[k], recv_sem=recv_sem.at[k],
            device_id=place(k), device_id_type=pl.DeviceIdType.MESH)
        c.start()
        copies.append(c)
    for c in copies:
        c.wait()
    state = [jnp.zeros((HEAD, HEAD), F32) for _ in range(heads)]
    for k in range(n - 1, 0, -1):
        there = k <= me
        for h in range(heads):
            block = held[k, h * HEAD:(h + 1) * HEAD, :].astype(F32)
            new = block[:, HEAD:] + jnp.dot(block[:, :HEAD], state[h], precision=lax.Precision.HIGHEST, preferred_element_type=F32)
            state[h] = jnp.where(there, new, state[h])
    outs = []
    for h in range(heads):
        x = reads_ref[h]
        o = x[:, HEAD:] + dot3(split2(x[:, :HEAD]), split2(state[h]), NN)
        center = o - jnp.mean(o, axis=-1, keepdims=True)
        var = jnp.mean(center * center, axis=-1, keepdims=True)
        outs.append(center * lax.rsqrt(var + 1e-5))
    mixed_ref[...] = (jnp.concatenate(outs, axis=1) * gain_ref[...]).astype(BF16)


def carry(total, reads, gain, nz, nx):
    heads, rows, _ = reads.shape
    width = heads * HEAD
    n = nz * nx
    vm = pl.BlockSpec(memory_space=pltpu.VMEM)
    return pl.pallas_call(
        functools.partial(carry_kernel, nz, nx),
        in_specs=[vm, vm, vm],
        out_specs=vm,
        out_shape=jax.ShapeDtypeStruct((rows, width), BF16),
        scratch_shapes=[
            pltpu.VMEM((n, width, 2 * HEAD), BF16),
            pltpu.SemaphoreType.DMA((n,)),
            pltpu.SemaphoreType.DMA((n,)),
        ],
        compiler_params=pltpu.CompilerParams(collective_id=1, has_side_effects=True, vmem_limit_bytes=24 * 2**20),
    )(total, reads, gain.reshape(1, width))


def send_z(block, nz):
    return [lax.ppermute(block, "z", [(s, (s + k) % nz) for s in range(nz)]) for k in range(1, nz)]


def in_order(block, came, nz, axis):
    z = lax.axis_index("z")
    size = block.shape[axis]
    shape = list(block.shape)
    shape[axis] = size * nz
    whole = jnp.zeros(shape, block.dtype)
    whole = lax.dynamic_update_slice_in_dim(whole, block, z * size, axis)
    for k in range(1, nz):
        whole = lax.dynamic_update_slice_in_dim(whole, came[k - 1], lax.rem(z - k + nz, nz) * size, axis)
    return whole


def per_device(
    nz, nx,
    resid, queries, keys, values, decay_input_part, decay_channel_offset, decay_head_extra,
    correction_rate_input, correction_rate_offset, head_norm_gain, mixer_output_weight,
    feedforward_norm_gain, gate_weight, up_weight, down_weight,
):
    ff = gate_weight.shape[1] // nx
    x = lax.axis_index("x")

    def exchange(weight, axis, join):
        pieces = weight.reshape(weight.shape[:axis] + (nx, ff) + weight.shape[axis + 1:])
        return lax.all_to_all(pieces, "x", split_axis=axis, concat_axis=join, tiled=False)

    def swap(weight, axis, join):
        if nx == 1:
            return weight
        if nx != 2:
            out = exchange(weight, axis, join)
            return out.reshape((-1, ff) if axis == 1 else (ff, -1))
        mine = lax.dynamic_slice_in_dim(weight, x * ff, ff, axis)
        other = lax.dynamic_slice_in_dim(weight, (1 - x) * ff, ff, axis)
        came = lax.ppermute(other, "x", [(0, 1), (1, 0)])
        first = jnp.where(x == 0, mine, came)
        second = jnp.where(x == 0, came, mine)
        return jnp.concatenate([first, second], axis=join)

    halves = (swap(gate_weight, 1, 0), swap(up_weight, 1, 0), swap(down_weight, 0, 1))
    halves, queries = lax.optimization_barrier((halves, queries))
    whole_gate = lax.all_gather(halves[0], "z", axis=0, tiled=True)
    up_came = send_z(halves[1], nz)
    down_came = send_z(halves[2], nz)

    reads, total = chunks(
        queries, keys, values, decay_input_part, decay_channel_offset, decay_head_extra,
        correction_rate_input, correction_rate_offset)
    total, up_came = lax.optimization_barrier((total, up_came))
    mixed = carry(total, reads, head_norm_gain, nz, nx)
    row_mixed = lax.all_to_all(mixed, "tp", split_axis=0, concat_axis=1, tiled=True)
    proj = jnp.dot(row_mixed, mixer_output_weight, preferred_element_type=F32)
    mid_f = (resid.astype(F32) + proj).astype(BF16).astype(F32)
    normed = (
        mid_f
        * lax.rsqrt(jnp.mean(mid_f * mid_f, axis=-1, keepdims=True) + 1e-06)
        * feedforward_norm_gain
    ).astype(BF16)
    normed, whole_gate = lax.optimization_barrier((normed, whole_gate))
    whole_up = in_order(halves[1], up_came, nz, 0)
    whole_down = in_order(halves[2], down_came, nz, 1)
    whole_rows = lax.all_gather(normed, ("x", "tp"), axis=0, tiled=True)
    gate = jnp.dot(whole_rows, whole_gate, preferred_element_type=F32)
    upper = jnp.dot(whole_rows, whole_up, preferred_element_type=F32)
    hidden = (jax.nn.silu(gate) * upper).astype(BF16)
    down_sum = lax.psum_scatter(
        jnp.dot(hidden, whole_down, preferred_element_type=F32).astype(BF16),
        ("x", "tp"), scatter_dimension=0, tiled=True,
    ).astype(F32)
    return (mid_f + 0.5 * down_sum).astype(BF16)


MESH = pl.DeviceIdType.MESH


def layer_kernel(
    chunk, q_ref, k_ref, v_ref, din_ref, doff_ref, extra_ref, rin_ref, roff_ref, gain_ref, resid_ref, fgain_ref, wo_hbm, gate_hbm, up_hbm, down_hbm, out_ref,
    total_ref, reads_ref, z_ref, held, mixed, mixrow, wo, mid, tok, gate, up, down, hidden, near_sum, far_sum, y_out, y_in, z_out, z_in,
    wo_sem, w_send, w_recv, c_send, c_recv, a_send, a_recv, t_send, t_recv, y_send, y_recv, z_send, z_recv,
):
    z, x, y, c = (lax.axis_index(name) for name in ("z", "x", "y", "c"))
    half, low = z // 2, lax.rem(z, 2)
    sib = z + 1 - 2 * low
    pair = lax.rem(z + 2, 4)
    near = 1 + half
    mine = c == half
    me = 2 * z + x
    n = 8
    depth = gate_hbm.shape[0]
    heads = reads_ref.shape[0]
    width = heads * HEAD
    rows = resid_ref.shape[0]
    model = resid_ref.shape[1]
    sources = (gate_hbm, up_hbm, down_hbm)

    def at(index, size):
        return pl.ds(pl.multiple_of(index * size, size), size)

    def remote(src, dst, send, recv, **where):
        return pltpu.make_async_remote_copy(
            src_ref=src, dst_ref=dst, send_sem=send, recv_sem=recv, device_id=where, device_id_type=MESH)

    def piece(m, s):
        return down.at[:, at(s, depth)] if m == 2 else (gate, up)[m].at[at(s, depth), :]

    def to(src, m, s, slot, **where):
        return remote(src, piece(m, s), w_send.at[m, slot], w_recv.at[m, s], **where)

    def landed(m, s):
        to(piece(m, s), m, s, 0, c=1 - c).wait_recv()

    def own(m):
        return pltpu.make_async_copy(sources[m], piece(m, me), w_recv.at[m, me])

    def side_sends(m):
        src = sources[m]
        return ((mine, (to(src, m, me, 1, x=1 - x), to(src, m, me, 2, c=1 - c))),)

    def line_sends(m):
        src = sources[m]
        return (
            (mine, (to(src, m, me, 0, z=sib, c=1 - half),)),
            (jnp.logical_not(mine), (to(src, m, me, 3, z=1 + c, c=low),)),
        )

    first = jnp.where(mine, z, sib)
    second = 2 * (1 - half) + c
    other_first = jnp.where(mine, sib, z)
    other_second = 2 * (1 - half) + 1 - c

    def relay(m, step):
        s = 2 * (first, second, first, second)[step] + (x, x, 1 - x, 1 - x)[step]
        p = piece(m, s)
        if step == 0:
            return s, ((jnp.logical_not(mine), (to(p, m, s, 4, x=1 - x), to(p, m, s, 5, c=1 - c))),)
        if step == 1:
            return s, (
                (z == near, (to(p, m, s, 6, z=3 * half),)),
                (None, (to(p, m, s, 7, x=1 - x), to(p, m, s, 8, c=1 - c))),
            )
        return s, ((None, (to(p, m, s, 7 + step, c=1 - c),)),)

    def each(groups, act):
        for when, copies in groups:
            if when is None:
                for copy in copies:
                    act(copy)
            else:
                @pl.when(when)
                def _():
                    for copy in copies:
                        act(copy)

    def start(copy):
        copy.start()

    def begin(m):
        @pl.when(mine)
        def _():
            own(m).start()
        each(side_sends(m), start)

    def pump(m, step):
        s, groups = relay(m, step)
        landed(m, s)
        each(groups, start)

    def rest_of(m):
        for plane in (other_first, other_second):
            for column in (x, 1 - x):
                landed(m, 2 * plane + column)

    def drain(m):
        for groups in (side_sends(m), line_sends(m), *(relay(m, step)[1] for step in range(4))):
            each(groups, lambda copy: copy.wait_send())

    barrier = pltpu.get_barrier_semaphore()
    for dz in range(4):
        for dx in range(2):
            for dy in range(2):
                for dc in range(2):
                    if dz or dx or dy or dc:
                        peer = {"z": lax.rem(z + dz, 4), "x": lax.rem(x + dx, 2), "y": lax.rem(y + dy, 2), "c": lax.rem(c + dc, 2)}
                        pl.semaphore_signal(barrier, inc=1, device_id=peer, device_id_type=MESH)
    pl.semaphore_wait(barrier, 31)

    load_wo = pltpu.make_async_copy(wo_hbm, wo, wo_sem)
    load_wo.start()

    def place(k):
        peer = lax.rem(me + k, n)
        return {"z": peer // 2, "x": lax.rem(peer, 2)}

    def carry_copy(k):
        return remote(total_ref, held.at[k], c_send.at[k], c_recv.at[k], **place(k))

    leftward = jnp.logical_or(z == 3, jnp.logical_and(c == 0, z >= 1))
    each(line_sends(0), start)
    begin(0)
    each(line_sends(1), start)
    begin(1)
    begin(2)

    @pl.when(leftward)
    def _():
        each(line_sends(2), start)
    is_near = z == near
    is_far = jnp.logical_not(is_near)
    tokens = q_ref.shape[0]

    def advance(i, _):
        span = at(i, chunk)
        chunk_step(
            heads, chunk, i, q_ref.at[span, :], k_ref.at[span, :], v_ref.at[span, :], din_ref.at[span, :], doff_ref,
            extra_ref.at[span, :], rin_ref.at[span, :], roff_ref, reads_ref.at[:, span, :], total_ref, z_ref)

        @pl.when(jnp.logical_and(i == 1, is_far))
        def _():
            pump(0, 0)

        @pl.when(jnp.logical_and(i == 3, is_far))
        def _():
            pump(1, 0)

        @pl.when(jnp.logical_and(i == 3, is_near))
        def _():
            pump(0, 0)
            pump(0, 1)

        return 0

    lax.fori_loop(0, tokens // chunk, advance, 0)

    for k in range(1, n):
        @pl.when(me + k < n)
        def _():
            carry_copy(k).start()
    @pl.when(jnp.logical_not(leftward))
    def _():
        each(line_sends(2), start)

    @pl.when(is_near)
    def _():
        pump(1, 0)
        pump(1, 1)
    for k in range(1, n):
        @pl.when(me >= k)
        def _():
            carry_copy(k).wait_recv()
    state = [jnp.zeros((HEAD, HEAD), F32) for _ in range(heads)]
    for k in range(n - 1, 0, -1):
        there = k <= me
        for h in range(heads):
            block = held[k, h * HEAD:(h + 1) * HEAD, :].astype(F32)
            new = block[:, HEAD:] + jnp.dot(block[:, :HEAD], state[h], precision=lax.Precision.HIGHEST, preferred_element_type=F32)
            state[h] = jnp.where(there, new, state[h])
    outs = []
    for h in range(heads):
        r = reads_ref[h]
        o = r[:, HEAD:] + dot3(split2(r[:, :HEAD]), split2(state[h]), NN)
        center = o - jnp.mean(o, axis=-1, keepdims=True)
        var = jnp.mean(center * center, axis=-1, keepdims=True)
        outs.append(center * lax.rsqrt(var + 1e-5))
    mixed[...] = (jnp.concatenate(outs, axis=1) * gain_ref[...]).astype(BF16)

    t = 2 * y + c

    def exchange(dy, dc):
        ty, tc = lax.rem(y + dy, 2), lax.rem(c + dc, 2)
        slot = 2 * dy + dc
        return remote(
            mixed.at[at(2 * ty + tc, rows), :], mixrow.at[:, at(t, width)], a_send.at[slot], a_recv.at[slot], y=ty, c=tc)

    swaps = [exchange(1, 0), exchange(1, 1), exchange(0, 1)]
    for copy in swaps:
        copy.start()
    mixrow[:, at(t, width)] = mixed[at(t, rows), :]

    @pl.when(is_far)
    def _():
        pump(0, 1)
    pump(2, 0)
    load_wo.wait()
    for copy in swaps:
        copy.wait()

    tile = 512
    square = jnp.zeros((rows, 1), F32)
    for j in range(0, model, tile):
        proj = jnp.dot(mixrow[...], wo[:, j:j + tile], preferred_element_type=F32)
        part = (resid_ref[:, j:j + tile].astype(F32) + proj).astype(BF16).astype(F32)
        mid[:, j:j + tile] = part
        square += jnp.sum(part * part, axis=-1, keepdims=True)
    g = 2 * half + y
    g_far = 2 * (1 - half) + y
    g_side = 2 * half + 1 - y
    g_diag = 2 * (1 - half) + 1 - y
    tok[at(g, rows), :] = (mid[...] * lax.rsqrt(square / model + 1e-06) * fgain_ref[...]).astype(BF16)

    def rows_to(block, slot, **where):
        r = tok.at[at(block, rows), :]
        return remote(r, r, t_send.at[slot], t_recv.at[slot], **where)

    def rows_from(block, slot):
        r = tok.at[at(block, rows), :]
        remote(r, r, t_send.at[slot], t_recv.at[slot], y=1 - y).wait_recv()

    ahead = rows_to(g, 0, z=pair)
    beside = rows_to(g, 1, y=1 - y)
    onward = rows_to(g_far, 2, y=1 - y)
    ahead.start()
    beside.start()

    @pl.when(is_near)
    def _():
        pump(2, 1)

    @pl.when(is_far)
    def _():
        pump(1, 1)
    pump(0, 2)
    pump(1, 2)
    pump(0, 3)
    rows_from(g_far, 0)
    onward.start()

    @pl.when(is_far)
    def _():
        pump(2, 1)
    pump(2, 2)
    pump(1, 3)
    rest_of(0)
    rest_of(1)
    rows_from(g_side, 1)
    rows_from(g_diag, 2)

    units = gate.shape[1]
    for j in range(0, units, 256):
        cols = slice(j, min(j + 256, units))
        gated = jnp.dot(tok[...], gate[:, cols], preferred_element_type=F32)
        upper = jnp.dot(tok[...], up[:, cols], preferred_element_type=F32)
        hidden[:, cols] = (gated * jax.nn.sigmoid(gated) * upper).astype(BF16)

    def side_copy(i):
        return remote(y_out.at[i], y_in.at[i], y_send.at[i], y_recv.at[i], y=1 - y)

    def far_copy(i):
        return remote(z_out.at[i], z_in.at[i], z_send.at[i], z_recv.at[i], z=pair)

    def slice_of(plane, column):
        i = 2 * plane + column
        cols = at(i, depth)
        for place_of, dst in ((g_diag, y_out.at[i, 0]), (g_side, y_out.at[i, 1])):
            dst[...] = jnp.dot(hidden[at(place_of, rows), :], down[:, cols], preferred_element_type=F32).astype(BF16)
        far_sum[:, cols] = jnp.dot(hidden[at(g_far, rows), :], down[:, cols], preferred_element_type=F32)
        side_copy(i).start()
        near_sum[:, cols] = jnp.dot(hidden[at(g, rows), :], down[:, cols], preferred_element_type=F32)

    def pass_on(plane, column):
        i = 2 * plane + column
        side_copy(i).wait_recv()
        z_out[i] = (far_sum[:, at(i, depth)] + y_in[i, 0].astype(F32)).astype(BF16)
        far_copy(i).start()

    slice_of(first, x)
    slice_of(first, 1 - x)
    for column in (x, 1 - x):
        landed(2, 2 * other_first + column)
        slice_of(other_first, column)
    for plane in (first, other_first):
        for column in (x, 1 - x):
            pass_on(plane, column)
    slice_of(second, x)
    landed(2, 2 * other_second + x)
    slice_of(other_second, x)
    pump(2, 3)
    slice_of(second, 1 - x)
    landed(2, 2 * other_second + 1 - x)
    slice_of(other_second, 1 - x)
    for column in (x, 1 - x):
        for plane in (second, other_second):
            pass_on(plane, column)
    for i in range(n):
        cols = slice(i * depth, (i + 1) * depth)
        far_copy(i).wait_recv()
        total = near_sum[:, cols] + y_in[i, 1].astype(F32) + z_in[i].astype(F32)
        out_ref[:, cols] = (mid[:, cols] + 0.5 * total).astype(BF16)

    for k in range(1, n):
        @pl.when(me + k < n)
        def _():
            carry_copy(k).wait_send()
    for m in range(3):
        drain(m)
    for copy in (ahead, beside, onward):
        copy.wait_send()
    for i in range(n):
        side_copy(i).wait_send()
        far_copy(i).wait_send()


def layer(q, k, v, din, doff, extra, rin, roff, gain, resid, fgain, wo, gate, up, down):
    tokens, width = q.shape
    heads = width // HEAD
    chunk = 64
    while tokens % chunk:
        chunk //= 2
    rows, model = resid.shape
    depth, units = gate.shape
    n = 8
    vm = pl.BlockSpec(memory_space=pltpu.VMEM)
    hbm = pl.BlockSpec(memory_space=pl.ANY)
    dma = pltpu.SemaphoreType.DMA
    return pl.pallas_call(
        functools.partial(layer_kernel, chunk),
        in_specs=[vm] * 11 + [hbm] * 4,
        out_specs=vm,
        out_shape=jax.ShapeDtypeStruct((rows, model), BF16),
        scratch_shapes=[
            pltpu.VMEM((width, 2 * HEAD), BF16),
            pltpu.VMEM((heads, tokens, 2 * HEAD), F32),
            pltpu.VMEM((width, 2 * HEAD), F32),
            pltpu.VMEM((n, width, 2 * HEAD), BF16),
            pltpu.VMEM((tokens, width), BF16),
            pltpu.VMEM((rows, wo.shape[0]), BF16),
            pltpu.VMEM(wo.shape, BF16),
            pltpu.VMEM((rows, model), F32),
            pltpu.VMEM((4 * rows, model), BF16),
            pltpu.VMEM((n * depth, units), BF16),
            pltpu.VMEM((n * depth, units), BF16),
            pltpu.VMEM((units, n * depth), BF16),
            pltpu.VMEM((4 * rows, units), BF16),
            pltpu.VMEM((rows, model), F32),
            pltpu.VMEM((rows, model), F32),
            pltpu.VMEM((n, 2, rows, depth), BF16),
            pltpu.VMEM((n, 2, rows, depth), BF16),
            pltpu.VMEM((n, rows, depth), BF16),
            pltpu.VMEM((n, rows, depth), BF16),
            dma, dma((3, 11)), dma((3, n)), dma((n,)), dma((n,)), dma((4,)), dma((4,)), dma((3,)), dma((3,)),
            dma((n,)), dma((n,)), dma((n,)), dma((n,)),
        ],
        compiler_params=pltpu.CompilerParams(collective_id=2, has_side_effects=True, vmem_limit_bytes=56 * 2**20),
    )(q, k, v, din, doff.reshape(1, width), extra, rin, roff.reshape(1, width), gain.reshape(1, width), resid, fgain.reshape(1, model), wo, gate, up, down)


def per_device_pairs(
    resid, queries, keys, values, decay_input_part, decay_channel_offset, decay_head_extra,
    correction_rate_input, correction_rate_offset, head_norm_gain, mixer_output_weight,
    feedforward_norm_gain, gate_weight, up_weight, down_weight,
):
    return layer(
        queries, keys, values, decay_input_part, decay_channel_offset, decay_head_extra,
        correction_rate_input, correction_rate_offset, head_norm_gain, resid, feedforward_norm_gain, mixer_output_weight, gate_weight, up_weight, down_weight)


def solution(mesh):
    n_sp, n_tp = mesh.shape["sp"], mesh.shape["tp"]
    if (n_sp, n_tp) == (8, 4):
        inner = Mesh(mesh.devices.reshape(4, 2, 2, 2), ("z", "x", "y", "c"))
        sp, tp = ("z", "x"), ("y", "c")
        body = per_device_pairs
    else:
        nx = 2 if n_sp % 2 == 0 else 1
        nz = n_sp // nx
        inner = Mesh(mesh.devices.reshape(nz, nx, n_tp), ("z", "x", "tp"))
        sp, tp = ("z", "x"), ("tp",)
        body = functools.partial(per_device, nz, nx)
    rows = P((*sp, *tp), None)
    placed = (
        rows, P(sp, tp), P(sp, tp), P(sp, tp), P(sp, tp), P(tp), P(sp, tp), P(sp, tp), P(tp), P(tp), P(), P(),
        P(sp, tp), P(sp, tp), P(tp, sp),
    )
    return jax.shard_map(body, mesh=inner, in_specs=placed, out_specs=rows, check_vma=False)
```

```python
import functools
import math

import jax
import jax.numpy as jnp
from jax import lax
from jax.experimental import pallas as pl
from jax.experimental.pallas import tpu as pltpu
from jax.sharding import Mesh, PartitionSpec as P

HEAD = 64
F32 = jnp.float32
BF16 = jnp.bfloat16


def split2(a):
    high = a.astype(BF16)
    return high, (a - high.astype(F32)).astype(BF16)


def dot3(a, b, dims):
    (ah, al), (bh, bl) = a, b
    dn = (dims, ((), ()))
    d = functools.partial(lax.dot_general, dimension_numbers=dn, preferred_element_type=F32)
    return d(ah, bh) + (d(ah, bl) + d(al, bh))


NN = ((1,), (0,))
NT = ((1,), (1,))
TN = ((0,), (0,))


def chunk_kernel(heads, chunk, *refs):
    chunk_step(heads, chunk, pl.program_id(0), *refs)


def chunk_step(heads, chunk, step, q_ref, k_ref, v_ref, din_ref, doff_ref, extra_ref, rin_ref, roff_ref, reads_ref, total_ref, z_ref):
    rows = q_ref.shape[0]
    width = heads * HEAD
    wide = heads * chunk

    @pl.when(step == 0)
    def _():
        r = lax.broadcasted_iota(jnp.int32, (width, 2 * HEAD), 0) % HEAD
        c = lax.broadcasted_iota(jnp.int32, (width, 2 * HEAD), 1)
        z_ref[...] = jnp.where(r == c, 1.0, 0.0).astype(F32)

    def load(ref):
        return ref[...].astype(F32)

    def stack(a):
        return jnp.concatenate([a[:, h * HEAD:(h + 1) * HEAD] for h in range(heads)], axis=0)

    spread_r = lax.broadcasted_iota(jnp.int32, (heads, width), 0)
    spread_c = lax.broadcasted_iota(jnp.int32, (heads, width), 1) // HEAD
    spread = jnp.where(spread_r == spread_c, 1.0, 0.0).astype(F32)
    extra = extra_ref[...]
    if extra.shape[1] == heads:
        extra = lax.dot_general(extra, spread, ((((1,), (0,))), ((), ())), precision=lax.Precision.HIGHEST, preferred_element_type=F32)
    log_decay = -jax.nn.sigmoid(load(din_ref) + doff_ref[...]) * math.exp(-0.5) - extra
    tr = lax.broadcasted_iota(jnp.int32, (chunk, chunk), 0)
    tc = lax.broadcasted_iota(jnp.int32, (chunk, chunk), 1)
    lower = jnp.where(tr >= tc, 1.0, 0.0).astype(F32)
    cum = lax.dot_general(lower, log_decay, (((1,), (0,)), ((), ())), precision=lax.Precision.HIGHEST, preferred_element_type=F32)
    last = cum[chunk - 1:chunk, :]
    mid = cum[chunk // 2 - 1:chunk // 2, :]
    before = cum - log_decay
    rate = jax.nn.sigmoid(load(rin_ref) + roff_ref[...])

    key = stack(load(k_ref))
    unit = key * lax.rsqrt(jnp.sum(key * key, axis=-1, keepdims=True) + 1e-6)
    base = unit * stack(rate)
    query = stack(load(q_ref))
    value = split2(stack(load(v_ref)))
    to_mid = stack(jnp.exp(mid - cum))
    key_mid = split2(key * to_mid)
    base_mid = split2(base * to_mid)
    query_mid = split2(query * stack(jnp.exp(cum - mid)))
    unit_mid = split2(unit * stack(jnp.exp(before - mid)))
    to_last = stack(jnp.exp(last - cum))

    row = lax.broadcasted_iota(jnp.int32, (wide, wide), 0)
    col = lax.broadcasted_iota(jnp.int32, (wide, wide), 1)
    same = (row // chunk) == (col // chunk)
    strict = same & (row > col)
    upto = same & (row >= col)
    a_ub = jnp.where(strict, dot3(unit_mid, base_mid, NT), 0.0)
    a_uk = jnp.where(strict, dot3(unit_mid, key_mid, NT), 0.0)
    a_qb = jnp.where(upto, dot3(query_mid, base_mid, NT), 0.0)
    a_qk = jnp.where(upto, dot3(query_mid, key_mid, NT), 0.0)

    inverse = jnp.where(row == col, 1.0, 0.0).astype(F32)
    size = 1
    while size < chunk:
        pair = ((row // (2 * size)) == (col // (2 * size))) & ((row // size) > (col // size))
        part = jnp.where(pair, a_ub, 0.0)
        if size == 1:
            inverse = inverse - part
        else:
            inv = split2(inverse)
            inverse = inverse - dot3(split2(dot3(inv, split2(part), NN)), inv, NN)
        size *= 2
    inverse = split2(inverse)

    wr = lax.broadcasted_iota(jnp.int32, (wide, width), 0) // chunk
    wc = lax.broadcasted_iota(jnp.int32, (wide, width), 1) // HEAD

    def spread_wide(a):
        return jnp.where(wr == wc, jnp.concatenate([a] * heads, axis=1), 0.0)

    unit_wide = split2(spread_wide(unit * stack(jnp.exp(before))))
    query_wide = spread_wide(query * stack(jnp.exp(cum)))
    base_wide = split2(spread_wide(base * to_last))
    key_wide = split2(spread_wide(key * to_last))
    qb = split2(a_qb)
    trans = split2(dot3(inverse, unit_wide, NN))
    own = split2(dot3(inverse, split2(dot3(split2(a_uk), value, NN)), NN))
    read = split2(query_wide - dot3(qb, trans, NN))
    out_own = dot3(split2(a_qk), value, NN) - dot3(qb, own, NN)
    pr = lax.broadcasted_iota(jnp.int32, (width, width), 0)
    pc = lax.broadcasted_iota(jnp.int32, (width, width), 1)
    move = jnp.where(pr == pc, jnp.exp(last), 0.0) - dot3(base_wide, trans, TN)
    end = dot3(key_wide, value, TN) - dot3(base_wide, own, TN)

    z = split2(z_ref[...])
    x = dot3(read, z, NN) + jnp.concatenate([jnp.zeros_like(out_own), out_own], axis=1)
    for h in range(heads):
        reads_ref[h] = x[h * chunk:(h + 1) * chunk, :]
    z_new = dot3(split2(move), z, NN) + jnp.concatenate([jnp.zeros_like(end), end], axis=1)
    z_ref[...] = z_new
    total_ref[...] = z_new.astype(BF16)


def chunks(q, k, v, din, doff, extra, rin, roff):
    rows, width = q.shape
    heads = width // HEAD
    chunk = 64
    while rows % chunk:
        chunk //= 2
    tile = pl.BlockSpec((chunk, width), lambda i: (i, 0))
    vec = pl.BlockSpec((1, width), lambda i: (0, 0))
    n = rows // chunk
    return pl.pallas_call(
        functools.partial(chunk_kernel, heads, chunk),
        grid=(n,),
        in_specs=[tile, tile, tile, tile, vec, pl.BlockSpec((chunk, heads), lambda i: (i, 0)), tile, vec],
        out_specs=(
            pl.BlockSpec((heads, chunk, 2 * HEAD), lambda i: (0, i, 0)),
            pl.BlockSpec((width, 2 * HEAD), lambda i: (0, 0)),
        ),
        out_shape=(
            jax.ShapeDtypeStruct((heads, rows, 2 * HEAD), F32),
            jax.ShapeDtypeStruct((width, 2 * HEAD), BF16),
        ),
        scratch_shapes=[pltpu.VMEM((width, 2 * HEAD), F32)],
        compiler_params=pltpu.CompilerParams(dimension_semantics=("arbitrary",), vmem_limit_bytes=40 * 2**20),
    )(q, k, v, din, doff.reshape(1, width), extra, rin, roff.reshape(1, width))


def carry_kernel(nz, nx, total_ref, reads_ref, gain_ref, mixed_ref, held, send_sem, recv_sem):
    n = nz * nx
    me = lax.axis_index("z") * nx + lax.axis_index("x")
    heads = reads_ref.shape[0]

    def place(k):
        peer = lax.rem(me + k, n)
        return {"z": peer // nx, "x": lax.rem(peer, nx)}

    barrier = pltpu.get_barrier_semaphore()
    for k in range(1, n):
        pl.semaphore_signal(barrier, inc=1, device_id=place(k), device_id_type=pl.DeviceIdType.MESH)
    pl.semaphore_wait(barrier, n - 1)
    copies = []
    for k in range(1, n):
        c = pltpu.make_async_remote_copy(
            src_ref=total_ref, dst_ref=held.at[k], send_sem=send_sem.at[k], recv_sem=recv_sem.at[k],
            device_id=place(k), device_id_type=pl.DeviceIdType.MESH)
        c.start()
        copies.append(c)
    for c in copies:
        c.wait()
    state = [jnp.zeros((HEAD, HEAD), F32) for _ in range(heads)]
    for k in range(n - 1, 0, -1):
        there = k <= me
        for h in range(heads):
            block = held[k, h * HEAD:(h + 1) * HEAD, :].astype(F32)
            new = block[:, HEAD:] + jnp.dot(block[:, :HEAD], state[h], precision=lax.Precision.HIGHEST, preferred_element_type=F32)
            state[h] = jnp.where(there, new, state[h])
    outs = []
    for h in range(heads):
        x = reads_ref[h]
        o = x[:, HEAD:] + dot3(split2(x[:, :HEAD]), split2(state[h]), NN)
        center = o - jnp.mean(o, axis=-1, keepdims=True)
        var = jnp.mean(center * center, axis=-1, keepdims=True)
        outs.append(center * lax.rsqrt(var + 1e-5))
    mixed_ref[...] = (jnp.concatenate(outs, axis=1) * gain_ref[...]).astype(BF16)


def carry(total, reads, gain, nz, nx):
    heads, rows, _ = reads.shape
    width = heads * HEAD
    n = nz * nx
    vm = pl.BlockSpec(memory_space=pltpu.VMEM)
    return pl.pallas_call(
        functools.partial(carry_kernel, nz, nx),
        in_specs=[vm, vm, vm],
        out_specs=vm,
        out_shape=jax.ShapeDtypeStruct((rows, width), BF16),
        scratch_shapes=[
            pltpu.VMEM((n, width, 2 * HEAD), BF16),
            pltpu.SemaphoreType.DMA((n,)),
            pltpu.SemaphoreType.DMA((n,)),
        ],
        compiler_params=pltpu.CompilerParams(collective_id=1, has_side_effects=True, vmem_limit_bytes=24 * 2**20),
    )(total, reads, gain.reshape(1, width))


def send_z(block, nz):
    return [lax.ppermute(block, "z", [(s, (s + k) % nz) for s in range(nz)]) for k in range(1, nz)]


def in_order(block, came, nz, axis):
    z = lax.axis_index("z")
    size = block.shape[axis]
    shape = list(block.shape)
    shape[axis] = size * nz
    whole = jnp.zeros(shape, block.dtype)
    whole = lax.dynamic_update_slice_in_dim(whole, block, z * size, axis)
    for k in range(1, nz):
        whole = lax.dynamic_update_slice_in_dim(whole, came[k - 1], lax.rem(z - k + nz, nz) * size, axis)
    return whole


def per_device(
    nz, nx,
    resid, queries, keys, values, decay_input_part, decay_channel_offset, decay_head_extra,
    correction_rate_input, correction_rate_offset, head_norm_gain, mixer_output_weight,
    feedforward_norm_gain, gate_weight, up_weight, down_weight,
):
    ff = gate_weight.shape[1] // nx
    x = lax.axis_index("x")

    def exchange(weight, axis, join):
        pieces = weight.reshape(weight.shape[:axis] + (nx, ff) + weight.shape[axis + 1:])
        return lax.all_to_all(pieces, "x", split_axis=axis, concat_axis=join, tiled=False)

    def swap(weight, axis, join):
        if nx == 1:
            return weight
        if nx != 2:
            out = exchange(weight, axis, join)
            return out.reshape((-1, ff) if axis == 1 else (ff, -1))
        mine = lax.dynamic_slice_in_dim(weight, x * ff, ff, axis)
        other = lax.dynamic_slice_in_dim(weight, (1 - x) * ff, ff, axis)
        came = lax.ppermute(other, "x", [(0, 1), (1, 0)])
        first = jnp.where(x == 0, mine, came)
        second = jnp.where(x == 0, came, mine)
        return jnp.concatenate([first, second], axis=join)

    halves = (swap(gate_weight, 1, 0), swap(up_weight, 1, 0), swap(down_weight, 0, 1))
    halves, queries = lax.optimization_barrier((halves, queries))
    whole_gate = lax.all_gather(halves[0], "z", axis=0, tiled=True)
    up_came = send_z(halves[1], nz)
    down_came = send_z(halves[2], nz)

    reads, total = chunks(
        queries, keys, values, decay_input_part, decay_channel_offset, decay_head_extra,
        correction_rate_input, correction_rate_offset)
    total, up_came = lax.optimization_barrier((total, up_came))
    mixed = carry(total, reads, head_norm_gain, nz, nx)
    row_mixed = lax.all_to_all(mixed, "tp", split_axis=0, concat_axis=1, tiled=True)
    proj = jnp.dot(row_mixed, mixer_output_weight, preferred_element_type=F32)
    mid_f = (resid.astype(F32) + proj).astype(BF16).astype(F32)
    normed = (
        mid_f
        * lax.rsqrt(jnp.mean(mid_f * mid_f, axis=-1, keepdims=True) + 1e-06)
        * feedforward_norm_gain
    ).astype(BF16)
    normed, whole_gate = lax.optimization_barrier((normed, whole_gate))
    whole_up = in_order(halves[1], up_came, nz, 0)
    whole_down = in_order(halves[2], down_came, nz, 1)
    whole_rows = lax.all_gather(normed, ("x", "tp"), axis=0, tiled=True)
    gate = jnp.dot(whole_rows, whole_gate, preferred_element_type=F32)
    upper = jnp.dot(whole_rows, whole_up, preferred_element_type=F32)
    hidden = (jax.nn.silu(gate) * upper).astype(BF16)
    down_sum = lax.psum_scatter(
        jnp.dot(hidden, whole_down, preferred_element_type=F32).astype(BF16),
        ("x", "tp"), scatter_dimension=0, tiled=True,
    ).astype(F32)
    return (mid_f + 0.5 * down_sum).astype(BF16)


MESH = pl.DeviceIdType.MESH


def wide_step(heads, q_ref, k_ref, v_ref, din_ref, doff_ref, extra_ref, rin_ref, roff_ref, read_ref, own_ref, zm_ref, ze_ref):
    chunk = q_ref.shape[0]
    width = heads * HEAD

    def load(ref):
        return ref[...].astype(F32)

    def dot(a, b, dims=NN):
        return lax.dot_general(a, b, (dims, ((), ())), preferred_element_type=F32)

    big_r = lax.broadcasted_iota(jnp.int32, (width, width), 0)
    big_c = lax.broadcasted_iota(jnp.int32, (width, width), 1)
    same = (big_r // HEAD) == (big_c // HEAD)
    blocks = jnp.where(same, 1.0, 0.0).astype(BF16)

    def blocked(pair):
        return tuple(jnp.concatenate([a] * heads, axis=0) * blocks for a in pair)

    def exact(pair, b):
        return dot(pair[0], b) + dot(pair[1], b)

    key = load(k_ref)
    unit = key * lax.rsqrt(exact(split2(key * key), blocks) + 1e-6)
    base = unit * jax.nn.sigmoid(load(rin_ref) + roff_ref[...])
    query = load(q_ref)
    log_decay = -jax.nn.sigmoid(load(din_ref) + doff_ref[...]) * math.exp(-0.5) - extra_ref[...]
    tr = lax.broadcasted_iota(jnp.int32, (chunk, chunk), 0)
    tc = lax.broadcasted_iota(jnp.int32, (chunk, chunk), 1)
    lower = jnp.where(tr >= tc, 1.0, 0.0).astype(BF16)
    ld_high, ld_rest = split2(log_decay)
    ld_mid, ld_low = split2(log_decay - ld_high.astype(F32))
    cum = dot(lower, ld_high) + (dot(lower, ld_mid) + dot(lower, ld_low))
    last = cum[chunk - 1:chunk, :]
    mid = cum[chunk // 2 - 1:chunk // 2, :]
    before = cum - log_decay
    to_mid = jnp.exp(mid - cum)
    to_last = jnp.exp(last - cum)
    key_mid = blocked(split2(key * to_mid))
    base_mid = blocked(split2(base * to_mid))
    left = split2(jnp.concatenate([unit * jnp.exp(before - mid), query * jnp.exp(cum - mid)], axis=0))
    by_base = dot3(left, base_mid, NT)
    by_key = dot3(left, key_mid, NT)
    row = lax.broadcasted_iota(jnp.int32, (chunk, width), 0)
    col = lax.rem(lax.broadcasted_iota(jnp.int32, (chunk, width), 1), HEAD)
    a_ub = jnp.where(row > col, by_base[:chunk], 0.0)
    a_uk = split2(jnp.where(row > col, by_key[:chunk], 0.0))
    a_qb = split2(jnp.where(row >= col, by_base[chunk:], 0.0))
    a_qk = split2(jnp.where(row >= col, by_key[chunk:], 0.0))

    inverse = jnp.where(row == col, 1.0, 0.0).astype(F32)
    size = 1
    while size < chunk:
        joined = ((row // (2 * size)) == (col // (2 * size))) & ((row // size) > (col // size))
        part = jnp.where(joined, a_ub, 0.0)
        if size == 1:
            inverse = inverse - part
        else:
            inv = split2(inverse)
            inverse = inverse - dot3(split2(dot3(inv, blocked(split2(part)), NN)), blocked(inv), NN)
        size *= 2
    inverse = split2(inverse)

    value = v_ref[...]
    (values,) = blocked((value,))
    trans = split2(dot3(inverse, blocked(split2(unit * jnp.exp(before))), NN))
    own = split2(dot3(inverse, blocked(split2(exact(a_uk, values))), NN))
    read = split2(query * jnp.exp(cum) - dot3(a_qb, blocked(trans), NN))
    out_own = exact(a_qk, values) - dot3(a_qb, blocked(own), NN)
    base_last = split2(base * to_last)
    key_last = split2(key * to_last)
    move = jnp.where(big_r == big_c, jnp.exp(last), 0.0) - jnp.where(same, dot3(base_last, trans, TN), 0.0)
    end = dot(key_last[0], value, TN) + dot(key_last[1], value, TN) - dot3(base_last, own, TN)

    zm, ze = split2(zm_ref[...]), split2(ze_ref[...])
    read_ref[...] = dot3(read, zm, NN)
    own_ref[...] = out_own + dot3(read, ze, NN)
    move = split2(move)
    zm_ref[...] = dot3(move, zm, NN)
    ze_ref[...] = dot3(move, ze, NN) + jnp.where(same, end, 0.0)


def layer_kernel(
    chunk, q_ref, k_ref, v_ref, din_ref, doff_ref, extra_ref, rin_ref, roff_ref, gain_ref, resid_ref, fgain_ref, wo_hbm, gate_hbm, up_hbm, down_hbm, out_ref,
    extra_wide, total_ref, read_ref, own_ref, zm_ref, ze_ref, held, mixed, mixrow, wo, mid, tok, gate, up, down, hidden, near_sum, far_sum, y_out, y_in, z_out, z_in,
    wo_sem, w_send, w_recv, c_send, c_recv, a_send, a_recv, t_send, t_recv, y_send, y_recv, z_send, z_recv,
):
    z, x, y, c = (lax.axis_index(name) for name in ("z", "x", "y", "c"))
    half, low = z // 2, lax.rem(z, 2)
    sib = z + 1 - 2 * low
    pair = lax.rem(z + 2, 4)
    near = 1 + half
    mine = c == half
    me = 2 * z + x
    n = 8
    depth = gate_hbm.shape[0]
    width = q_ref.shape[1]
    heads = width // HEAD
    rows = resid_ref.shape[0]
    model = resid_ref.shape[1]
    sources = (gate_hbm, up_hbm, down_hbm)

    def at(index, size):
        return pl.ds(pl.multiple_of(index * size, size), size)

    def remote(src, dst, send, recv, **where):
        return pltpu.make_async_remote_copy(
            src_ref=src, dst_ref=dst, send_sem=send, recv_sem=recv, device_id=where, device_id_type=MESH)

    def piece(m, s):
        return down.at[:, at(s, depth)] if m == 2 else (gate, up)[m].at[at(s, depth), :]

    def to(src, m, s, slot, **where):
        return remote(src, piece(m, s), w_send.at[m, slot], w_recv.at[m, s], **where)

    def landed(m, s):
        to(piece(m, s), m, s, 0, c=1 - c).wait_recv()

    def own(m):
        return pltpu.make_async_copy(sources[m], piece(m, me), w_recv.at[m, me])

    def side_sends(m):
        src = sources[m]
        return ((mine, (to(src, m, me, 1, x=1 - x), to(src, m, me, 2, c=1 - c))),)

    def line_sends(m):
        src = sources[m]
        return (
            (mine, (to(src, m, me, 0, z=sib, c=1 - half),)),
            (jnp.logical_not(mine), (to(src, m, me, 3, z=1 + c, c=low),)),
        )

    first = jnp.where(mine, z, sib)
    second = 2 * (1 - half) + c
    other_first = jnp.where(mine, sib, z)
    other_second = 2 * (1 - half) + 1 - c

    early, late = jnp.where(z == near, second, first), jnp.where(z == near, first, second)
    other_early, other_late = jnp.where(z == near, other_second, other_first), jnp.where(z == near, other_first, other_second)

    def relay(m, step):
        s = 2 * (first, second, *((early, late) if m == 2 else (first, second)))[step] + (x, x, 1 - x, 1 - x)[step]
        p = piece(m, s)
        if step == 0:
            return s, ((jnp.logical_not(mine), (to(p, m, s, 4, x=1 - x), to(p, m, s, 5, c=1 - c))),)
        if step == 1:
            return s, (
                (z == near, (to(p, m, s, 6, z=3 * half),)),
                (None, (to(p, m, s, 7, x=1 - x), to(p, m, s, 8, c=1 - c))),
            )
        return s, ((None, (to(p, m, s, 7 + step, c=1 - c),)),)

    def each(groups, act):
        for when, copies in groups:
            if when is None:
                for copy in copies:
                    act(copy)
            else:
                @pl.when(when)
                def _():
                    for copy in copies:
                        act(copy)

    def start(copy):
        copy.start()

    def begin(m):
        @pl.when(mine)
        def _():
            own(m).start()
        each(side_sends(m), start)

    def pump(m, step):
        s, groups = relay(m, step)
        landed(m, s)
        each(groups, start)

    def pump_far(m):
        s, groups = relay(m, 1)
        landed(m, s)
        each(groups[:1], start)

    def pump_side(m):
        each(relay(m, 1)[1][1:], start)

    def rest_of(m):
        for plane in (other_first, other_second):
            for column in (x, 1 - x):
                landed(m, 2 * plane + column)

    def drain(m):
        for groups in (side_sends(m), line_sends(m), *(relay(m, step)[1] for step in range(4))):
            each(groups, lambda copy: copy.wait_send())

    barrier = pltpu.get_barrier_semaphore()
    for dz in range(4):
        for dx in range(2):
            for dy in range(2):
                for dc in range(2):
                    if dz or dx or dy or dc:
                        peer = {"z": lax.rem(z + dz, 4), "x": lax.rem(x + dx, 2), "y": lax.rem(y + dy, 2), "c": lax.rem(c + dc, 2)}
                        pl.semaphore_signal(barrier, inc=1, device_id=peer, device_id_type=MESH)
    pl.semaphore_wait(barrier, 31)

    load_wo = pltpu.make_async_copy(wo_hbm, wo, wo_sem)
    load_wo.start()

    def place(k):
        peer = lax.rem(me + k, n)
        return {"z": peer // 2, "x": lax.rem(peer, 2)}

    def carry_copy(k):
        return remote(total_ref, held.at[k], c_send.at[k], c_recv.at[k], **place(k))

    leftward = jnp.logical_or(z == 3, jnp.logical_and(c == 0, z >= 1))
    rightward = jnp.logical_not(leftward)
    is_near = z == near
    is_far = jnp.logical_not(is_near)
    is_last = z == 3
    not_mine = jnp.logical_not(mine)
    for m in range(2):
        each(line_sends(m), start)
        begin(m)

    @pl.when(jnp.logical_and(leftward, not_mine))
    def _():
        each(line_sends(2), start)
    tokens = q_ref.shape[0]
    spread_r = lax.broadcasted_iota(jnp.int32, (heads, width), 0)
    spread_c = lax.broadcasted_iota(jnp.int32, (heads, width), 1) // HEAD
    spread = jnp.where(spread_r == spread_c, 1.0, 0.0).astype(F32)
    extra_wide[...] = lax.dot_general(
        extra_ref[...], spread, (TN, ((), ())), precision=lax.Precision.HIGHEST, preferred_element_type=F32)

    big_r = lax.broadcasted_iota(jnp.int32, (width, width), 0)
    big_c = lax.broadcasted_iota(jnp.int32, (width, width), 1)
    blocks = jnp.where((big_r // HEAD) == (big_c // HEAD), 1.0, 0.0).astype(BF16)
    zm_ref[...] = jnp.where(big_r == big_c, 1.0, 0.0).astype(F32)
    ze_ref[...] = jnp.zeros_like(ze_ref)

    def advance(i, _):
        span = at(i, chunk)
        wide_step(
            heads, q_ref.at[span, :], k_ref.at[span, :], v_ref.at[span, :], din_ref.at[span, :], doff_ref,
            extra_wide.at[span, :], rin_ref.at[span, :], roff_ref, read_ref.at[span, :], own_ref.at[span, :], zm_ref, ze_ref)

        @pl.when(jnp.logical_and(i == 2, is_far))
        def _():
            pump(0, 0)

        @pl.when(jnp.logical_and(i == 3, is_near))
        def _():
            pump(0, 0)
            pump_far(0)

        @pl.when(jnp.logical_and(i == 3, jnp.logical_and(is_near, mine)))
        def _():
            pump_side(0)

        @pl.when(jnp.logical_and(i == 3, jnp.logical_and(is_last, mine)))
        def _():
            each(line_sends(2), start)

        @pl.when(jnp.logical_and(i == 4, is_far))
        def _():
            pump(1, 0)

        return 0

    lax.fori_loop(0, tokens // chunk, advance, 0)

    for h in range(heads):
        span = slice(h * HEAD, (h + 1) * HEAD)
        total_ref[span, :] = jnp.concatenate([zm_ref[span, span], ze_ref[span, span]], axis=1).astype(BF16)
    for k in range(1, n):
        @pl.when(me + k < n)
        def _():
            carry_copy(k).start()
    @pl.when(jnp.logical_and(rightward, not_mine))
    def _():
        each(line_sends(2), start)

    @pl.when(jnp.logical_and(rightward, jnp.logical_and(mine, is_far)))
    def _():
        each(line_sends(2), start)

    @pl.when(jnp.logical_and(is_near, not_mine))
    def _():
        pump_side(0)

    @pl.when(is_near)
    def _():
        pump(1, 0)
        pump(1, 1)

    @pl.when(jnp.logical_and(mine, is_near))
    def _():
        each(line_sends(2), start)

    @pl.when(is_far)
    def _():
        begin(2)

    @pl.when(is_last)
    def _():
        pump(0, 1)
    for k in range(1, n):
        @pl.when(me >= k)
        def _():
            carry_copy(k).wait_recv()
    state = [jnp.zeros((HEAD, HEAD), F32) for _ in range(heads)]
    for k in range(n - 1, 0, -1):
        there = k <= me
        for h in range(heads):
            block = held[k, h * HEAD:(h + 1) * HEAD, :].astype(F32)
            new = block[:, HEAD:] + jnp.dot(block[:, :HEAD], state[h], precision=lax.Precision.HIGHEST, preferred_element_type=F32)
            state[h] = jnp.where(there, new, state[h])
    def head_mean(a):
        high, low_part = split2(a)
        return (jnp.dot(high, blocks, preferred_element_type=F32) + jnp.dot(low_part, blocks, preferred_element_type=F32)) / HEAD

    carried = tuple(jnp.concatenate([a] * heads, axis=0) * blocks for a in split2(jnp.concatenate(state, axis=1)))
    o = own_ref[...] + dot3(split2(read_ref[...]), carried, NN)
    center = o - head_mean(o)
    mixed[...] = (center * lax.rsqrt(head_mean(center * center) + 1e-5) * gain_ref[...]).astype(BF16)

    t = 2 * y + c

    def exchange(dy, dc):
        ty, tc = lax.rem(y + dy, 2), lax.rem(c + dc, 2)
        slot = 2 * dy + dc
        return remote(
            mixed.at[at(2 * ty + tc, rows), :], mixrow.at[:, at(t, width)], a_send.at[slot], a_recv.at[slot], y=ty, c=tc)

    swaps = [exchange(1, 0), exchange(1, 1), exchange(0, 1)]
    for copy in swaps:
        copy.start()
    mixrow[:, at(t, width)] = mixed[at(t, rows), :]


    @pl.when(z == 0)
    def _():
        pump(0, 1)
    load_wo.wait()
    for copy in swaps:
        copy.wait()

    tile = 512
    square = jnp.zeros((rows, 1), F32)
    for j in range(0, model, tile):
        proj = jnp.dot(mixrow[...], wo[:, j:j + tile], preferred_element_type=F32)
        part = (resid_ref[:, j:j + tile].astype(F32) + proj).astype(BF16).astype(F32)
        mid[:, j:j + tile] = part
        square += jnp.sum(part * part, axis=-1, keepdims=True)
    g = 2 * half + y
    g_far = 2 * (1 - half) + y
    g_side = 2 * half + 1 - y
    g_diag = 2 * (1 - half) + 1 - y
    tok[at(g, rows), :] = (mid[...] * lax.rsqrt(square / model + 1e-06) * fgain_ref[...]).astype(BF16)

    def rows_to(block, slot, **where):
        r = tok.at[at(block, rows), :]
        return remote(r, r, t_send.at[slot], t_recv.at[slot], **where)

    def rows_from(block, slot):
        r = tok.at[at(block, rows), :]
        remote(r, r, t_send.at[slot], t_recv.at[slot], y=1 - y).wait_recv()

    ahead = rows_to(g, 0, z=pair)
    beside = rows_to(g, 1, y=1 - y)
    onward = rows_to(g_far, 2, y=1 - y)
    ahead.start()
    beside.start()

    @pl.when(is_far)
    def _():
        pump(1, 1)
    pump(0, 2)
    pump(0, 3)

    @pl.when(z == 1)
    def _():
        pump_far(2)
    rows_from(g_far, 0)
    onward.start()
    pump(1, 2)

    @pl.when(is_near)
    def _():
        begin(2)

    @pl.when(z == 1)
    def _():
        pump_side(2)

    @pl.when(z == 2)
    def _():
        pump(2, 1)
    pump(2, 0)

    pump(1, 3)

    rest_of(0)
    rest_of(1)
    rows_from(g_side, 1)
    rows_from(g_diag, 2)

    units = gate.shape[1]
    for j in range(0, units, 256):
        cols = slice(j, min(j + 256, units))
        gated = jnp.dot(tok[...], gate[:, cols], preferred_element_type=F32)
        upper = jnp.dot(tok[...], up[:, cols], preferred_element_type=F32)
        hidden[:, cols] = (gated * jax.nn.sigmoid(gated) * upper).astype(BF16)

    def side_copy(i):
        return remote(y_out.at[i], y_in.at[i], y_send.at[i], y_recv.at[i], y=1 - y)

    def far_copy(i):
        return remote(z_out.at[i], z_in.at[i], z_send.at[i], z_recv.at[i], z=pair)

    def slice_of(plane, column):
        i = 2 * plane + column
        cols = at(i, depth)
        for place_of, dst in ((g_diag, y_out.at[i, 0]), (g_side, y_out.at[i, 1])):
            dst[...] = jnp.dot(hidden[at(place_of, rows), :], down[:, cols], preferred_element_type=F32).astype(BF16)
        far_sum[:, cols] = jnp.dot(hidden[at(g_far, rows), :], down[:, cols], preferred_element_type=F32)
        side_copy(i).start()
        near_sum[:, cols] = jnp.dot(hidden[at(g, rows), :], down[:, cols], preferred_element_type=F32)

    def pass_on(plane, column):
        i = 2 * plane + column
        side_copy(i).wait_recv()
        z_out[i] = (far_sum[:, at(i, depth)] + y_in[i, 0].astype(F32)).astype(BF16)
        far_copy(i).start()

    @pl.when(z == 0)
    def _():
        pump(2, 1)
    slice_of(first, x)
    landed(2, 2 * other_first + x)
    slice_of(other_first, x)

    @pl.when(is_last)
    def _():
        pump(2, 1)
    slice_of(second, x)
    landed(2, 2 * other_second + x)
    slice_of(other_second, x)
    for plane in (first, other_first, second, other_second):
        pass_on(plane, x)
    drain(0)
    drain(1)
    for k in range(1, n):
        @pl.when(me + k < n)
        def _():
            carry_copy(k).wait_send()
    pump(2, 2)
    slice_of(early, 1 - x)
    landed(2, 2 * other_early + 1 - x)
    slice_of(other_early, 1 - x)
    pass_on(early, 1 - x)
    pass_on(other_early, 1 - x)
    pump(2, 3)
    slice_of(late, 1 - x)
    landed(2, 2 * other_late + 1 - x)
    slice_of(other_late, 1 - x)
    pass_on(late, 1 - x)
    pass_on(other_late, 1 - x)
    for i in range(n):
        cols = slice(i * depth, (i + 1) * depth)
        far_copy(i).wait_recv()
        total = near_sum[:, cols] + y_in[i, 1].astype(F32) + z_in[i].astype(F32)
        out_ref[:, cols] = (mid[:, cols] + 0.5 * total).astype(BF16)

    drain(2)
    for copy in (ahead, beside, onward):
        copy.wait_send()
    for i in range(n):
        side_copy(i).wait_send()
        far_copy(i).wait_send()


def layer(q, k, v, din, doff, extra, rin, roff, gain, resid, fgain, wo, gate, up, down):
    tokens, width = q.shape
    heads = width // HEAD
    chunk = 64
    while tokens % chunk:
        chunk //= 2
    rows, model = resid.shape
    depth, units = gate.shape
    n = 8
    vm = pl.BlockSpec(memory_space=pltpu.VMEM)
    hbm = pl.BlockSpec(memory_space=pl.ANY)
    dma = pltpu.SemaphoreType.DMA
    return pl.pallas_call(
        functools.partial(layer_kernel, chunk),
        in_specs=[vm] * 11 + [hbm] * 4,
        out_specs=vm,
        out_shape=jax.ShapeDtypeStruct((rows, model), BF16),
        scratch_shapes=[
            pltpu.VMEM((tokens, width), F32),
            pltpu.VMEM((width, 2 * HEAD), BF16),
            pltpu.VMEM((tokens, width), F32),
            pltpu.VMEM((tokens, width), F32),
            pltpu.VMEM((width, width), F32),
            pltpu.VMEM((width, width), F32),
            pltpu.VMEM((n, width, 2 * HEAD), BF16),
            pltpu.VMEM((tokens, width), BF16),
            pltpu.VMEM((rows, wo.shape[0]), BF16),
            pltpu.VMEM(wo.shape, BF16),
            pltpu.VMEM((rows, model), F32),
            pltpu.VMEM((4 * rows, model), BF16),
            pltpu.VMEM((n * depth, units), BF16),
            pltpu.VMEM((n * depth, units), BF16),
            pltpu.VMEM((units, n * depth), BF16),
            pltpu.VMEM((4 * rows, units), BF16),
            pltpu.VMEM((rows, model), F32),
            pltpu.VMEM((rows, model), F32),
            pltpu.VMEM((n, 2, rows, depth), BF16),
            pltpu.VMEM((n, 2, rows, depth), BF16),
            pltpu.VMEM((n, rows, depth), BF16),
            pltpu.VMEM((n, rows, depth), BF16),
            dma, dma((3, 11)), dma((3, n)), dma((n,)), dma((n,)), dma((4,)), dma((4,)), dma((3,)), dma((3,)),
            dma((n,)), dma((n,)), dma((n,)), dma((n,)),
        ],
        compiler_params=pltpu.CompilerParams(collective_id=2, has_side_effects=True, vmem_limit_bytes=56 * 2**20),
    )(q, k, v, din, doff.reshape(1, width), extra.T, rin, roff.reshape(1, width), gain.reshape(1, width), resid, fgain.reshape(1, model), wo, gate, up, down)


def per_device_pairs(
    resid, queries, keys, values, decay_input_part, decay_channel_offset, decay_head_extra,
    correction_rate_input, correction_rate_offset, head_norm_gain, mixer_output_weight,
    feedforward_norm_gain, gate_weight, up_weight, down_weight,
):
    return layer(
        queries, keys, values, decay_input_part, decay_channel_offset, decay_head_extra,
        correction_rate_input, correction_rate_offset, head_norm_gain, resid, feedforward_norm_gain, mixer_output_weight, gate_weight, up_weight, down_weight)


def solution(mesh):
    n_sp, n_tp = mesh.shape["sp"], mesh.shape["tp"]
    if (n_sp, n_tp) == (8, 4):
        inner = Mesh(mesh.devices.reshape(4, 2, 2, 2), ("z", "x", "y", "c"))
        sp, tp = ("z", "x"), ("y", "c")
        body = per_device_pairs
    else:
        nx = 2 if n_sp % 2 == 0 else 1
        nz = n_sp // nx
        inner = Mesh(mesh.devices.reshape(nz, nx, n_tp), ("z", "x", "tp"))
        sp, tp = ("z", "x"), ("tp",)
        body = functools.partial(per_device, nz, nx)
    rows = P((*sp, *tp), None)
    placed = (
        rows, P(sp, tp), P(sp, tp), P(sp, tp), P(sp, tp), P(tp), P(sp, tp), P(sp, tp), P(tp), P(tp), P(), P(),
        P(sp, tp), P(sp, tp), P(tp, sp),
    )
    return jax.shard_map(body, mesh=inner, in_specs=placed, out_specs=rows, check_vma=False)
```

```python
import functools
import math

import jax
import jax.numpy as jnp
from jax import lax
from jax.experimental import pallas as pl
from jax.experimental.pallas import tpu as pltpu
from jax.sharding import Mesh, PartitionSpec as P

HEAD = 64
F32 = jnp.float32
BF16 = jnp.bfloat16


def split2(a):
    high = a.astype(BF16)
    return high, (a - high.astype(F32)).astype(BF16)


def dot3(a, b, dims):
    (ah, al), (bh, bl) = a, b
    dn = (dims, ((), ()))
    d = functools.partial(lax.dot_general, dimension_numbers=dn, preferred_element_type=F32)
    return d(ah, bh) + (d(ah, bl) + d(al, bh))


NN = ((1,), (0,))
NT = ((1,), (1,))
TN = ((0,), (0,))


def chunk_kernel(heads, chunk, *refs):
    chunk_step(heads, chunk, pl.program_id(0), *refs)


def chunk_step(heads, chunk, step, q_ref, k_ref, v_ref, din_ref, doff_ref, extra_ref, rin_ref, roff_ref, reads_ref, total_ref, z_ref):
    rows = q_ref.shape[0]
    width = heads * HEAD
    wide = heads * chunk

    @pl.when(step == 0)
    def _():
        r = lax.broadcasted_iota(jnp.int32, (width, 2 * HEAD), 0) % HEAD
        c = lax.broadcasted_iota(jnp.int32, (width, 2 * HEAD), 1)
        z_ref[...] = jnp.where(r == c, 1.0, 0.0).astype(F32)

    def load(ref):
        return ref[...].astype(F32)

    def stack(a):
        return jnp.concatenate([a[:, h * HEAD:(h + 1) * HEAD] for h in range(heads)], axis=0)

    spread_r = lax.broadcasted_iota(jnp.int32, (heads, width), 0)
    spread_c = lax.broadcasted_iota(jnp.int32, (heads, width), 1) // HEAD
    spread = jnp.where(spread_r == spread_c, 1.0, 0.0).astype(F32)
    extra = extra_ref[...]
    if extra.shape[1] == heads:
        extra = lax.dot_general(extra, spread, ((((1,), (0,))), ((), ())), precision=lax.Precision.HIGHEST, preferred_element_type=F32)
    log_decay = -jax.nn.sigmoid(load(din_ref) + doff_ref[...]) * math.exp(-0.5) - extra
    tr = lax.broadcasted_iota(jnp.int32, (chunk, chunk), 0)
    tc = lax.broadcasted_iota(jnp.int32, (chunk, chunk), 1)
    lower = jnp.where(tr >= tc, 1.0, 0.0).astype(F32)
    cum = lax.dot_general(lower, log_decay, (((1,), (0,)), ((), ())), precision=lax.Precision.HIGHEST, preferred_element_type=F32)
    last = cum[chunk - 1:chunk, :]
    mid = cum[chunk // 2 - 1:chunk // 2, :]
    before = cum - log_decay
    rate = jax.nn.sigmoid(load(rin_ref) + roff_ref[...])

    key = stack(load(k_ref))
    unit = key * lax.rsqrt(jnp.sum(key * key, axis=-1, keepdims=True) + 1e-6)
    base = unit * stack(rate)
    query = stack(load(q_ref))
    value = split2(stack(load(v_ref)))
    to_mid = stack(jnp.exp(mid - cum))
    key_mid = split2(key * to_mid)
    base_mid = split2(base * to_mid)
    query_mid = split2(query * stack(jnp.exp(cum - mid)))
    unit_mid = split2(unit * stack(jnp.exp(before - mid)))
    to_last = stack(jnp.exp(last - cum))

    row = lax.broadcasted_iota(jnp.int32, (wide, wide), 0)
    col = lax.broadcasted_iota(jnp.int32, (wide, wide), 1)
    same = (row // chunk) == (col // chunk)
    strict = same & (row > col)
    upto = same & (row >= col)
    a_ub = jnp.where(strict, dot3(unit_mid, base_mid, NT), 0.0)
    a_uk = jnp.where(strict, dot3(unit_mid, key_mid, NT), 0.0)
    a_qb = jnp.where(upto, dot3(query_mid, base_mid, NT), 0.0)
    a_qk = jnp.where(upto, dot3(query_mid, key_mid, NT), 0.0)

    inverse = jnp.where(row == col, 1.0, 0.0).astype(F32)
    size = 1
    while size < chunk:
        pair = ((row // (2 * size)) == (col // (2 * size))) & ((row // size) > (col // size))
        part = jnp.where(pair, a_ub, 0.0)
        if size == 1:
            inverse = inverse - part
        else:
            inv = split2(inverse)
            inverse = inverse - dot3(split2(dot3(inv, split2(part), NN)), inv, NN)
        size *= 2
    inverse = split2(inverse)

    wr = lax.broadcasted_iota(jnp.int32, (wide, width), 0) // chunk
    wc = lax.broadcasted_iota(jnp.int32, (wide, width), 1) // HEAD

    def spread_wide(a):
        return jnp.where(wr == wc, jnp.concatenate([a] * heads, axis=1), 0.0)

    unit_wide = split2(spread_wide(unit * stack(jnp.exp(before))))
    query_wide = spread_wide(query * stack(jnp.exp(cum)))
    base_wide = split2(spread_wide(base * to_last))
    key_wide = split2(spread_wide(key * to_last))
    qb = split2(a_qb)
    trans = split2(dot3(inverse, unit_wide, NN))
    own = split2(dot3(inverse, split2(dot3(split2(a_uk), value, NN)), NN))
    read = split2(query_wide - dot3(qb, trans, NN))
    out_own = dot3(split2(a_qk), value, NN) - dot3(qb, own, NN)
    pr = lax.broadcasted_iota(jnp.int32, (width, width), 0)
    pc = lax.broadcasted_iota(jnp.int32, (width, width), 1)
    move = jnp.where(pr == pc, jnp.exp(last), 0.0) - dot3(base_wide, trans, TN)
    end = dot3(key_wide, value, TN) - dot3(base_wide, own, TN)

    z = split2(z_ref[...])
    x = dot3(read, z, NN) + jnp.concatenate([jnp.zeros_like(out_own), out_own], axis=1)
    for h in range(heads):
        reads_ref[h] = x[h * chunk:(h + 1) * chunk, :]
    z_new = dot3(split2(move), z, NN) + jnp.concatenate([jnp.zeros_like(end), end], axis=1)
    z_ref[...] = z_new
    total_ref[...] = z_new.astype(BF16)


def chunks(q, k, v, din, doff, extra, rin, roff):
    rows, width = q.shape
    heads = width // HEAD
    chunk = 64
    while rows % chunk:
        chunk //= 2
    tile = pl.BlockSpec((chunk, width), lambda i: (i, 0))
    vec = pl.BlockSpec((1, width), lambda i: (0, 0))
    n = rows // chunk
    return pl.pallas_call(
        functools.partial(chunk_kernel, heads, chunk),
        grid=(n,),
        in_specs=[tile, tile, tile, tile, vec, pl.BlockSpec((chunk, heads), lambda i: (i, 0)), tile, vec],
        out_specs=(
            pl.BlockSpec((heads, chunk, 2 * HEAD), lambda i: (0, i, 0)),
            pl.BlockSpec((width, 2 * HEAD), lambda i: (0, 0)),
        ),
        out_shape=(
            jax.ShapeDtypeStruct((heads, rows, 2 * HEAD), F32),
            jax.ShapeDtypeStruct((width, 2 * HEAD), BF16),
        ),
        scratch_shapes=[pltpu.VMEM((width, 2 * HEAD), F32)],
        compiler_params=pltpu.CompilerParams(dimension_semantics=("arbitrary",), vmem_limit_bytes=40 * 2**20),
    )(q, k, v, din, doff.reshape(1, width), extra, rin, roff.reshape(1, width))


def carry_kernel(nz, nx, total_ref, reads_ref, gain_ref, mixed_ref, held, send_sem, recv_sem):
    n = nz * nx
    me = lax.axis_index("z") * nx + lax.axis_index("x")
    heads = reads_ref.shape[0]

    def place(k):
        peer = lax.rem(me + k, n)
        return {"z": peer // nx, "x": lax.rem(peer, nx)}

    barrier = pltpu.get_barrier_semaphore()
    for k in range(1, n):
        pl.semaphore_signal(barrier, inc=1, device_id=place(k), device_id_type=pl.DeviceIdType.MESH)
    pl.semaphore_wait(barrier, n - 1)
    copies = []
    for k in range(1, n):
        c = pltpu.make_async_remote_copy(
            src_ref=total_ref, dst_ref=held.at[k], send_sem=send_sem.at[k], recv_sem=recv_sem.at[k],
            device_id=place(k), device_id_type=pl.DeviceIdType.MESH)
        c.start()
        copies.append(c)
    for c in copies:
        c.wait()
    state = [jnp.zeros((HEAD, HEAD), F32) for _ in range(heads)]
    for k in range(n - 1, 0, -1):
        there = k <= me
        for h in range(heads):
            block = held[k, h * HEAD:(h + 1) * HEAD, :].astype(F32)
            new = block[:, HEAD:] + jnp.dot(block[:, :HEAD], state[h], precision=lax.Precision.HIGHEST, preferred_element_type=F32)
            state[h] = jnp.where(there, new, state[h])
    outs = []
    for h in range(heads):
        x = reads_ref[h]
        o = x[:, HEAD:] + dot3(split2(x[:, :HEAD]), split2(state[h]), NN)
        center = o - jnp.mean(o, axis=-1, keepdims=True)
        var = jnp.mean(center * center, axis=-1, keepdims=True)
        outs.append(center * lax.rsqrt(var + 1e-5))
    mixed_ref[...] = (jnp.concatenate(outs, axis=1) * gain_ref[...]).astype(BF16)


def carry(total, reads, gain, nz, nx):
    heads, rows, _ = reads.shape
    width = heads * HEAD
    n = nz * nx
    vm = pl.BlockSpec(memory_space=pltpu.VMEM)
    return pl.pallas_call(
        functools.partial(carry_kernel, nz, nx),
        in_specs=[vm, vm, vm],
        out_specs=vm,
        out_shape=jax.ShapeDtypeStruct((rows, width), BF16),
        scratch_shapes=[
            pltpu.VMEM((n, width, 2 * HEAD), BF16),
            pltpu.SemaphoreType.DMA((n,)),
            pltpu.SemaphoreType.DMA((n,)),
        ],
        compiler_params=pltpu.CompilerParams(collective_id=1, has_side_effects=True, vmem_limit_bytes=24 * 2**20),
    )(total, reads, gain.reshape(1, width))


def send_z(block, nz):
    return [lax.ppermute(block, "z", [(s, (s + k) % nz) for s in range(nz)]) for k in range(1, nz)]


def in_order(block, came, nz, axis):
    z = lax.axis_index("z")
    size = block.shape[axis]
    shape = list(block.shape)
    shape[axis] = size * nz
    whole = jnp.zeros(shape, block.dtype)
    whole = lax.dynamic_update_slice_in_dim(whole, block, z * size, axis)
    for k in range(1, nz):
        whole = lax.dynamic_update_slice_in_dim(whole, came[k - 1], lax.rem(z - k + nz, nz) * size, axis)
    return whole


def per_device(
    nz, nx,
    resid, queries, keys, values, decay_input_part, decay_channel_offset, decay_head_extra,
    correction_rate_input, correction_rate_offset, head_norm_gain, mixer_output_weight,
    feedforward_norm_gain, gate_weight, up_weight, down_weight,
):
    ff = gate_weight.shape[1] // nx
    x = lax.axis_index("x")

    def exchange(weight, axis, join):
        pieces = weight.reshape(weight.shape[:axis] + (nx, ff) + weight.shape[axis + 1:])
        return lax.all_to_all(pieces, "x", split_axis=axis, concat_axis=join, tiled=False)

    def swap(weight, axis, join):
        if nx == 1:
            return weight
        if nx != 2:
            out = exchange(weight, axis, join)
            return out.reshape((-1, ff) if axis == 1 else (ff, -1))
        mine = lax.dynamic_slice_in_dim(weight, x * ff, ff, axis)
        other = lax.dynamic_slice_in_dim(weight, (1 - x) * ff, ff, axis)
        came = lax.ppermute(other, "x", [(0, 1), (1, 0)])
        first = jnp.where(x == 0, mine, came)
        second = jnp.where(x == 0, came, mine)
        return jnp.concatenate([first, second], axis=join)

    halves = (swap(gate_weight, 1, 0), swap(up_weight, 1, 0), swap(down_weight, 0, 1))
    halves, queries = lax.optimization_barrier((halves, queries))
    whole_gate = lax.all_gather(halves[0], "z", axis=0, tiled=True)
    up_came = send_z(halves[1], nz)
    down_came = send_z(halves[2], nz)

    reads, total = chunks(
        queries, keys, values, decay_input_part, decay_channel_offset, decay_head_extra,
        correction_rate_input, correction_rate_offset)
    total, up_came = lax.optimization_barrier((total, up_came))
    mixed = carry(total, reads, head_norm_gain, nz, nx)
    row_mixed = lax.all_to_all(mixed, "tp", split_axis=0, concat_axis=1, tiled=True)
    proj = jnp.dot(row_mixed, mixer_output_weight, preferred_element_type=F32)
    mid_f = (resid.astype(F32) + proj).astype(BF16).astype(F32)
    normed = (
        mid_f
        * lax.rsqrt(jnp.mean(mid_f * mid_f, axis=-1, keepdims=True) + 1e-06)
        * feedforward_norm_gain
    ).astype(BF16)
    normed, whole_gate = lax.optimization_barrier((normed, whole_gate))
    whole_up = in_order(halves[1], up_came, nz, 0)
    whole_down = in_order(halves[2], down_came, nz, 1)
    whole_rows = lax.all_gather(normed, ("x", "tp"), axis=0, tiled=True)
    gate = jnp.dot(whole_rows, whole_gate, preferred_element_type=F32)
    upper = jnp.dot(whole_rows, whole_up, preferred_element_type=F32)
    hidden = (jax.nn.silu(gate) * upper).astype(BF16)
    down_sum = lax.psum_scatter(
        jnp.dot(hidden, whole_down, preferred_element_type=F32).astype(BF16),
        ("x", "tp"), scatter_dimension=0, tiled=True,
    ).astype(F32)
    return (mid_f + 0.5 * down_sum).astype(BF16)


MESH = pl.DeviceIdType.MESH


def wide_step(heads, q_ref, k_ref, v_ref, din_ref, doff_ref, extra_ref, rin_ref, roff_ref, read_ref, own_ref, zm_ref, ze_ref):
    chunk = q_ref.shape[0]
    width = heads * HEAD

    def load(ref):
        return ref[...].astype(F32)

    def dot(a, b, dims=NN):
        return lax.dot_general(a, b, (dims, ((), ())), preferred_element_type=F32)

    big_r = lax.broadcasted_iota(jnp.int32, (width, width), 0)
    big_c = lax.broadcasted_iota(jnp.int32, (width, width), 1)
    same = (big_r // HEAD) == (big_c // HEAD)
    blocks = jnp.where(same, 1.0, 0.0).astype(BF16)

    def blocked(pair):
        return tuple(jnp.concatenate([a] * heads, axis=0) * blocks for a in pair)

    def exact(pair, b):
        return dot(pair[0], b) + dot(pair[1], b)

    key = load(k_ref)
    unit = key * lax.rsqrt(exact(split2(key * key), blocks) + 1e-6)
    base = unit * jax.nn.sigmoid(load(rin_ref) + roff_ref[...])
    query = load(q_ref)
    log_decay = -jax.nn.sigmoid(load(din_ref) + doff_ref[...]) * math.exp(-0.5) - extra_ref[...]
    tr = lax.broadcasted_iota(jnp.int32, (chunk, chunk), 0)
    tc = lax.broadcasted_iota(jnp.int32, (chunk, chunk), 1)
    lower = jnp.where(tr >= tc, 1.0, 0.0).astype(BF16)
    ld_high, ld_rest = split2(log_decay)
    ld_mid, ld_low = split2(log_decay - ld_high.astype(F32))
    cum = dot(lower, ld_high) + (dot(lower, ld_mid) + dot(lower, ld_low))
    last = cum[chunk - 1:chunk, :]
    mid = cum[chunk // 2 - 1:chunk // 2, :]
    before = cum - log_decay
    to_mid = jnp.exp(mid - cum)
    to_last = jnp.exp(last - cum)
    key_mid = blocked(split2(key * to_mid))
    base_mid = blocked(split2(base * to_mid))
    left = split2(jnp.concatenate([unit * jnp.exp(before - mid), query * jnp.exp(cum - mid)], axis=0))
    by_base = dot3(left, base_mid, NT)
    by_key = dot3(left, key_mid, NT)
    row = lax.broadcasted_iota(jnp.int32, (chunk, width), 0)
    col = lax.rem(lax.broadcasted_iota(jnp.int32, (chunk, width), 1), HEAD)
    a_ub = jnp.where(row > col, by_base[:chunk], 0.0)
    a_uk = split2(jnp.where(row > col, by_key[:chunk], 0.0))
    a_qb = split2(jnp.where(row >= col, by_base[chunk:], 0.0))
    a_qk = split2(jnp.where(row >= col, by_key[chunk:], 0.0))

    inverse = jnp.where(row == col, 1.0, 0.0).astype(F32)
    size = 1
    while size < chunk:
        joined = ((row // (2 * size)) == (col // (2 * size))) & ((row // size) > (col // size))
        part = jnp.where(joined, a_ub, 0.0)
        if size == 1:
            inverse = inverse - part
        else:
            inv = split2(inverse)
            inverse = inverse - dot3(split2(dot3(inv, blocked(split2(part)), NN)), blocked(inv), NN)
        size *= 2
    inverse = split2(inverse)

    value = v_ref[...]
    (values,) = blocked((value,))
    trans = split2(dot3(inverse, blocked(split2(unit * jnp.exp(before))), NN))
    own = split2(dot3(inverse, blocked(split2(exact(a_uk, values))), NN))
    read = split2(query * jnp.exp(cum) - dot3(a_qb, blocked(trans), NN))
    out_own = exact(a_qk, values) - dot3(a_qb, blocked(own), NN)
    base_last = split2(base * to_last)
    key_last = split2(key * to_last)
    move = jnp.where(big_r == big_c, jnp.exp(last), 0.0) - jnp.where(same, dot3(base_last, trans, TN), 0.0)
    end = dot(key_last[0], value, TN) + dot(key_last[1], value, TN) - dot3(base_last, own, TN)

    zm, ze = split2(zm_ref[...]), split2(ze_ref[...])
    read_ref[...] = dot3(read, zm, NN)
    own_ref[...] = out_own + dot3(read, ze, NN)
    move = split2(move)
    zm_ref[...] = dot3(move, zm, NN)
    ze_ref[...] = dot3(move, ze, NN) + jnp.where(same, end, 0.0)


def layer_kernel(
    chunk, q_hbm, k_hbm, v_hbm, din_hbm, doff_hbm, extra_hbm, rin_hbm,
    roff_hbm, gain_hbm, resid_hbm, fgain_hbm, wo_hbm, gate_hbm, up_hbm, down_hbm, out_ref,
    q_ref, k_ref, v_ref, din_ref, doff_ref, extra_ref, rin_ref, roff_ref, gain_ref, resid_ref, fgain_ref,
    extra_wide, total_ref, read_ref, own_ref, zm_ref, ze_ref, held, mixed, mixrow, wo, mid, tok, gate, up, down, hidden, near_sum, far_sum, y_out, y_in, z_out, z_in,
    in_sem, wo_sem, w_send, w_recv, c_send, c_recv, a_send, a_recv, t_send, t_recv, y_send, y_recv, z_send, z_recv,
):
    whole = (q_hbm, k_hbm, v_hbm, din_hbm, doff_hbm, extra_hbm, rin_hbm, roff_hbm, gain_hbm, resid_hbm, fgain_hbm)
    local = (q_ref, k_ref, v_ref, din_ref, doff_ref, extra_ref, rin_ref, roff_ref, gain_ref, resid_ref, fgain_ref)
    loads = [pltpu.make_async_copy(src, dst, in_sem.at[i]) for i, (src, dst) in enumerate(zip(whole, local))]
    for load in loads:
        load.start()
    z, x, y, c = (lax.axis_index(name) for name in ("z", "x", "y", "c"))
    half, low = z // 2, lax.rem(z, 2)
    sib = z + 1 - 2 * low
    pair = lax.rem(z + 2, 4)
    near = 1 + half
    mine = c == half
    me = 2 * z + x
    n = 8
    depth = gate_hbm.shape[0]
    width = q_ref.shape[1]
    heads = width // HEAD
    rows = resid_ref.shape[0]
    model = resid_ref.shape[1]
    cut = down_hbm.shape[0] // 2
    sources = (gate_hbm, up_hbm, down_hbm.at[pl.ds(0, cut), :], down_hbm.at[pl.ds(cut, cut), :])

    def at(index, size):
        return pl.ds(pl.multiple_of(index * size, size), size)

    def remote(src, dst, send, recv, **where):
        return pltpu.make_async_remote_copy(
            src_ref=src, dst_ref=dst, send_sem=send, recv_sem=recv, device_id=where, device_id_type=MESH)

    def piece(m, s):
        if m < 2:
            return (gate, up)[m].at[at(s, depth), :]
        return down.at[pl.ds((m - 2) * cut, cut), at(s, depth)]

    def to(src, m, s, slot, **where):
        return remote(src, piece(m, s), w_send.at[m, slot], w_recv.at[m, s], **where)

    def landed(m, s):
        to(piece(m, s), m, s, 0, c=1 - c).wait_recv()

    def down_landed(s):
        landed(2, s)
        landed(3, s)

    def own(m):
        return pltpu.make_async_copy(sources[m], piece(m, me), w_recv.at[m, me])

    def side_sends(m):
        src = sources[m]
        return ((mine, (to(src, m, me, 1, x=1 - x), to(src, m, me, 2, c=1 - c))),)

    def line_sends(m):
        src = sources[m]
        return (
            (mine, (to(src, m, me, 0, z=sib, c=1 - half),)),
            (jnp.logical_not(mine), (to(src, m, me, 3, z=1 + c, c=low),)),
        )

    first = jnp.where(mine, z, sib)
    second = 2 * (1 - half) + c
    other_first = jnp.where(mine, sib, z)
    other_second = 2 * (1 - half) + 1 - c

    swapped = jnp.logical_and(z == near, c != half)
    early, late = jnp.where(swapped, second, first), jnp.where(swapped, first, second)
    other_swapped = jnp.logical_and(z == near, mine)
    other_early, other_late = jnp.where(other_swapped, other_second, other_first), jnp.where(other_swapped, other_first, other_second)

    def relay(m, step):
        s = 2 * (first, second, *((early, late) if m >= 2 else (first, second)))[step] + (x, x, 1 - x, 1 - x)[step]
        p = piece(m, s)
        if step == 0:
            return s, ((jnp.logical_not(mine), (to(p, m, s, 4, x=1 - x), to(p, m, s, 5, c=1 - c))),)
        if step == 1:
            return s, (
                (z == near, (to(p, m, s, 6, z=3 * half),)),
                (None, (to(p, m, s, 7, x=1 - x), to(p, m, s, 8, c=1 - c))),
            )
        return s, ((None, (to(p, m, s, 7 + step, c=1 - c),)),)

    def each(groups, act):
        for when, copies in groups:
            if when is None:
                for copy in copies:
                    act(copy)
            else:
                @pl.when(when)
                def _():
                    for copy in copies:
                        act(copy)

    def start(copy):
        copy.start()

    def begin(m):
        @pl.when(mine)
        def _():
            own(m).start()
        each(side_sends(m), start)

    def pump(m, step):
        s, groups = relay(m, step)
        landed(m, s)
        each(groups, start)

    def pump_far(m):
        s, groups = relay(m, 1)
        landed(m, s)
        each(groups[:1], start)

    def pump_side(m):
        each(relay(m, 1)[1][1:], start)

    def rest_of(m):
        for plane in (other_first, other_second):
            for column in (x, 1 - x):
                landed(m, 2 * plane + column)

    def drain(m):
        for groups in (side_sends(m), line_sends(m), *(relay(m, step)[1] for step in range(4))):
            each(groups, lambda copy: copy.wait_send())

    barrier = pltpu.get_barrier_semaphore()
    for dz in range(4):
        for dx in range(2):
            for dy in range(2):
                for dc in range(2):
                    if dz or dx or dy or dc:
                        peer = {"z": lax.rem(z + dz, 4), "x": lax.rem(x + dx, 2), "y": lax.rem(y + dy, 2), "c": lax.rem(c + dc, 2)}
                        pl.semaphore_signal(barrier, inc=1, device_id=peer, device_id_type=MESH)
    pl.semaphore_wait(barrier, 31)

    load_wo = pltpu.make_async_copy(wo_hbm, wo, wo_sem)
    load_wo.start()

    def place(k):
        peer = lax.rem(me + k, n)
        return {"z": peer // 2, "x": lax.rem(peer, 2)}

    def carry_copy(k):
        return remote(total_ref, held.at[k], c_send.at[k], c_recv.at[k], **place(k))

    leftward = jnp.logical_or(z == 3, jnp.logical_and(c == 0, z >= 1))
    rightward = jnp.logical_not(leftward)
    is_near = z == near
    is_far = jnp.logical_not(is_near)
    is_last = z == 3
    not_mine = jnp.logical_not(mine)
    for m in range(2):
        each(line_sends(m), start)
        begin(m)

    @pl.when(jnp.logical_and(leftward, not_mine))
    def _():
        each(line_sends(2), start)
        each(line_sends(3), start)
    tokens = q_ref.shape[0]
    for load in loads:
        load.wait()
    spread_r = lax.broadcasted_iota(jnp.int32, (heads, width), 0)
    spread_c = lax.broadcasted_iota(jnp.int32, (heads, width), 1) // HEAD
    spread = jnp.where(spread_r == spread_c, 1.0, 0.0).astype(F32)
    extra_wide[...] = lax.dot_general(
        extra_ref[...], spread, (TN, ((), ())), precision=lax.Precision.HIGHEST, preferred_element_type=F32)

    big_r = lax.broadcasted_iota(jnp.int32, (width, width), 0)
    big_c = lax.broadcasted_iota(jnp.int32, (width, width), 1)
    blocks = jnp.where((big_r // HEAD) == (big_c // HEAD), 1.0, 0.0).astype(BF16)
    zm_ref[...] = jnp.where(big_r == big_c, 1.0, 0.0).astype(F32)
    ze_ref[...] = jnp.zeros_like(ze_ref)

    def advance(i, _):
        span = at(i, chunk)
        wide_step(
            heads, q_ref.at[span, :], k_ref.at[span, :], v_ref.at[span, :], din_ref.at[span, :], doff_ref,
            extra_wide.at[span, :], rin_ref.at[span, :], roff_ref, read_ref.at[span, :], own_ref.at[span, :], zm_ref, ze_ref)

        @pl.when(jnp.logical_and(i == 2, is_far))
        def _():
            pump(0, 0)

        @pl.when(jnp.logical_and(i == 3, is_near))
        def _():
            pump(0, 0)
            pump_far(0)

        @pl.when(jnp.logical_and(i == 3, jnp.logical_and(is_near, mine)))
        def _():
            pump_side(0)

        @pl.when(jnp.logical_and(i == 3, jnp.logical_and(is_last, mine)))
        def _():
            each(line_sends(2), start)
            each(line_sends(3), start)

        @pl.when(jnp.logical_and(i == 4, is_far))
        def _():
            pump(1, 0)

        return 0

    lax.fori_loop(0, tokens // chunk, advance, 0)

    for h in range(heads):
        span = slice(h * HEAD, (h + 1) * HEAD)
        total_ref[span, :] = jnp.concatenate([zm_ref[span, span], ze_ref[span, span]], axis=1).astype(BF16)
    for k in range(1, n):
        @pl.when(me + k < n)
        def _():
            carry_copy(k).start()
    @pl.when(jnp.logical_and(rightward, not_mine))
    def _():
        each(line_sends(2), start)
        each(line_sends(3), start)

    @pl.when(jnp.logical_and(rightward, jnp.logical_and(mine, is_far)))
    def _():
        each(line_sends(2), start)
        each(line_sends(3), start)

    @pl.when(jnp.logical_and(is_near, not_mine))
    def _():
        pump_side(0)

    @pl.when(is_near)
    def _():
        pump(1, 0)
        pump(1, 1)

    @pl.when(jnp.logical_and(mine, is_near))
    def _():
        each(line_sends(2), start)
        each(line_sends(3), start)

    @pl.when(is_far)
    def _():
        begin(2)
        begin(3)

    @pl.when(is_last)
    def _():
        pump(0, 1)
    for k in range(1, n):
        @pl.when(me >= k)
        def _():
            carry_copy(k).wait_recv()
    state = [jnp.zeros((HEAD, HEAD), F32) for _ in range(heads)]
    for k in range(n - 1, 0, -1):
        there = k <= me
        for h in range(heads):
            block = held[k, h * HEAD:(h + 1) * HEAD, :].astype(F32)
            new = block[:, HEAD:] + jnp.dot(block[:, :HEAD], state[h], precision=lax.Precision.HIGHEST, preferred_element_type=F32)
            state[h] = jnp.where(there, new, state[h])
    def head_mean(a):
        high, low_part = split2(a)
        return (jnp.dot(high, blocks, preferred_element_type=F32) + jnp.dot(low_part, blocks, preferred_element_type=F32)) / HEAD

    carried = tuple(jnp.concatenate([a] * heads, axis=0) * blocks for a in split2(jnp.concatenate(state, axis=1)))
    o = own_ref[...] + dot3(split2(read_ref[...]), carried, NN)
    center = o - head_mean(o)
    mixed[...] = (center * lax.rsqrt(head_mean(center * center) + 1e-5) * gain_ref[...]).astype(BF16)

    t = 2 * y + c

    def exchange(dy, dc):
        ty, tc = lax.rem(y + dy, 2), lax.rem(c + dc, 2)
        slot = 2 * dy + dc
        return remote(
            mixed.at[at(2 * ty + tc, rows), :], mixrow.at[:, at(t, width)], a_send.at[slot], a_recv.at[slot], y=ty, c=tc)

    swaps = [exchange(1, 0), exchange(1, 1), exchange(0, 1)]
    for copy in swaps:
        copy.start()
    mixrow[:, at(t, width)] = mixed[at(t, rows), :]


    @pl.when(z == 0)
    def _():
        pump(0, 1)
    load_wo.wait()
    for copy in swaps:
        copy.wait()

    tile = 512
    square = jnp.zeros((rows, 1), F32)
    for j in range(0, model, tile):
        proj = jnp.dot(mixrow[...], wo[:, j:j + tile], preferred_element_type=F32)
        part = (resid_ref[:, j:j + tile].astype(F32) + proj).astype(BF16).astype(F32)
        mid[:, j:j + tile] = part
        square += jnp.sum(part * part, axis=-1, keepdims=True)
    g = 2 * half + y
    g_far = 2 * (1 - half) + y
    g_side = 2 * half + 1 - y
    g_diag = 2 * (1 - half) + 1 - y
    tok[at(g, rows), :] = (mid[...] * lax.rsqrt(square / model + 1e-06) * fgain_ref[...]).astype(BF16)

    def rows_to(block, slot, **where):
        r = tok.at[at(block, rows), :]
        return remote(r, r, t_send.at[slot], t_recv.at[slot], **where)

    def rows_from(block, slot):
        r = tok.at[at(block, rows), :]
        remote(r, r, t_send.at[slot], t_recv.at[slot], y=1 - y).wait_recv()

    ahead = rows_to(g, 0, z=pair)
    beside = rows_to(g, 1, y=1 - y)
    onward = rows_to(g_far, 2, y=1 - y)
    beside.start()

    @pl.when(is_far)
    def _():
        ahead.start()

    @pl.when(is_far)
    def _():
        pump(1, 1)
    pump(0, 2)
    pump(0, 3)

    @pl.when(z == 1)
    def _():
        pump_far(2)
        pump_far(3)

    @pl.when(is_near)
    def _():
        ahead.start()
    rows_from(g_far, 0)
    onward.start()
    pump(1, 2)

    @pl.when(is_near)
    def _():
        begin(2)
        begin(3)

    @pl.when(z == 1)
    def _():
        pump_side(2)
        pump_side(3)

    @pl.when(z == 2)
    def _():
        pump(2, 1)
        pump(3, 1)

    @pl.when(is_near)
    def _():
        pump(2, 0)
        pump(3, 0)

    pump(1, 3)

    @pl.when(is_far)
    def _():
        pump(2, 0)
        pump(3, 0)

    rest_of(0)
    rest_of(1)
    rows_from(g_side, 1)
    rows_from(g_diag, 2)

    units = gate.shape[1]
    for j in range(0, units, 256):
        cols = slice(j, min(j + 256, units))
        gated = jnp.dot(tok[...], gate[:, cols], preferred_element_type=F32)
        upper = jnp.dot(tok[...], up[:, cols], preferred_element_type=F32)
        hidden[:, cols] = (gated * jax.nn.sigmoid(gated) * upper).astype(BF16)

    def side_copy(i):
        return remote(y_out.at[i], y_in.at[i], y_send.at[i], y_recv.at[i], y=1 - y)

    def far_copy(i):
        return remote(z_out.at[i], z_in.at[i], z_send.at[i], z_recv.at[i], z=pair)

    def slice_of(plane, column):
        i = 2 * plane + column
        cols = at(i, depth)
        for place_of, dst in ((g_diag, y_out.at[i, 0]), (g_side, y_out.at[i, 1])):
            dst[...] = jnp.dot(hidden[at(place_of, rows), :], down[:, cols], preferred_element_type=F32).astype(BF16)
        far_sum[:, cols] = jnp.dot(hidden[at(g_far, rows), :], down[:, cols], preferred_element_type=F32)
        side_copy(i).start()
        near_sum[:, cols] = jnp.dot(hidden[at(g, rows), :], down[:, cols], preferred_element_type=F32)

    def pass_on(plane, column):
        i = 2 * plane + column
        side_copy(i).wait_recv()
        z_out[i] = (far_sum[:, at(i, depth)] + y_in[i, 0].astype(F32)).astype(BF16)
        far_copy(i).start()

    next_first, next_other = jnp.where(is_far, first, second), jnp.where(is_far, other_first, other_second)
    next_column = jnp.where(is_far, 1 - x, x)
    then_first, then_other = jnp.where(is_far, second, early), jnp.where(is_far, other_second, other_early)
    then_column = jnp.where(is_far, x, 1 - x)

    @pl.when(is_far)
    def _():
        pump(2, 1)
    slice_of(first, x)
    down_landed(2 * other_first + x)
    slice_of(other_first, x)

    @pl.when(is_far)
    def _():
        pump(2, 2)
        pump(3, 2)

    @pl.when(z == 0)
    def _():
        pump(3, 1)
    slice_of(next_first, next_column)
    down_landed(2 * next_other + next_column)
    slice_of(next_other, next_column)
    pass_on(first, x)
    pass_on(other_first, x)

    @pl.when(is_last)
    def _():
        pump(3, 1)
    drain(0)
    drain(1)
    for k in range(1, n):
        @pl.when(me + k < n)
        def _():
            carry_copy(k).wait_send()

    @pl.when(is_near)
    def _():
        pump(2, 2)
        pump(3, 2)
    slice_of(then_first, then_column)
    down_landed(2 * then_other + then_column)
    slice_of(then_other, then_column)
    pass_on(next_first, next_column)
    pass_on(next_other, next_column)
    pass_on(then_first, then_column)
    pass_on(then_other, then_column)
    pump(2, 3)
    pump(3, 3)
    slice_of(late, 1 - x)
    down_landed(2 * other_late + 1 - x)
    slice_of(other_late, 1 - x)
    pass_on(late, 1 - x)
    pass_on(other_late, 1 - x)
    for i in range(n):
        cols = slice(i * depth, (i + 1) * depth)
        far_copy(i).wait_recv()
        total = near_sum[:, cols] + y_in[i, 1].astype(F32) + z_in[i].astype(F32)
        out_ref[:, cols] = (mid[:, cols] + 0.5 * total).astype(BF16)

    drain(2)
    drain(3)
    for copy in (ahead, beside, onward):
        copy.wait_send()
    for i in range(n):
        side_copy(i).wait_send()
        far_copy(i).wait_send()


def layer(q, k, v, din, doff, extra, rin, roff, gain, resid, fgain, wo, gate, up, down):
    tokens, width = q.shape
    heads = width // HEAD
    chunk = 64
    while tokens % chunk:
        chunk //= 2
    rows, model = resid.shape
    depth, units = gate.shape
    n = 8
    vm = pl.BlockSpec(memory_space=pltpu.VMEM)
    hbm = pl.BlockSpec(memory_space=pl.ANY)
    dma = pltpu.SemaphoreType.DMA
    inputs = (
        q, k, v, din, doff.reshape(1, width), extra.T, rin, roff.reshape(1, width), gain.reshape(1, width), resid, fgain.reshape(1, model))
    return pl.pallas_call(
        functools.partial(layer_kernel, chunk),
        in_specs=[hbm] * 15,
        out_specs=vm,
        out_shape=jax.ShapeDtypeStruct((rows, model), BF16),
        scratch_shapes=[pltpu.VMEM(a.shape, a.dtype) for a in inputs] + [
            pltpu.VMEM((tokens, width), F32),
            pltpu.VMEM((width, 2 * HEAD), BF16),
            pltpu.VMEM((tokens, width), F32),
            pltpu.VMEM((tokens, width), F32),
            pltpu.VMEM((width, width), F32),
            pltpu.VMEM((width, width), F32),
            pltpu.VMEM((n, width, 2 * HEAD), BF16),
            pltpu.VMEM((tokens, width), BF16),
            pltpu.VMEM((rows, wo.shape[0]), BF16),
            pltpu.VMEM(wo.shape, BF16),
            pltpu.VMEM((rows, model), F32),
            pltpu.VMEM((4 * rows, model), BF16),
            pltpu.VMEM((n * depth, units), BF16),
            pltpu.VMEM((n * depth, units), BF16),
            pltpu.VMEM((units, n * depth), BF16),
            pltpu.VMEM((4 * rows, units), BF16),
            pltpu.VMEM((rows, model), F32),
            pltpu.VMEM((rows, model), F32),
            pltpu.VMEM((n, 2, rows, depth), BF16),
            pltpu.VMEM((n, 2, rows, depth), BF16),
            pltpu.VMEM((n, rows, depth), BF16),
            pltpu.VMEM((n, rows, depth), BF16),
            dma((11,)), dma, dma((4, 11)), dma((4, n)), dma((n,)), dma((n,)), dma((4,)), dma((4,)), dma((3,)), dma((3,)),
            dma((n,)), dma((n,)), dma((n,)), dma((n,)),
        ],
        compiler_params=pltpu.CompilerParams(collective_id=2, has_side_effects=True, vmem_limit_bytes=63 * 2**20),
    )(*inputs, wo, gate, up, down)


def per_device_pairs(
    resid, queries, keys, values, decay_input_part, decay_channel_offset, decay_head_extra,
    correction_rate_input, correction_rate_offset, head_norm_gain, mixer_output_weight,
    feedforward_norm_gain, gate_weight, up_weight, down_weight,
):
    return layer(
        queries, keys, values, decay_input_part, decay_channel_offset, decay_head_extra,
        correction_rate_input, correction_rate_offset, head_norm_gain, resid, feedforward_norm_gain, mixer_output_weight, gate_weight, up_weight, down_weight)


def solution(mesh):
    n_sp, n_tp = mesh.shape["sp"], mesh.shape["tp"]
    if (n_sp, n_tp) == (8, 4):
        inner = Mesh(mesh.devices.reshape(4, 2, 2, 2), ("z", "x", "y", "c"))
        sp, tp = ("z", "x"), ("y", "c")
        body = per_device_pairs
    else:
        nx = 2 if n_sp % 2 == 0 else 1
        nz = n_sp // nx
        inner = Mesh(mesh.devices.reshape(nz, nx, n_tp), ("z", "x", "tp"))
        sp, tp = ("z", "x"), ("tp",)
        body = functools.partial(per_device, nz, nx)
    rows = P((*sp, *tp), None)
    placed = (
        rows, P(sp, tp), P(sp, tp), P(sp, tp), P(sp, tp), P(tp), P(sp, tp), P(sp, tp), P(tp), P(tp), P(), P(),
        P(sp, tp), P(sp, tp), P(tp, sp),
    )
    return jax.shard_map(body, mesh=inner, in_specs=placed, out_specs=rows, check_vma=False)
```

```python
import functools
import math

import jax
import jax.numpy as jnp
from jax import lax
from jax.experimental import pallas as pl
from jax.experimental.pallas import tpu as pltpu
from jax.sharding import Mesh, PartitionSpec as P

HEAD = 64
F32 = jnp.float32
BF16 = jnp.bfloat16


def split2(a):
    high = a.astype(BF16)
    return high, (a - high.astype(F32)).astype(BF16)


def dot3(a, b, dims):
    (ah, al), (bh, bl) = a, b
    dn = (dims, ((), ()))
    d = functools.partial(lax.dot_general, dimension_numbers=dn, preferred_element_type=F32)
    return d(ah, bh) + (d(ah, bl) + d(al, bh))


NN = ((1,), (0,))
NT = ((1,), (1,))
TN = ((0,), (0,))


def chunk_kernel(heads, chunk, *refs):
    chunk_step(heads, chunk, pl.program_id(0), *refs)


def chunk_step(heads, chunk, step, q_ref, k_ref, v_ref, din_ref, doff_ref, extra_ref, rin_ref, roff_ref, reads_ref, total_ref, z_ref):
    rows = q_ref.shape[0]
    width = heads * HEAD
    wide = heads * chunk

    @pl.when(step == 0)
    def _():
        r = lax.broadcasted_iota(jnp.int32, (width, 2 * HEAD), 0) % HEAD
        c = lax.broadcasted_iota(jnp.int32, (width, 2 * HEAD), 1)
        z_ref[...] = jnp.where(r == c, 1.0, 0.0).astype(F32)

    def load(ref):
        return ref[...].astype(F32)

    def stack(a):
        return jnp.concatenate([a[:, h * HEAD:(h + 1) * HEAD] for h in range(heads)], axis=0)

    spread_r = lax.broadcasted_iota(jnp.int32, (heads, width), 0)
    spread_c = lax.broadcasted_iota(jnp.int32, (heads, width), 1) // HEAD
    spread = jnp.where(spread_r == spread_c, 1.0, 0.0).astype(F32)
    extra = extra_ref[...]
    if extra.shape[1] == heads:
        extra = lax.dot_general(extra, spread, ((((1,), (0,))), ((), ())), precision=lax.Precision.HIGHEST, preferred_element_type=F32)
    log_decay = -jax.nn.sigmoid(load(din_ref) + doff_ref[...]) * math.exp(-0.5) - extra
    tr = lax.broadcasted_iota(jnp.int32, (chunk, chunk), 0)
    tc = lax.broadcasted_iota(jnp.int32, (chunk, chunk), 1)
    lower = jnp.where(tr >= tc, 1.0, 0.0).astype(F32)
    cum = lax.dot_general(lower, log_decay, (((1,), (0,)), ((), ())), precision=lax.Precision.HIGHEST, preferred_element_type=F32)
    last = cum[chunk - 1:chunk, :]
    mid = cum[chunk // 2 - 1:chunk // 2, :]
    before = cum - log_decay
    rate = jax.nn.sigmoid(load(rin_ref) + roff_ref[...])

    key = stack(load(k_ref))
    unit = key * lax.rsqrt(jnp.sum(key * key, axis=-1, keepdims=True) + 1e-6)
    base = unit * stack(rate)
    query = stack(load(q_ref))
    value = split2(stack(load(v_ref)))
    to_mid = stack(jnp.exp(mid - cum))
    key_mid = split2(key * to_mid)
    base_mid = split2(base * to_mid)
    query_mid = split2(query * stack(jnp.exp(cum - mid)))
    unit_mid = split2(unit * stack(jnp.exp(before - mid)))
    to_last = stack(jnp.exp(last - cum))

    row = lax.broadcasted_iota(jnp.int32, (wide, wide), 0)
    col = lax.broadcasted_iota(jnp.int32, (wide, wide), 1)
    same = (row // chunk) == (col // chunk)
    strict = same & (row > col)
    upto = same & (row >= col)
    a_ub = jnp.where(strict, dot3(unit_mid, base_mid, NT), 0.0)
    a_uk = jnp.where(strict, dot3(unit_mid, key_mid, NT), 0.0)
    a_qb = jnp.where(upto, dot3(query_mid, base_mid, NT), 0.0)
    a_qk = jnp.where(upto, dot3(query_mid, key_mid, NT), 0.0)

    inverse = jnp.where(row == col, 1.0, 0.0).astype(F32)
    size = 1
    while size < chunk:
        pair = ((row // (2 * size)) == (col // (2 * size))) & ((row // size) > (col // size))
        part = jnp.where(pair, a_ub, 0.0)
        if size == 1:
            inverse = inverse - part
        else:
            inv = split2(inverse)
            inverse = inverse - dot3(split2(dot3(inv, split2(part), NN)), inv, NN)
        size *= 2
    inverse = split2(inverse)

    wr = lax.broadcasted_iota(jnp.int32, (wide, width), 0) // chunk
    wc = lax.broadcasted_iota(jnp.int32, (wide, width), 1) // HEAD

    def spread_wide(a):
        return jnp.where(wr == wc, jnp.concatenate([a] * heads, axis=1), 0.0)

    unit_wide = split2(spread_wide(unit * stack(jnp.exp(before))))
    query_wide = spread_wide(query * stack(jnp.exp(cum)))
    base_wide = split2(spread_wide(base * to_last))
    key_wide = split2(spread_wide(key * to_last))
    qb = split2(a_qb)
    trans = split2(dot3(inverse, unit_wide, NN))
    own = split2(dot3(inverse, split2(dot3(split2(a_uk), value, NN)), NN))
    read = split2(query_wide - dot3(qb, trans, NN))
    out_own = dot3(split2(a_qk), value, NN) - dot3(qb, own, NN)
    pr = lax.broadcasted_iota(jnp.int32, (width, width), 0)
    pc = lax.broadcasted_iota(jnp.int32, (width, width), 1)
    move = jnp.where(pr == pc, jnp.exp(last), 0.0) - dot3(base_wide, trans, TN)
    end = dot3(key_wide, value, TN) - dot3(base_wide, own, TN)

    z = split2(z_ref[...])
    x = dot3(read, z, NN) + jnp.concatenate([jnp.zeros_like(out_own), out_own], axis=1)
    for h in range(heads):
        reads_ref[h] = x[h * chunk:(h + 1) * chunk, :]
    z_new = dot3(split2(move), z, NN) + jnp.concatenate([jnp.zeros_like(end), end], axis=1)
    z_ref[...] = z_new
    total_ref[...] = z_new.astype(BF16)


def chunks(q, k, v, din, doff, extra, rin, roff):
    rows, width = q.shape
    heads = width // HEAD
    chunk = 64
    while rows % chunk:
        chunk //= 2
    tile = pl.BlockSpec((chunk, width), lambda i: (i, 0))
    vec = pl.BlockSpec((1, width), lambda i: (0, 0))
    n = rows // chunk
    return pl.pallas_call(
        functools.partial(chunk_kernel, heads, chunk),
        grid=(n,),
        in_specs=[tile, tile, tile, tile, vec, pl.BlockSpec((chunk, heads), lambda i: (i, 0)), tile, vec],
        out_specs=(
            pl.BlockSpec((heads, chunk, 2 * HEAD), lambda i: (0, i, 0)),
            pl.BlockSpec((width, 2 * HEAD), lambda i: (0, 0)),
        ),
        out_shape=(
            jax.ShapeDtypeStruct((heads, rows, 2 * HEAD), F32),
            jax.ShapeDtypeStruct((width, 2 * HEAD), BF16),
        ),
        scratch_shapes=[pltpu.VMEM((width, 2 * HEAD), F32)],
        compiler_params=pltpu.CompilerParams(dimension_semantics=("arbitrary",), vmem_limit_bytes=40 * 2**20),
    )(q, k, v, din, doff.reshape(1, width), extra, rin, roff.reshape(1, width))


def carry_kernel(nz, nx, total_ref, reads_ref, gain_ref, mixed_ref, held, send_sem, recv_sem):
    n = nz * nx
    me = lax.axis_index("z") * nx + lax.axis_index("x")
    heads = reads_ref.shape[0]

    def place(k):
        peer = lax.rem(me + k, n)
        return {"z": peer // nx, "x": lax.rem(peer, nx)}

    barrier = pltpu.get_barrier_semaphore()
    for k in range(1, n):
        pl.semaphore_signal(barrier, inc=1, device_id=place(k), device_id_type=pl.DeviceIdType.MESH)
    pl.semaphore_wait(barrier, n - 1)
    copies = []
    for k in range(1, n):
        c = pltpu.make_async_remote_copy(
            src_ref=total_ref, dst_ref=held.at[k], send_sem=send_sem.at[k], recv_sem=recv_sem.at[k],
            device_id=place(k), device_id_type=pl.DeviceIdType.MESH)
        c.start()
        copies.append(c)
    for c in copies:
        c.wait()
    state = [jnp.zeros((HEAD, HEAD), F32) for _ in range(heads)]
    for k in range(n - 1, 0, -1):
        there = k <= me
        for h in range(heads):
            block = held[k, h * HEAD:(h + 1) * HEAD, :].astype(F32)
            new = block[:, HEAD:] + jnp.dot(block[:, :HEAD], state[h], precision=lax.Precision.HIGHEST, preferred_element_type=F32)
            state[h] = jnp.where(there, new, state[h])
    outs = []
    for h in range(heads):
        x = reads_ref[h]
        o = x[:, HEAD:] + dot3(split2(x[:, :HEAD]), split2(state[h]), NN)
        center = o - jnp.mean(o, axis=-1, keepdims=True)
        var = jnp.mean(center * center, axis=-1, keepdims=True)
        outs.append(center * lax.rsqrt(var + 1e-5))
    mixed_ref[...] = (jnp.concatenate(outs, axis=1) * gain_ref[...]).astype(BF16)


def carry(total, reads, gain, nz, nx):
    heads, rows, _ = reads.shape
    width = heads * HEAD
    n = nz * nx
    vm = pl.BlockSpec(memory_space=pltpu.VMEM)
    return pl.pallas_call(
        functools.partial(carry_kernel, nz, nx),
        in_specs=[vm, vm, vm],
        out_specs=vm,
        out_shape=jax.ShapeDtypeStruct((rows, width), BF16),
        scratch_shapes=[
            pltpu.VMEM((n, width, 2 * HEAD), BF16),
            pltpu.SemaphoreType.DMA((n,)),
            pltpu.SemaphoreType.DMA((n,)),
        ],
        compiler_params=pltpu.CompilerParams(collective_id=1, has_side_effects=True, vmem_limit_bytes=24 * 2**20),
    )(total, reads, gain.reshape(1, width))


def send_z(block, nz):
    return [lax.ppermute(block, "z", [(s, (s + k) % nz) for s in range(nz)]) for k in range(1, nz)]


def in_order(block, came, nz, axis):
    z = lax.axis_index("z")
    size = block.shape[axis]
    shape = list(block.shape)
    shape[axis] = size * nz
    whole = jnp.zeros(shape, block.dtype)
    whole = lax.dynamic_update_slice_in_dim(whole, block, z * size, axis)
    for k in range(1, nz):
        whole = lax.dynamic_update_slice_in_dim(whole, came[k - 1], lax.rem(z - k + nz, nz) * size, axis)
    return whole


def per_device(
    nz, nx,
    resid, queries, keys, values, decay_input_part, decay_channel_offset, decay_head_extra,
    correction_rate_input, correction_rate_offset, head_norm_gain, mixer_output_weight,
    feedforward_norm_gain, gate_weight, up_weight, down_weight,
):
    ff = gate_weight.shape[1] // nx
    x = lax.axis_index("x")

    def exchange(weight, axis, join):
        pieces = weight.reshape(weight.shape[:axis] + (nx, ff) + weight.shape[axis + 1:])
        return lax.all_to_all(pieces, "x", split_axis=axis, concat_axis=join, tiled=False)

    def swap(weight, axis, join):
        if nx == 1:
            return weight
        if nx != 2:
            out = exchange(weight, axis, join)
            return out.reshape((-1, ff) if axis == 1 else (ff, -1))
        mine = lax.dynamic_slice_in_dim(weight, x * ff, ff, axis)
        other = lax.dynamic_slice_in_dim(weight, (1 - x) * ff, ff, axis)
        came = lax.ppermute(other, "x", [(0, 1), (1, 0)])
        first = jnp.where(x == 0, mine, came)
        second = jnp.where(x == 0, came, mine)
        return jnp.concatenate([first, second], axis=join)

    halves = (swap(gate_weight, 1, 0), swap(up_weight, 1, 0), swap(down_weight, 0, 1))
    halves, queries = lax.optimization_barrier((halves, queries))
    whole_gate = lax.all_gather(halves[0], "z", axis=0, tiled=True)
    up_came = send_z(halves[1], nz)
    down_came = send_z(halves[2], nz)

    reads, total = chunks(
        queries, keys, values, decay_input_part, decay_channel_offset, decay_head_extra,
        correction_rate_input, correction_rate_offset)
    total, up_came = lax.optimization_barrier((total, up_came))
    mixed = carry(total, reads, head_norm_gain, nz, nx)
    row_mixed = lax.all_to_all(mixed, "tp", split_axis=0, concat_axis=1, tiled=True)
    proj = jnp.dot(row_mixed, mixer_output_weight, preferred_element_type=F32)
    mid_f = (resid.astype(F32) + proj).astype(BF16).astype(F32)
    normed = (
        mid_f
        * lax.rsqrt(jnp.mean(mid_f * mid_f, axis=-1, keepdims=True) + 1e-06)
        * feedforward_norm_gain
    ).astype(BF16)
    normed, whole_gate = lax.optimization_barrier((normed, whole_gate))
    whole_up = in_order(halves[1], up_came, nz, 0)
    whole_down = in_order(halves[2], down_came, nz, 1)
    whole_rows = lax.all_gather(normed, ("x", "tp"), axis=0, tiled=True)
    gate = jnp.dot(whole_rows, whole_gate, preferred_element_type=F32)
    upper = jnp.dot(whole_rows, whole_up, preferred_element_type=F32)
    hidden = (jax.nn.silu(gate) * upper).astype(BF16)
    down_sum = lax.psum_scatter(
        jnp.dot(hidden, whole_down, preferred_element_type=F32).astype(BF16),
        ("x", "tp"), scatter_dimension=0, tiled=True,
    ).astype(F32)
    return (mid_f + 0.5 * down_sum).astype(BF16)


MESH = pl.DeviceIdType.MESH


def wide_step(heads, q_ref, k_ref, v_ref, din_ref, doff_ref, extra_ref, rin_ref, roff_ref, read_ref, own_ref, zm_ref, ze_ref):
    chunk = q_ref.shape[0]
    width = heads * HEAD

    def load(ref):
        return ref[...].astype(F32)

    def dot(a, b, dims=NN):
        return lax.dot_general(a, b, (dims, ((), ())), preferred_element_type=F32)

    big_r = lax.broadcasted_iota(jnp.int32, (width, width), 0)
    big_c = lax.broadcasted_iota(jnp.int32, (width, width), 1)
    same = (big_r // HEAD) == (big_c // HEAD)
    blocks = jnp.where(same, 1.0, 0.0).astype(BF16)

    def blocked(pair):
        return tuple(jnp.concatenate([a] * heads, axis=0) * blocks for a in pair)

    def exact(pair, b):
        return dot(pair[0], b) + dot(pair[1], b)

    key = load(k_ref)
    unit = key * lax.rsqrt(exact(split2(key * key), blocks) + 1e-6)
    base = unit * jax.nn.sigmoid(load(rin_ref) + roff_ref[...])
    query = load(q_ref)
    log_decay = -jax.nn.sigmoid(load(din_ref) + doff_ref[...]) * math.exp(-0.5) - extra_ref[...]
    tr = lax.broadcasted_iota(jnp.int32, (chunk, chunk), 0)
    tc = lax.broadcasted_iota(jnp.int32, (chunk, chunk), 1)
    lower = jnp.where(tr >= tc, 1.0, 0.0).astype(BF16)
    ld_high, ld_rest = split2(log_decay)
    ld_mid, ld_low = split2(log_decay - ld_high.astype(F32))
    cum = dot(lower, ld_high) + (dot(lower, ld_mid) + dot(lower, ld_low))
    last = cum[chunk - 1:chunk, :]
    mid = cum[chunk // 2 - 1:chunk // 2, :]
    before = cum - log_decay
    to_mid = jnp.exp(mid - cum)
    to_last = jnp.exp(last - cum)
    key_mid = blocked(split2(key * to_mid))
    base_mid = blocked(split2(base * to_mid))
    left = split2(jnp.concatenate([unit * jnp.exp(before - mid), query * jnp.exp(cum - mid)], axis=0))
    by_base = dot3(left, base_mid, NT)
    by_key = dot3(left, key_mid, NT)
    row = lax.broadcasted_iota(jnp.int32, (chunk, width), 0)
    col = lax.rem(lax.broadcasted_iota(jnp.int32, (chunk, width), 1), HEAD)
    a_ub = jnp.where(row > col, by_base[:chunk], 0.0)
    a_uk = split2(jnp.where(row > col, by_key[:chunk], 0.0))
    a_qb = split2(jnp.where(row >= col, by_base[chunk:], 0.0))
    a_qk = split2(jnp.where(row >= col, by_key[chunk:], 0.0))

    inverse = jnp.where(row == col, 1.0, 0.0).astype(F32)
    size = 1
    while size < chunk:
        joined = ((row // (2 * size)) == (col // (2 * size))) & ((row // size) > (col // size))
        part = jnp.where(joined, a_ub, 0.0)
        if size == 1:
            inverse = inverse - part
        else:
            inv = split2(inverse)
            inverse = inverse - dot3(split2(dot3(inv, blocked(split2(part)), NN)), blocked(inv), NN)
        size *= 2
    inverse = split2(inverse)

    value = v_ref[...]
    (values,) = blocked((value,))
    trans = split2(dot3(inverse, blocked(split2(unit * jnp.exp(before))), NN))
    own = split2(dot3(inverse, blocked(split2(exact(a_uk, values))), NN))
    read = split2(query * jnp.exp(cum) - dot3(a_qb, blocked(trans), NN))
    out_own = exact(a_qk, values) - dot3(a_qb, blocked(own), NN)
    base_last = split2(base * to_last)
    key_last = split2(key * to_last)
    move = jnp.where(big_r == big_c, jnp.exp(last), 0.0) - jnp.where(same, dot3(base_last, trans, TN), 0.0)
    end = dot(key_last[0], value, TN) + dot(key_last[1], value, TN) - dot3(base_last, own, TN)

    zm, ze = split2(zm_ref[...]), split2(ze_ref[...])
    read_ref[...] = dot3(read, zm, NN)
    own_ref[...] = out_own + dot3(read, ze, NN)
    move = split2(move)
    zm_ref[...] = dot3(move, zm, NN)
    ze_ref[...] = dot3(move, ze, NN) + jnp.where(same, end, 0.0)


def layer_kernel(
    chunk, q_hbm, k_hbm, v_hbm, din_hbm, doff_hbm, extra_hbm, rin_hbm,
    roff_hbm, gain_hbm, resid_hbm, fgain_hbm, wo_hbm, gate_hbm, up_hbm, down_hbm, out_ref,
    q_ref, k_ref, v_ref, din_ref, doff_ref, extra_ref, rin_ref, roff_ref, gain_ref, resid_ref, fgain_ref,
    extra_wide, total_ref, other_ref, pair_ref, read_ref, own_ref, zm_ref, ze_ref, held, mixed, mixrow, wo, mid, tok, gate, up, down, hidden, near_sum, far_sum, y_out, y_in, z_out, z_in,
    in_sem, wo_sem, w_send, w_recv, c_send, c_recv, a_send, a_recv, t_send, t_recv, y_send, y_recv, z_send, z_recv,
):
    whole = (q_hbm, k_hbm, v_hbm, din_hbm, doff_hbm, extra_hbm, rin_hbm, roff_hbm, gain_hbm, resid_hbm, fgain_hbm)
    local = (q_ref, k_ref, v_ref, din_ref, doff_ref, extra_ref, rin_ref, roff_ref, gain_ref, resid_ref, fgain_ref)
    loads = [pltpu.make_async_copy(src, dst, in_sem.at[i]) for i, (src, dst) in enumerate(zip(whole, local))]
    for load in loads:
        load.start()
    z, x, y, c = (lax.axis_index(name) for name in ("z", "x", "y", "c"))
    half, low = z // 2, lax.rem(z, 2)
    sib = z + 1 - 2 * low
    pair = lax.rem(z + 2, 4)
    near = 1 + half
    mine = c == half
    me = 2 * z + x
    n = 8
    depth = gate_hbm.shape[0]
    width = q_ref.shape[1]
    heads = width // HEAD
    rows = resid_ref.shape[0]
    model = resid_ref.shape[1]
    cut = down_hbm.shape[0] // 2
    sources = (gate_hbm, up_hbm, down_hbm.at[pl.ds(0, cut), :], down_hbm.at[pl.ds(cut, cut), :])

    def at(index, size):
        return pl.ds(pl.multiple_of(index * size, size), size)

    def remote(src, dst, send, recv, **where):
        return pltpu.make_async_remote_copy(
            src_ref=src, dst_ref=dst, send_sem=send, recv_sem=recv, device_id=where, device_id_type=MESH)

    def piece(m, s):
        if m < 2:
            return (gate, up)[m].at[at(s, depth), :]
        return down.at[pl.ds((m - 2) * cut, cut), at(s, depth)]

    def to(src, m, s, slot, **where):
        return remote(src, piece(m, s), w_send.at[m, slot], w_recv.at[m, s], **where)

    def landed(m, s):
        to(piece(m, s), m, s, 0, c=1 - c).wait_recv()

    def down_landed(s):
        landed(2, s)
        landed(3, s)

    def own(m):
        return pltpu.make_async_copy(sources[m], piece(m, me), w_recv.at[m, me])

    def side_sends(m):
        src = sources[m]
        return ((mine, (to(src, m, me, 1, x=1 - x), to(src, m, me, 2, c=1 - c))),)

    def line_sends(m):
        src = sources[m]
        return (
            (mine, (to(src, m, me, 0, z=sib, c=1 - half),)),
            (jnp.logical_not(mine), (to(src, m, me, 3, z=1 + c, c=low),)),
        )

    first = jnp.where(mine, z, sib)
    second = 2 * (1 - half) + c
    other_first = jnp.where(mine, sib, z)
    other_second = 2 * (1 - half) + 1 - c

    swapped = jnp.logical_and(z == near, c != half)
    early, late = jnp.where(swapped, second, first), jnp.where(swapped, first, second)
    other_swapped = jnp.logical_and(z == near, mine)
    other_early, other_late = jnp.where(other_swapped, other_second, other_first), jnp.where(other_swapped, other_first, other_second)

    def relay(m, step):
        s = 2 * (first, second, *((early, late) if m >= 2 else (first, second)))[step] + (x, x, 1 - x, 1 - x)[step]
        p = piece(m, s)
        if step == 0:
            return s, ((jnp.logical_not(mine), (to(p, m, s, 4, x=1 - x), to(p, m, s, 5, c=1 - c))),)
        if step == 1:
            return s, (
                (z == near, (to(p, m, s, 6, z=3 * half),)),
                (None, (to(p, m, s, 7, x=1 - x), to(p, m, s, 8, c=1 - c))),
            )
        return s, ((None, (to(p, m, s, 7 + step, c=1 - c),)),)

    def each(groups, act):
        for when, copies in groups:
            if when is None:
                for copy in copies:
                    act(copy)
            else:
                @pl.when(when)
                def _():
                    for copy in copies:
                        act(copy)

    def start(copy):
        copy.start()

    def begin(m):
        @pl.when(mine)
        def _():
            own(m).start()
        each(side_sends(m), start)

    def pump(m, step):
        s, groups = relay(m, step)
        landed(m, s)
        each(groups, start)

    def pump_far(m):
        s, groups = relay(m, 1)
        landed(m, s)
        each(groups[:1], start)

    def pump_side(m):
        each(relay(m, 1)[1][1:], start)

    def rest_of(m):
        for plane in (other_first, other_second):
            for column in (x, 1 - x):
                landed(m, 2 * plane + column)

    def drain(m):
        for groups in (side_sends(m), line_sends(m), *(relay(m, step)[1] for step in range(4))):
            each(groups, lambda copy: copy.wait_send())

    barrier = pltpu.get_barrier_semaphore()
    for dz in range(4):
        for dx in range(2):
            for dy in range(2):
                for dc in range(2):
                    if dz or dx or dy or dc:
                        peer = {"z": lax.rem(z + dz, 4), "x": lax.rem(x + dx, 2), "y": lax.rem(y + dy, 2), "c": lax.rem(c + dc, 2)}
                        pl.semaphore_signal(barrier, inc=1, device_id=peer, device_id_type=MESH)
    pl.semaphore_wait(barrier, 31)

    load_wo = pltpu.make_async_copy(wo_hbm, wo, wo_sem)
    load_wo.start()

    def carry_copy(k):
        return remote(pair_ref, held.at[k], c_send.at[k], c_recv.at[k], z=lax.rem(z + k, 4))

    leftward = jnp.logical_or(z == 3, jnp.logical_and(c == 0, z >= 1))
    rightward = jnp.logical_not(leftward)
    is_near = z == near
    is_far = jnp.logical_not(is_near)
    is_last = z == 3
    not_mine = jnp.logical_not(mine)
    for m in range(2):
        each(line_sends(m), start)
        begin(m)

    @pl.when(jnp.logical_and(leftward, not_mine))
    def _():
        each(line_sends(2), start)
        each(line_sends(3), start)
    tokens = q_ref.shape[0]
    for load in loads:
        load.wait()
    spread_r = lax.broadcasted_iota(jnp.int32, (heads, width), 0)
    spread_c = lax.broadcasted_iota(jnp.int32, (heads, width), 1) // HEAD
    spread = jnp.where(spread_r == spread_c, 1.0, 0.0).astype(F32)
    extra_wide[...] = lax.dot_general(
        extra_ref[...], spread, (TN, ((), ())), precision=lax.Precision.HIGHEST, preferred_element_type=F32)

    big_r = lax.broadcasted_iota(jnp.int32, (width, width), 0)
    big_c = lax.broadcasted_iota(jnp.int32, (width, width), 1)
    blocks = jnp.where((big_r // HEAD) == (big_c // HEAD), 1.0, 0.0).astype(BF16)
    zm_ref[...] = jnp.where(big_r == big_c, 1.0, 0.0).astype(F32)
    ze_ref[...] = jnp.zeros_like(ze_ref)

    def advance(i, _):
        span = at(i, chunk)
        wide_step(
            heads, q_ref.at[span, :], k_ref.at[span, :], v_ref.at[span, :], din_ref.at[span, :], doff_ref,
            extra_wide.at[span, :], rin_ref.at[span, :], roff_ref, read_ref.at[span, :], own_ref.at[span, :], zm_ref, ze_ref)

        @pl.when(jnp.logical_and(i == 2, is_far))
        def _():
            pump(0, 0)

        @pl.when(jnp.logical_and(i == 3, is_near))
        def _():
            pump(0, 0)
            pump_far(0)

        @pl.when(jnp.logical_and(i == 3, jnp.logical_and(is_last, mine)))
        def _():
            each(line_sends(2), start)
            each(line_sends(3), start)

        return 0

    lax.fori_loop(0, tokens // chunk, advance, 0)

    for h in range(heads):
        span = slice(h * HEAD, (h + 1) * HEAD)
        total_ref[span, :] = jnp.concatenate([zm_ref[span, span], ze_ref[span, span]], axis=1).astype(BF16)
    swap = remote(total_ref, other_ref, c_send.at[0], c_recv.at[0], x=1 - x)
    swap.start()

    @pl.when(is_near)
    def _():
        pump_side(0)

    @pl.when(is_far)
    def _():
        pump(1, 0)
    swap.wait_recv()

    def tall(block):
        return jnp.concatenate([block[:, :HEAD]] * heads, axis=1) * blocks

    ours, theirs = total_ref[...].astype(F32), other_ref[...].astype(F32)
    older, newer = jnp.where(x == 0, ours, theirs).astype(BF16), jnp.where(x == 0, theirs, ours).astype(BF16)
    joint = jnp.dot(tall(newer), older, preferred_element_type=F32)
    pair_ref[...] = (joint + jnp.where(
        lax.broadcasted_iota(jnp.int32, joint.shape, 1) >= HEAD, newer.astype(F32), 0.0)).astype(BF16)
    for k in range(1, 4):
        @pl.when(z + k < 4)
        def _():
            carry_copy(k).start()

    @pl.when(jnp.logical_and(rightward, not_mine))
    def _():
        each(line_sends(2), start)
        each(line_sends(3), start)

    @pl.when(jnp.logical_and(rightward, jnp.logical_and(mine, is_far)))
    def _():
        each(line_sends(2), start)
        each(line_sends(3), start)

    @pl.when(is_near)
    def _():
        pump(1, 0)
        pump(1, 1)

    @pl.when(jnp.logical_and(mine, is_near))
    def _():
        each(line_sends(2), start)
        each(line_sends(3), start)

    @pl.when(is_last)
    def _():
        pump(0, 1)
        begin(2)
        begin(3)
    for k in range(1, 4):
        @pl.when(z >= k)
        def _():
            carry_copy(k).wait_recv()
    state = jnp.zeros((width, HEAD), F32)
    for there, block in [(z >= k, held[k]) for k in (3, 2, 1)] + [(x == 1, older)]:
        move = tall(block)
        high, rest = split2(state)
        moved = jnp.dot(move, high, preferred_element_type=F32) + jnp.dot(move, rest, preferred_element_type=F32)
        state = jnp.where(there, block[:, HEAD:].astype(F32) + moved, state)

    def head_mean(a):
        high, low_part = split2(a)
        return (jnp.dot(high, blocks, preferred_element_type=F32) + jnp.dot(low_part, blocks, preferred_element_type=F32)) / HEAD

    carried = tuple(tall(a) for a in split2(state))
    o = own_ref[...] + dot3(split2(read_ref[...]), carried, NN)
    center = o - head_mean(o)
    mixed[...] = (center * lax.rsqrt(head_mean(center * center) + 1e-5) * gain_ref[...]).astype(BF16)

    t = 2 * y + c

    def exchange(dy, dc):
        ty, tc = lax.rem(y + dy, 2), lax.rem(c + dc, 2)
        slot = 2 * dy + dc
        return remote(
            mixed.at[at(2 * ty + tc, rows), :], mixrow.at[:, at(t, width)], a_send.at[slot], a_recv.at[slot], y=ty, c=tc)

    swaps = [exchange(1, 0), exchange(1, 1), exchange(0, 1)]
    for copy in swaps:
        copy.start()
    mixrow[:, at(t, width)] = mixed[at(t, rows), :]


    @pl.when(z == 0)
    def _():
        pump(0, 1)
    load_wo.wait()
    for copy in swaps:
        copy.wait()

    tile = 512
    square = jnp.zeros((rows, 1), F32)
    for j in range(0, model, tile):
        proj = jnp.dot(mixrow[...], wo[:, j:j + tile], preferred_element_type=F32)
        part = (resid_ref[:, j:j + tile].astype(F32) + proj).astype(BF16).astype(F32)
        mid[:, j:j + tile] = part
        square += jnp.sum(part * part, axis=-1, keepdims=True)
    g = 2 * half + y
    g_far = 2 * (1 - half) + y
    g_side = 2 * half + 1 - y
    g_diag = 2 * (1 - half) + 1 - y
    tok[at(g, rows), :] = (mid[...] * lax.rsqrt(square / model + 1e-06) * fgain_ref[...]).astype(BF16)

    def rows_to(block, slot, **where):
        r = tok.at[at(block, rows), :]
        return remote(r, r, t_send.at[slot], t_recv.at[slot], **where)

    def rows_from(block, slot):
        r = tok.at[at(block, rows), :]
        remote(r, r, t_send.at[slot], t_recv.at[slot], y=1 - y).wait_recv()

    ahead = rows_to(g, 0, z=pair)
    beside = rows_to(g, 1, y=1 - y)
    onward = rows_to(g_far, 2, y=1 - y)
    beside.start()

    @pl.when(is_far)
    def _():
        ahead.start()

    @pl.when(is_far)
    def _():
        pump(1, 1)

    @pl.when(z == 0)
    def _():
        begin(2)
        begin(3)
    pump(0, 2)
    pump(0, 3)

    @pl.when(is_near)
    def _():
        ahead.start()

    @pl.when(z == 1)
    def _():
        pump_far(2)
        pump_far(3)
    rows_from(g_far, 0)
    onward.start()
    pump(1, 2)

    @pl.when(is_near)
    def _():
        begin(2)
        begin(3)

    @pl.when(z == 1)
    def _():
        pump_side(2)
        pump_side(3)

    @pl.when(z == 2)
    def _():
        pump(2, 1)
        pump(3, 1)

    @pl.when(is_near)
    def _():
        pump(2, 0)
        pump(3, 0)

    pump(1, 3)

    @pl.when(is_far)
    def _():
        pump(2, 0)
        pump(3, 0)

    rest_of(0)
    rest_of(1)
    rows_from(g_side, 1)
    rows_from(g_diag, 2)

    units = gate.shape[1]
    for j in range(0, units, 256):
        cols = slice(j, min(j + 256, units))
        gated = jnp.dot(tok[...], gate[:, cols], preferred_element_type=F32)
        upper = jnp.dot(tok[...], up[:, cols], preferred_element_type=F32)
        hidden[:, cols] = (gated * jax.nn.sigmoid(gated) * upper).astype(BF16)

    def side_copy(i):
        return remote(y_out.at[i], y_in.at[i], y_send.at[i], y_recv.at[i], y=1 - y)

    def far_copy(i):
        return remote(z_out.at[i], z_in.at[i], z_send.at[i], z_recv.at[i], z=pair)

    def slice_of(plane, column):
        i = 2 * plane + column
        cols = at(i, depth)
        for place_of, dst in ((g_diag, y_out.at[i, 0]), (g_side, y_out.at[i, 1])):
            dst[...] = jnp.dot(hidden[at(place_of, rows), :], down[:, cols], preferred_element_type=F32).astype(BF16)
        far_sum[:, cols] = jnp.dot(hidden[at(g_far, rows), :], down[:, cols], preferred_element_type=F32)
        side_copy(i).start()
        near_sum[:, cols] = jnp.dot(hidden[at(g, rows), :], down[:, cols], preferred_element_type=F32)

    def pass_on(plane, column):
        i = 2 * plane + column
        side_copy(i).wait_recv()
        z_out[i] = (far_sum[:, at(i, depth)] + y_in[i, 0].astype(F32)).astype(BF16)
        far_copy(i).start()

    next_first, next_other = jnp.where(is_far, first, second), jnp.where(is_far, other_first, other_second)
    next_column = jnp.where(is_far, 1 - x, x)
    then_first, then_other = jnp.where(is_far, second, early), jnp.where(is_far, other_second, other_early)
    then_column = jnp.where(is_far, x, 1 - x)

    @pl.when(is_far)
    def _():
        pump(2, 1)
    slice_of(first, x)
    down_landed(2 * other_first + x)
    slice_of(other_first, x)

    @pl.when(z == 0)
    def _():
        pump(3, 1)

    @pl.when(is_far)
    def _():
        pump(2, 2)
        pump(3, 2)
    slice_of(next_first, next_column)
    down_landed(2 * next_other + next_column)
    slice_of(next_other, next_column)
    pass_on(first, x)
    pass_on(other_first, x)

    @pl.when(is_last)
    def _():
        pump(3, 1)
    drain(0)
    drain(1)
    swap.wait_send()
    for k in range(1, 4):
        @pl.when(z + k < 4)
        def _():
            carry_copy(k).wait_send()

    @pl.when(is_near)
    def _():
        pump(2, 2)
        pump(3, 2)
    slice_of(then_first, then_column)
    down_landed(2 * then_other + then_column)
    slice_of(then_other, then_column)
    pass_on(next_first, next_column)
    pass_on(next_other, next_column)
    pass_on(then_first, then_column)
    pass_on(then_other, then_column)
    pump(2, 3)
    pump(3, 3)
    slice_of(late, 1 - x)
    down_landed(2 * other_late + 1 - x)
    slice_of(other_late, 1 - x)
    pass_on(late, 1 - x)
    pass_on(other_late, 1 - x)
    for i in range(n):
        cols = slice(i * depth, (i + 1) * depth)
        far_copy(i).wait_recv()
        total = near_sum[:, cols] + y_in[i, 1].astype(F32) + z_in[i].astype(F32)
        out_ref[:, cols] = (mid[:, cols] + 0.5 * total).astype(BF16)

    drain(2)
    drain(3)
    for copy in (ahead, beside, onward):
        copy.wait_send()
    for i in range(n):
        side_copy(i).wait_send()
        far_copy(i).wait_send()


def layer(q, k, v, din, doff, extra, rin, roff, gain, resid, fgain, wo, gate, up, down):
    tokens, width = q.shape
    heads = width // HEAD
    chunk = 64
    while tokens % chunk:
        chunk //= 2
    rows, model = resid.shape
    depth, units = gate.shape
    n = 8
    vm = pl.BlockSpec(memory_space=pltpu.VMEM)
    hbm = pl.BlockSpec(memory_space=pl.ANY)
    dma = pltpu.SemaphoreType.DMA
    inputs = (
        q, k, v, din, doff.reshape(1, width), extra.T, rin, roff.reshape(1, width), gain.reshape(1, width), resid, fgain.reshape(1, model))
    return pl.pallas_call(
        functools.partial(layer_kernel, chunk),
        in_specs=[hbm] * 15,
        out_specs=vm,
        out_shape=pltpu.VMEM((rows, model), BF16),
        scratch_shapes=[pltpu.VMEM(a.shape, a.dtype) for a in inputs] + [
            pltpu.VMEM((tokens, width), F32),
            pltpu.VMEM((width, 2 * HEAD), BF16),
            pltpu.VMEM((width, 2 * HEAD), BF16),
            pltpu.VMEM((width, 2 * HEAD), BF16),
            pltpu.VMEM((tokens, width), F32),
            pltpu.VMEM((tokens, width), F32),
            pltpu.VMEM((width, width), F32),
            pltpu.VMEM((width, width), F32),
            pltpu.VMEM((4, width, 2 * HEAD), BF16),
            pltpu.VMEM((tokens, width), BF16),
            pltpu.VMEM((rows, wo.shape[0]), BF16),
            pltpu.VMEM(wo.shape, BF16),
            pltpu.VMEM((rows, model), F32),
            pltpu.VMEM((4 * rows, model), BF16),
            pltpu.VMEM((n * depth, units), BF16),
            pltpu.VMEM((n * depth, units), BF16),
            pltpu.VMEM((units, n * depth), BF16),
            pltpu.VMEM((4 * rows, units), BF16),
            pltpu.VMEM((rows, model), F32),
            pltpu.VMEM((rows, model), F32),
            pltpu.VMEM((n, 2, rows, depth), BF16),
            pltpu.VMEM((n, 2, rows, depth), BF16),
            pltpu.VMEM((n, rows, depth), BF16),
            pltpu.VMEM((n, rows, depth), BF16),
            dma((11,)), dma, dma((4, 11)), dma((4, n)), dma((4,)), dma((4,)), dma((4,)), dma((4,)), dma((3,)), dma((3,)),
            dma((n,)), dma((n,)), dma((n,)), dma((n,)),
        ],
        compiler_params=pltpu.CompilerParams(collective_id=2, has_side_effects=True, vmem_limit_bytes=67043328 - 2 * rows * model),
    )(*inputs, wo, gate, up, down)


def per_device_pairs(
    resid, queries, keys, values, decay_input_part, decay_channel_offset, decay_head_extra,
    correction_rate_input, correction_rate_offset, head_norm_gain, mixer_output_weight,
    feedforward_norm_gain, gate_weight, up_weight, down_weight,
):
    return layer(
        queries, keys, values, decay_input_part, decay_channel_offset, decay_head_extra,
        correction_rate_input, correction_rate_offset, head_norm_gain, resid, feedforward_norm_gain, mixer_output_weight, gate_weight, up_weight, down_weight)


def solution(mesh):
    n_sp, n_tp = mesh.shape["sp"], mesh.shape["tp"]
    if (n_sp, n_tp) == (8, 4):
        inner = Mesh(mesh.devices.reshape(4, 2, 2, 2), ("z", "x", "y", "c"))
        sp, tp = ("z", "x"), ("y", "c")
        body = per_device_pairs
    else:
        nx = 2 if n_sp % 2 == 0 else 1
        nz = n_sp // nx
        inner = Mesh(mesh.devices.reshape(nz, nx, n_tp), ("z", "x", "tp"))
        sp, tp = ("z", "x"), ("tp",)
        body = functools.partial(per_device, nz, nx)
    rows = P((*sp, *tp), None)
    placed = (
        rows, P(sp, tp), P(sp, tp), P(sp, tp), P(sp, tp), P(tp), P(sp, tp), P(sp, tp), P(tp), P(tp), P(), P(),
        P(sp, tp), P(sp, tp), P(tp, sp),
    )
    return jax.shard_map(body, mesh=inner, in_specs=placed, out_specs=rows, check_vma=False)
```

```python
import functools
import math

import jax
import jax.numpy as jnp
from jax import lax
from jax.experimental import pallas as pl
from jax.experimental.pallas import tpu as pltpu
from jax.sharding import Mesh, PartitionSpec as P

HEAD = 64
F32 = jnp.float32
BF16 = jnp.bfloat16


def split2(a):
    high = a.astype(BF16)
    return high, (a - high.astype(F32)).astype(BF16)


def dot3(a, b, dims):
    (ah, al), (bh, bl) = a, b
    dn = (dims, ((), ()))
    d = functools.partial(lax.dot_general, dimension_numbers=dn, preferred_element_type=F32)
    return d(ah, bh) + (d(ah, bl) + d(al, bh))


NN = ((1,), (0,))
NT = ((1,), (1,))
TN = ((0,), (0,))


def chunk_kernel(heads, chunk, *refs):
    chunk_step(heads, chunk, pl.program_id(0), *refs)


def chunk_step(heads, chunk, step, q_ref, k_ref, v_ref, din_ref, doff_ref, extra_ref, rin_ref, roff_ref, reads_ref, total_ref, z_ref):
    rows = q_ref.shape[0]
    width = heads * HEAD
    wide = heads * chunk

    @pl.when(step == 0)
    def _():
        r = lax.broadcasted_iota(jnp.int32, (width, 2 * HEAD), 0) % HEAD
        c = lax.broadcasted_iota(jnp.int32, (width, 2 * HEAD), 1)
        z_ref[...] = jnp.where(r == c, 1.0, 0.0).astype(F32)

    def load(ref):
        return ref[...].astype(F32)

    def stack(a):
        return jnp.concatenate([a[:, h * HEAD:(h + 1) * HEAD] for h in range(heads)], axis=0)

    spread_r = lax.broadcasted_iota(jnp.int32, (heads, width), 0)
    spread_c = lax.broadcasted_iota(jnp.int32, (heads, width), 1) // HEAD
    spread = jnp.where(spread_r == spread_c, 1.0, 0.0).astype(F32)
    extra = extra_ref[...]
    if extra.shape[1] == heads:
        extra = lax.dot_general(extra, spread, ((((1,), (0,))), ((), ())), precision=lax.Precision.HIGHEST, preferred_element_type=F32)
    log_decay = -jax.nn.sigmoid(load(din_ref) + doff_ref[...]) * math.exp(-0.5) - extra
    tr = lax.broadcasted_iota(jnp.int32, (chunk, chunk), 0)
    tc = lax.broadcasted_iota(jnp.int32, (chunk, chunk), 1)
    lower = jnp.where(tr >= tc, 1.0, 0.0).astype(F32)
    cum = lax.dot_general(lower, log_decay, (((1,), (0,)), ((), ())), precision=lax.Precision.HIGHEST, preferred_element_type=F32)
    last = cum[chunk - 1:chunk, :]
    mid = cum[chunk // 2 - 1:chunk // 2, :]
    before = cum - log_decay
    rate = jax.nn.sigmoid(load(rin_ref) + roff_ref[...])

    key = stack(load(k_ref))
    unit = key * lax.rsqrt(jnp.sum(key * key, axis=-1, keepdims=True) + 1e-6)
    base = unit * stack(rate)
    query = stack(load(q_ref))
    value = split2(stack(load(v_ref)))
    to_mid = stack(jnp.exp(mid - cum))
    key_mid = split2(key * to_mid)
    base_mid = split2(base * to_mid)
    query_mid = split2(query * stack(jnp.exp(cum - mid)))
    unit_mid = split2(unit * stack(jnp.exp(before - mid)))
    to_last = stack(jnp.exp(last - cum))

    row = lax.broadcasted_iota(jnp.int32, (wide, wide), 0)
    col = lax.broadcasted_iota(jnp.int32, (wide, wide), 1)
    same = (row // chunk) == (col // chunk)
    strict = same & (row > col)
    upto = same & (row >= col)
    a_ub = jnp.where(strict, dot3(unit_mid, base_mid, NT), 0.0)
    a_uk = jnp.where(strict, dot3(unit_mid, key_mid, NT), 0.0)
    a_qb = jnp.where(upto, dot3(query_mid, base_mid, NT), 0.0)
    a_qk = jnp.where(upto, dot3(query_mid, key_mid, NT), 0.0)

    inverse = jnp.where(row == col, 1.0, 0.0).astype(F32)
    size = 1
    while size < chunk:
        pair = ((row // (2 * size)) == (col // (2 * size))) & ((row // size) > (col // size))
        part = jnp.where(pair, a_ub, 0.0)
        if size == 1:
            inverse = inverse - part
        else:
            inv = split2(inverse)
            inverse = inverse - dot3(split2(dot3(inv, split2(part), NN)), inv, NN)
        size *= 2
    inverse = split2(inverse)

    wr = lax.broadcasted_iota(jnp.int32, (wide, width), 0) // chunk
    wc = lax.broadcasted_iota(jnp.int32, (wide, width), 1) // HEAD

    def spread_wide(a):
        return jnp.where(wr == wc, jnp.concatenate([a] * heads, axis=1), 0.0)

    unit_wide = split2(spread_wide(unit * stack(jnp.exp(before))))
    query_wide = spread_wide(query * stack(jnp.exp(cum)))
    base_wide = split2(spread_wide(base * to_last))
    key_wide = split2(spread_wide(key * to_last))
    qb = split2(a_qb)
    trans = split2(dot3(inverse, unit_wide, NN))
    own = split2(dot3(inverse, split2(dot3(split2(a_uk), value, NN)), NN))
    read = split2(query_wide - dot3(qb, trans, NN))
    out_own = dot3(split2(a_qk), value, NN) - dot3(qb, own, NN)
    pr = lax.broadcasted_iota(jnp.int32, (width, width), 0)
    pc = lax.broadcasted_iota(jnp.int32, (width, width), 1)
    move = jnp.where(pr == pc, jnp.exp(last), 0.0) - dot3(base_wide, trans, TN)
    end = dot3(key_wide, value, TN) - dot3(base_wide, own, TN)

    z = split2(z_ref[...])
    x = dot3(read, z, NN) + jnp.concatenate([jnp.zeros_like(out_own), out_own], axis=1)
    for h in range(heads):
        reads_ref[h] = x[h * chunk:(h + 1) * chunk, :]
    z_new = dot3(split2(move), z, NN) + jnp.concatenate([jnp.zeros_like(end), end], axis=1)
    z_ref[...] = z_new
    total_ref[...] = z_new.astype(BF16)


def chunks(q, k, v, din, doff, extra, rin, roff):
    rows, width = q.shape
    heads = width // HEAD
    chunk = 64
    while rows % chunk:
        chunk //= 2
    tile = pl.BlockSpec((chunk, width), lambda i: (i, 0))
    vec = pl.BlockSpec((1, width), lambda i: (0, 0))
    n = rows // chunk
    return pl.pallas_call(
        functools.partial(chunk_kernel, heads, chunk),
        grid=(n,),
        in_specs=[tile, tile, tile, tile, vec, pl.BlockSpec((chunk, heads), lambda i: (i, 0)), tile, vec],
        out_specs=(
            pl.BlockSpec((heads, chunk, 2 * HEAD), lambda i: (0, i, 0)),
            pl.BlockSpec((width, 2 * HEAD), lambda i: (0, 0)),
        ),
        out_shape=(
            jax.ShapeDtypeStruct((heads, rows, 2 * HEAD), F32),
            jax.ShapeDtypeStruct((width, 2 * HEAD), BF16),
        ),
        scratch_shapes=[pltpu.VMEM((width, 2 * HEAD), F32)],
        compiler_params=pltpu.CompilerParams(dimension_semantics=("arbitrary",), vmem_limit_bytes=40 * 2**20),
    )(q, k, v, din, doff.reshape(1, width), extra, rin, roff.reshape(1, width))


def carry_kernel(nz, nx, total_ref, reads_ref, gain_ref, mixed_ref, held, send_sem, recv_sem):
    n = nz * nx
    me = lax.axis_index("z") * nx + lax.axis_index("x")
    heads = reads_ref.shape[0]

    def place(k):
        peer = lax.rem(me + k, n)
        return {"z": peer // nx, "x": lax.rem(peer, nx)}

    barrier = pltpu.get_barrier_semaphore()
    for k in range(1, n):
        pl.semaphore_signal(barrier, inc=1, device_id=place(k), device_id_type=pl.DeviceIdType.MESH)
    pl.semaphore_wait(barrier, n - 1)
    copies = []
    for k in range(1, n):
        c = pltpu.make_async_remote_copy(
            src_ref=total_ref, dst_ref=held.at[k], send_sem=send_sem.at[k], recv_sem=recv_sem.at[k],
            device_id=place(k), device_id_type=pl.DeviceIdType.MESH)
        c.start()
        copies.append(c)
    for c in copies:
        c.wait()
    state = [jnp.zeros((HEAD, HEAD), F32) for _ in range(heads)]
    for k in range(n - 1, 0, -1):
        there = k <= me
        for h in range(heads):
            block = held[k, h * HEAD:(h + 1) * HEAD, :].astype(F32)
            new = block[:, HEAD:] + jnp.dot(block[:, :HEAD], state[h], precision=lax.Precision.HIGHEST, preferred_element_type=F32)
            state[h] = jnp.where(there, new, state[h])
    outs = []
    for h in range(heads):
        x = reads_ref[h]
        o = x[:, HEAD:] + dot3(split2(x[:, :HEAD]), split2(state[h]), NN)
        center = o - jnp.mean(o, axis=-1, keepdims=True)
        var = jnp.mean(center * center, axis=-1, keepdims=True)
        outs.append(center * lax.rsqrt(var + 1e-5))
    mixed_ref[...] = (jnp.concatenate(outs, axis=1) * gain_ref[...]).astype(BF16)


def carry(total, reads, gain, nz, nx):
    heads, rows, _ = reads.shape
    width = heads * HEAD
    n = nz * nx
    vm = pl.BlockSpec(memory_space=pltpu.VMEM)
    return pl.pallas_call(
        functools.partial(carry_kernel, nz, nx),
        in_specs=[vm, vm, vm],
        out_specs=vm,
        out_shape=jax.ShapeDtypeStruct((rows, width), BF16),
        scratch_shapes=[
            pltpu.VMEM((n, width, 2 * HEAD), BF16),
            pltpu.SemaphoreType.DMA((n,)),
            pltpu.SemaphoreType.DMA((n,)),
        ],
        compiler_params=pltpu.CompilerParams(collective_id=1, has_side_effects=True, vmem_limit_bytes=24 * 2**20),
    )(total, reads, gain.reshape(1, width))


def send_z(block, nz):
    return [lax.ppermute(block, "z", [(s, (s + k) % nz) for s in range(nz)]) for k in range(1, nz)]


def in_order(block, came, nz, axis):
    z = lax.axis_index("z")
    size = block.shape[axis]
    shape = list(block.shape)
    shape[axis] = size * nz
    whole = jnp.zeros(shape, block.dtype)
    whole = lax.dynamic_update_slice_in_dim(whole, block, z * size, axis)
    for k in range(1, nz):
        whole = lax.dynamic_update_slice_in_dim(whole, came[k - 1], lax.rem(z - k + nz, nz) * size, axis)
    return whole


def per_device(
    nz, nx,
    resid, queries, keys, values, decay_input_part, decay_channel_offset, decay_head_extra,
    correction_rate_input, correction_rate_offset, head_norm_gain, mixer_output_weight,
    feedforward_norm_gain, gate_weight, up_weight, down_weight,
):
    ff = gate_weight.shape[1] // nx
    x = lax.axis_index("x")

    def exchange(weight, axis, join):
        pieces = weight.reshape(weight.shape[:axis] + (nx, ff) + weight.shape[axis + 1:])
        return lax.all_to_all(pieces, "x", split_axis=axis, concat_axis=join, tiled=False)

    def swap(weight, axis, join):
        if nx == 1:
            return weight
        if nx != 2:
            out = exchange(weight, axis, join)
            return out.reshape((-1, ff) if axis == 1 else (ff, -1))
        mine = lax.dynamic_slice_in_dim(weight, x * ff, ff, axis)
        other = lax.dynamic_slice_in_dim(weight, (1 - x) * ff, ff, axis)
        came = lax.ppermute(other, "x", [(0, 1), (1, 0)])
        first = jnp.where(x == 0, mine, came)
        second = jnp.where(x == 0, came, mine)
        return jnp.concatenate([first, second], axis=join)

    halves = (swap(gate_weight, 1, 0), swap(up_weight, 1, 0), swap(down_weight, 0, 1))
    halves, queries = lax.optimization_barrier((halves, queries))
    whole_gate = lax.all_gather(halves[0], "z", axis=0, tiled=True)
    up_came = send_z(halves[1], nz)
    down_came = send_z(halves[2], nz)

    reads, total = chunks(
        queries, keys, values, decay_input_part, decay_channel_offset, decay_head_extra,
        correction_rate_input, correction_rate_offset)
    total, up_came = lax.optimization_barrier((total, up_came))
    mixed = carry(total, reads, head_norm_gain, nz, nx)
    row_mixed = lax.all_to_all(mixed, "tp", split_axis=0, concat_axis=1, tiled=True)
    proj = jnp.dot(row_mixed, mixer_output_weight, preferred_element_type=F32)
    mid_f = (resid.astype(F32) + proj).astype(BF16).astype(F32)
    normed = (
        mid_f
        * lax.rsqrt(jnp.mean(mid_f * mid_f, axis=-1, keepdims=True) + 1e-06)
        * feedforward_norm_gain
    ).astype(BF16)
    normed, whole_gate = lax.optimization_barrier((normed, whole_gate))
    whole_up = in_order(halves[1], up_came, nz, 0)
    whole_down = in_order(halves[2], down_came, nz, 1)
    whole_rows = lax.all_gather(normed, ("x", "tp"), axis=0, tiled=True)
    gate = jnp.dot(whole_rows, whole_gate, preferred_element_type=F32)
    upper = jnp.dot(whole_rows, whole_up, preferred_element_type=F32)
    hidden = (jax.nn.silu(gate) * upper).astype(BF16)
    down_sum = lax.psum_scatter(
        jnp.dot(hidden, whole_down, preferred_element_type=F32).astype(BF16),
        ("x", "tp"), scatter_dimension=0, tiled=True,
    ).astype(F32)
    return (mid_f + 0.5 * down_sum).astype(BF16)


MESH = pl.DeviceIdType.MESH


def wide_step(heads, q_ref, k_ref, v_ref, din_ref, doff_ref, extra_ref, rin_ref, roff_ref, read_ref, own_ref, zm_ref, ze_ref):
    chunk = q_ref.shape[0]
    width = heads * HEAD

    def load(ref):
        return ref[...].astype(F32)

    def dot(a, b, dims=NN):
        return lax.dot_general(a, b, (dims, ((), ())), preferred_element_type=F32)

    big_r = lax.broadcasted_iota(jnp.int32, (width, width), 0)
    big_c = lax.broadcasted_iota(jnp.int32, (width, width), 1)
    same = (big_r // HEAD) == (big_c // HEAD)
    blocks = jnp.where(same, 1.0, 0.0).astype(BF16)

    def blocked(pair):
        return tuple(jnp.concatenate([a] * heads, axis=0) * blocks for a in pair)

    def exact(pair, b):
        return dot(pair[0], b) + dot(pair[1], b)

    key = load(k_ref)
    unit = key * lax.rsqrt(exact(split2(key * key), blocks) + 1e-6)
    base = unit * jax.nn.sigmoid(load(rin_ref) + roff_ref[...])
    query = load(q_ref)
    log_decay = -jax.nn.sigmoid(load(din_ref) + doff_ref[...]) * math.exp(-0.5) - extra_ref[...]
    tr = lax.broadcasted_iota(jnp.int32, (chunk, chunk), 0)
    tc = lax.broadcasted_iota(jnp.int32, (chunk, chunk), 1)
    lower = jnp.where(tr >= tc, 1.0, 0.0).astype(BF16)
    ld_high, ld_rest = split2(log_decay)
    ld_mid, ld_low = split2(log_decay - ld_high.astype(F32))
    cum = dot(lower, ld_high) + (dot(lower, ld_mid) + dot(lower, ld_low))
    last = cum[chunk - 1:chunk, :]
    mid = cum[chunk // 2 - 1:chunk // 2, :]
    before = cum - log_decay
    to_mid = jnp.exp(mid - cum)
    to_last = jnp.exp(last - cum)
    key_mid = blocked(split2(key * to_mid))
    base_mid = blocked(split2(base * to_mid))
    left = split2(jnp.concatenate([unit * jnp.exp(before - mid), query * jnp.exp(cum - mid)], axis=0))
    by_base = dot3(left, base_mid, NT)
    by_key = dot3(left, key_mid, NT)
    row = lax.broadcasted_iota(jnp.int32, (chunk, width), 0)
    col = lax.rem(lax.broadcasted_iota(jnp.int32, (chunk, width), 1), HEAD)
    a_ub = jnp.where(row > col, by_base[:chunk], 0.0)
    a_uk = split2(jnp.where(row > col, by_key[:chunk], 0.0))
    a_qb = split2(jnp.where(row >= col, by_base[chunk:], 0.0))
    a_qk = split2(jnp.where(row >= col, by_key[chunk:], 0.0))

    inverse = jnp.where(row == col, 1.0, 0.0).astype(F32)
    size = 1
    while size < chunk:
        joined = ((row // (2 * size)) == (col // (2 * size))) & ((row // size) > (col // size))
        part = jnp.where(joined, a_ub, 0.0)
        if size == 1:
            inverse = inverse - part
        else:
            inv = split2(inverse)
            inverse = inverse - dot3(split2(dot3(inv, blocked(split2(part)), NN)), blocked(inv), NN)
        size *= 2
    inverse = split2(inverse)

    value = v_ref[...]
    (values,) = blocked((value,))
    trans = split2(dot3(inverse, blocked(split2(unit * jnp.exp(before))), NN))
    own = split2(dot3(inverse, blocked(split2(exact(a_uk, values))), NN))
    read = split2(query * jnp.exp(cum) - dot3(a_qb, blocked(trans), NN))
    out_own = exact(a_qk, values) - dot3(a_qb, blocked(own), NN)
    base_last = split2(base * to_last)
    key_last = split2(key * to_last)
    move = jnp.where(big_r == big_c, jnp.exp(last), 0.0) - jnp.where(same, dot3(base_last, trans, TN), 0.0)
    end = dot(key_last[0], value, TN) + dot(key_last[1], value, TN) - dot3(base_last, own, TN)

    zm, ze = split2(zm_ref[...]), split2(ze_ref[...])
    read_ref[...] = dot3(read, zm, NN)
    own_ref[...] = out_own + dot3(read, ze, NN)
    move = split2(move)
    zm_ref[...] = dot3(move, zm, NN)
    ze_ref[...] = dot3(move, ze, NN) + jnp.where(same, end, 0.0)


def layer_kernel(
    chunk, q_hbm, k_hbm, v_hbm, din_hbm, doff_hbm, extra_hbm, rin_hbm,
    roff_hbm, gain_hbm, resid_hbm, fgain_hbm, wo_hbm, gate_hbm, up_hbm, down_hbm, out_ref,
    q_ref, k_ref, v_ref, din_ref, doff_ref, extra_ref, rin_ref, roff_ref, gain_ref, resid_ref, fgain_ref,
    extra_wide, total_ref, other_ref, pair_ref, read_ref, own_ref, zm_ref, ze_ref, held, mixed, mixrow, wo, mid, tok, gate, up, down, hidden, near_sum, far_sum, y_out, y_in, z_out, z_in,
    in_sem, wo_sem, w_send, w_recv, c_send, c_recv, a_send, a_recv, t_send, t_recv, y_send, y_recv, z_send, z_recv,
):
    whole = (q_hbm, k_hbm, v_hbm, din_hbm, doff_hbm, extra_hbm, rin_hbm, roff_hbm, gain_hbm, resid_hbm, fgain_hbm)
    local = (q_ref, k_ref, v_ref, din_ref, doff_ref, extra_ref, rin_ref, roff_ref, gain_ref, resid_ref, fgain_ref)
    loads = [pltpu.make_async_copy(src, dst, in_sem.at[i]) for i, (src, dst) in enumerate(zip(whole, local))]
    for load in loads:
        load.start()
    z, x, y, c = (lax.axis_index(name) for name in ("z", "x", "y", "c"))
    half, low = z // 2, lax.rem(z, 2)
    sib = z + 1 - 2 * low
    pair = lax.rem(z + 2, 4)
    near = 1 + half
    mine = c == half
    me = 2 * z + x
    n = 8
    depth = gate_hbm.shape[0]
    width = q_ref.shape[1]
    heads = width // HEAD
    rows = resid_ref.shape[0]
    model = resid_ref.shape[1]
    cut = down_hbm.shape[0] // 2
    sources = (gate_hbm, up_hbm, down_hbm.at[pl.ds(0, cut), :], down_hbm.at[pl.ds(cut, cut), :])

    def at(index, size):
        return pl.ds(pl.multiple_of(index * size, size), size)

    def remote(src, dst, send, recv, **where):
        return pltpu.make_async_remote_copy(
            src_ref=src, dst_ref=dst, send_sem=send, recv_sem=recv, device_id=where, device_id_type=MESH)

    def piece(m, s):
        if m < 2:
            return (gate, up)[m].at[at(s, depth), :]
        return down.at[pl.ds((m - 2) * cut, cut), at(s, depth)]

    def to(src, m, s, slot, **where):
        return remote(src, piece(m, s), w_send.at[m, slot], w_recv.at[m, s], **where)

    def landed(m, s):
        to(piece(m, s), m, s, 0, c=1 - c).wait_recv()

    def down_landed(s):
        landed(2, s)
        landed(3, s)

    def own(m):
        return pltpu.make_async_copy(sources[m], piece(m, me), w_recv.at[m, me])

    def side_sends(m):
        src = sources[m]
        return ((mine, (to(src, m, me, 1, x=1 - x), to(src, m, me, 2, c=1 - c))),)

    def line_sends(m):
        src = sources[m]
        return (
            (mine, (to(src, m, me, 0, z=sib, c=1 - half),)),
            (jnp.logical_not(mine), (to(src, m, me, 3, z=1 + c, c=low),)),
        )

    first = jnp.where(mine, z, sib)
    second = 2 * (1 - half) + c
    other_first = jnp.where(mine, sib, z)
    other_second = 2 * (1 - half) + 1 - c

    swapped = jnp.logical_and(z == near, c != half)
    early, late = jnp.where(swapped, second, first), jnp.where(swapped, first, second)
    other_swapped = jnp.logical_and(z == near, mine)
    other_early, other_late = jnp.where(other_swapped, other_second, other_first), jnp.where(other_swapped, other_first, other_second)

    def relay(m, step):
        s = 2 * (first, second, *((early, late) if m >= 2 else (first, second)))[step] + (x, x, 1 - x, 1 - x)[step]
        p = piece(m, s)
        if step == 0:
            return s, ((jnp.logical_not(mine), (to(p, m, s, 4, x=1 - x), to(p, m, s, 5, c=1 - c))),)
        if step == 1:
            return s, (
                (z == near, (to(p, m, s, 6, z=3 * half),)),
                (None, (to(p, m, s, 7, x=1 - x), to(p, m, s, 8, c=1 - c))),
            )
        return s, ((None, (to(p, m, s, 7 + step, c=1 - c),)),)

    def each(groups, act):
        for when, copies in groups:
            if when is None:
                for copy in copies:
                    act(copy)
            else:
                @pl.when(when)
                def _():
                    for copy in copies:
                        act(copy)

    def start(copy):
        copy.start()

    def begin(m):
        @pl.when(mine)
        def _():
            own(m).start()
        each(side_sends(m), start)

    def pump(m, step):
        s, groups = relay(m, step)
        landed(m, s)
        each(groups, start)

    def pump_far(m):
        s, groups = relay(m, 1)
        landed(m, s)
        each(groups[:1], start)

    def pump_side(m):
        each(relay(m, 1)[1][1:], start)

    def rest_of(m):
        for plane in (other_first, other_second):
            for column in (x, 1 - x):
                landed(m, 2 * plane + column)

    def drain(m):
        for groups in (side_sends(m), line_sends(m), *(relay(m, step)[1] for step in range(4))):
            each(groups, lambda copy: copy.wait_send())

    barrier = pltpu.get_barrier_semaphore()
    for dz in range(4):
        for dx in range(2):
            for dy in range(2):
                for dc in range(2):
                    if dz or dx or dy or dc:
                        peer = {"z": lax.rem(z + dz, 4), "x": lax.rem(x + dx, 2), "y": lax.rem(y + dy, 2), "c": lax.rem(c + dc, 2)}
                        pl.semaphore_signal(barrier, inc=1, device_id=peer, device_id_type=MESH)
    pl.semaphore_wait(barrier, 31)

    load_wo = pltpu.make_async_copy(wo_hbm, wo, wo_sem)
    load_wo.start()

    def carry_copy(k):
        return remote(pair_ref, held.at[k], c_send.at[k], c_recv.at[k], z=lax.rem(z + k, 4))

    leftward = jnp.logical_or(z == 3, jnp.logical_and(c == 0, z >= 1))
    rightward = jnp.logical_not(leftward)
    is_near = z == near
    is_far = jnp.logical_not(is_near)
    is_last = z == 3
    not_mine = jnp.logical_not(mine)
    for m in range(2):
        each(line_sends(m), start)
        begin(m)

    @pl.when(jnp.logical_and(leftward, not_mine))
    def _():
        each(line_sends(2), start)
        each(line_sends(3), start)
    tokens = q_ref.shape[0]
    for load in loads:
        load.wait()
    spread_r = lax.broadcasted_iota(jnp.int32, (heads, width), 0)
    spread_c = lax.broadcasted_iota(jnp.int32, (heads, width), 1) // HEAD
    spread = jnp.where(spread_r == spread_c, 1.0, 0.0).astype(F32)
    extra_wide[...] = lax.dot_general(
        extra_ref[...], spread, (TN, ((), ())), precision=lax.Precision.HIGHEST, preferred_element_type=F32)

    big_r = lax.broadcasted_iota(jnp.int32, (width, width), 0)
    big_c = lax.broadcasted_iota(jnp.int32, (width, width), 1)
    blocks = jnp.where((big_r // HEAD) == (big_c // HEAD), 1.0, 0.0).astype(BF16)
    zm_ref[...] = jnp.where(big_r == big_c, 1.0, 0.0).astype(F32)
    ze_ref[...] = jnp.zeros_like(ze_ref)

    def advance(i, _):
        span = at(i, chunk)
        wide_step(
            heads, q_ref.at[span, :], k_ref.at[span, :], v_ref.at[span, :], din_ref.at[span, :], doff_ref,
            extra_wide.at[span, :], rin_ref.at[span, :], roff_ref, read_ref.at[span, :], own_ref.at[span, :], zm_ref, ze_ref)

        @pl.when(jnp.logical_and(i == 2, is_far))
        def _():
            pump(0, 0)

        @pl.when(jnp.logical_and(i == 3, is_near))
        def _():
            pump(0, 0)
            pump_far(0)

        @pl.when(jnp.logical_and(i == 3, jnp.logical_and(is_last, mine)))
        def _():
            each(line_sends(2), start)
            each(line_sends(3), start)

        return 0

    lax.fori_loop(0, tokens // chunk, advance, 0)

    for h in range(heads):
        span = slice(h * HEAD, (h + 1) * HEAD)
        total_ref[span, :] = jnp.concatenate([zm_ref[span, span], ze_ref[span, span]], axis=1).astype(BF16)
    swap = remote(total_ref, other_ref, c_send.at[0], c_recv.at[0], x=1 - x)
    swap.start()

    @pl.when(is_near)
    def _():
        pump_side(0)

    @pl.when(is_far)
    def _():
        pump(1, 0)
        begin(2)
    swap.wait_recv()

    def tall(block):
        return jnp.concatenate([block[:, :HEAD]] * heads, axis=1) * blocks

    ours, theirs = total_ref[...].astype(F32), other_ref[...].astype(F32)
    older, newer = jnp.where(x == 0, ours, theirs).astype(BF16), jnp.where(x == 0, theirs, ours).astype(BF16)
    joint = jnp.dot(tall(newer), older, preferred_element_type=F32)
    pair_ref[...] = (joint + jnp.where(
        lax.broadcasted_iota(jnp.int32, joint.shape, 1) >= HEAD, newer.astype(F32), 0.0)).astype(BF16)
    for k in range(1, 4):
        @pl.when(z + k < 4)
        def _():
            carry_copy(k).start()

    @pl.when(jnp.logical_and(rightward, not_mine))
    def _():
        each(line_sends(2), start)
        each(line_sends(3), start)

    @pl.when(jnp.logical_and(rightward, jnp.logical_and(mine, is_far)))
    def _():
        each(line_sends(2), start)
        each(line_sends(3), start)

    @pl.when(is_near)
    def _():
        pump(1, 0)
        pump(1, 1)

    @pl.when(jnp.logical_and(mine, is_near))
    def _():
        each(line_sends(2), start)
        each(line_sends(3), start)

    @pl.when(is_last)
    def _():
        pump(0, 1)
        begin(3)
    for k in range(1, 4):
        @pl.when(z >= k)
        def _():
            carry_copy(k).wait_recv()
    state = jnp.zeros((width, HEAD), F32)
    for there, block in [(z >= k, held[k]) for k in (3, 2, 1)] + [(x == 1, older)]:
        move = tall(block)
        high, rest = split2(state)
        moved = jnp.dot(move, high, preferred_element_type=F32) + jnp.dot(move, rest, preferred_element_type=F32)
        state = jnp.where(there, block[:, HEAD:].astype(F32) + moved, state)

    def head_mean(a):
        high, low_part = split2(a)
        return (jnp.dot(high, blocks, preferred_element_type=F32) + jnp.dot(low_part, blocks, preferred_element_type=F32)) / HEAD

    carried = tuple(tall(a) for a in split2(state))
    o = own_ref[...] + dot3(split2(read_ref[...]), carried, NN)
    center = o - head_mean(o)
    mixed[...] = (center * lax.rsqrt(head_mean(center * center) + 1e-5) * gain_ref[...]).astype(BF16)

    t = 2 * y + c

    def exchange(dy, dc):
        ty, tc = lax.rem(y + dy, 2), lax.rem(c + dc, 2)
        slot = 2 * dy + dc
        return remote(
            mixed.at[at(2 * ty + tc, rows), :], mixrow.at[:, at(t, width)], a_send.at[slot], a_recv.at[slot], y=ty, c=tc)

    swaps = [exchange(1, 0), exchange(1, 1), exchange(0, 1)]
    for copy in swaps:
        copy.start()
    mixrow[:, at(t, width)] = mixed[at(t, rows), :]


    @pl.when(z == 0)
    def _():
        pump(0, 1)
    load_wo.wait()
    for copy in swaps:
        copy.wait()

    tile = 512
    square = jnp.zeros((rows, 1), F32)
    for j in range(0, model, tile):
        proj = jnp.dot(mixrow[...], wo[:, j:j + tile], preferred_element_type=F32)
        part = (resid_ref[:, j:j + tile].astype(F32) + proj).astype(BF16).astype(F32)
        mid[:, j:j + tile] = part
        square += jnp.sum(part * part, axis=-1, keepdims=True)
    g = 2 * half + y
    g_far = 2 * (1 - half) + y
    g_side = 2 * half + 1 - y
    g_diag = 2 * (1 - half) + 1 - y
    tok[at(g, rows), :] = (mid[...] * lax.rsqrt(square / model + 1e-06) * fgain_ref[...]).astype(BF16)

    def rows_to(block, slot, **where):
        r = tok.at[at(block, rows), :]
        return remote(r, r, t_send.at[slot], t_recv.at[slot], **where)

    def rows_from(block, slot):
        r = tok.at[at(block, rows), :]
        remote(r, r, t_send.at[slot], t_recv.at[slot], y=1 - y).wait_recv()

    ahead = rows_to(g, 0, z=pair)
    beside = rows_to(g, 1, y=1 - y)
    onward = rows_to(g_far, 2, y=1 - y)
    beside.start()

    @pl.when(is_far)
    def _():
        ahead.start()

    @pl.when(is_far)
    def _():
        pump(1, 1)

    @pl.when(z == 0)
    def _():
        begin(3)
    pump(0, 2)
    pump(0, 3)

    @pl.when(is_near)
    def _():
        ahead.start()

    @pl.when(z == 1)
    def _():
        pump_far(2)
        pump_far(3)
    rows_from(g_far, 0)
    onward.start()
    pump(1, 2)

    @pl.when(is_near)
    def _():
        begin(2)
        begin(3)

    @pl.when(z == 1)
    def _():
        pump_side(2)
        pump_side(3)

    @pl.when(z == 2)
    def _():
        pump(2, 1)
        pump(3, 1)

    @pl.when(is_near)
    def _():
        pump(2, 0)
        pump(3, 0)

    pump(1, 3)

    @pl.when(is_far)
    def _():
        pump(2, 0)

    @pl.when(is_last)
    def _():
        pump(3, 0)

    rest_of(0)
    rest_of(1)
    rows_from(g_side, 1)
    rows_from(g_diag, 2)

    units = gate.shape[1]
    for j in range(0, units, 256):
        cols = slice(j, min(j + 256, units))
        gated = jnp.dot(tok[...], gate[:, cols], preferred_element_type=F32)
        upper = jnp.dot(tok[...], up[:, cols], preferred_element_type=F32)
        hidden[:, cols] = (gated * jax.nn.sigmoid(gated) * upper).astype(BF16)

    def side_copy(i, b):
        return remote(y_out.at[i, b], y_in.at[i, b], y_send.at[i, b], y_recv.at[i, b], y=1 - y)

    def far_copy(i):
        return remote(z_out.at[i], z_in.at[i], z_send.at[i], z_recv.at[i], z=pair)

    def slices_of(column, plane, other):
        for b, block_half, sums in ((0, 1 - half, far_sum), (1, half, near_sum)):
            for k, source in enumerate((plane, other)):
                i = 2 * source + column
                if b == 0 and k == 1:
                    down_landed(i)
                sums[:, at(i, depth)] = jnp.dot(
                    hidden[at(block_half, 2 * rows), :], down[:, at(i, depth)], preferred_element_type=F32)
                y_out[i, b] = sums[at(1 - y, rows), at(i, depth)].astype(BF16)
                side_copy(i, b).start()

    def pass_on(plane, column):
        i = 2 * plane + column
        side_copy(i, 0).wait_recv()
        z_out[i] = (far_sum[at(y, rows), at(i, depth)] + y_in[i, 0].astype(F32)).astype(BF16)
        far_copy(i).start()

    next_first, next_other = jnp.where(is_far, first, second), jnp.where(is_far, other_first, other_second)
    next_column = jnp.where(is_far, 1 - x, x)
    then_first, then_other = jnp.where(is_far, second, early), jnp.where(is_far, other_second, other_early)
    then_column = jnp.where(is_far, x, 1 - x)

    @pl.when(z == 0)
    def _():
        pump(3, 0)

    @pl.when(is_far)
    def _():
        pump(2, 1)
    slices_of(x, first, other_first)

    @pl.when(z == 0)
    def _():
        pump(3, 1)

    @pl.when(is_far)
    def _():
        pump(2, 2)
        pump(3, 2)
    slices_of(next_column, next_first, next_other)
    pass_on(first, x)
    pass_on(other_first, x)

    @pl.when(is_last)
    def _():
        pump(3, 1)
    drain(0)
    drain(1)
    swap.wait_send()
    for k in range(1, 4):
        @pl.when(z + k < 4)
        def _():
            carry_copy(k).wait_send()

    @pl.when(is_near)
    def _():
        pump(2, 2)
        pump(3, 2)
    slices_of(then_column, then_first, then_other)
    pass_on(next_first, next_column)
    pass_on(next_other, next_column)
    pass_on(then_first, then_column)
    pass_on(then_other, then_column)
    pump(2, 3)
    pump(3, 3)
    slices_of(1 - x, late, other_late)
    pass_on(late, 1 - x)
    pass_on(other_late, 1 - x)
    for i in range(n):
        cols = slice(i * depth, (i + 1) * depth)
        side_copy(i, 1).wait_recv()
        far_copy(i).wait_recv()
        total = near_sum[at(y, rows), cols] + y_in[i, 1].astype(F32) + z_in[i].astype(F32)
        out_ref[:, cols] = (mid[:, cols] + 0.5 * total).astype(BF16)

    drain(2)
    drain(3)
    for copy in (ahead, beside, onward):
        copy.wait_send()
    for i in range(n):
        side_copy(i, 0).wait_send()
        side_copy(i, 1).wait_send()
        far_copy(i).wait_send()


def layer(q, k, v, din, doff, extra, rin, roff, gain, resid, fgain, wo, gate, up, down):
    tokens, width = q.shape
    heads = width // HEAD
    chunk = 64
    while tokens % chunk:
        chunk //= 2
    rows, model = resid.shape
    depth, units = gate.shape
    n = 8
    vm = pl.BlockSpec(memory_space=pltpu.VMEM)
    hbm = pl.BlockSpec(memory_space=pl.ANY)
    dma = pltpu.SemaphoreType.DMA
    inputs = (
        q, k, v, din, doff.reshape(1, width), extra.T, rin, roff.reshape(1, width), gain.reshape(1, width), resid, fgain.reshape(1, model))
    return pl.pallas_call(
        functools.partial(layer_kernel, chunk),
        in_specs=[hbm] * 15,
        out_specs=vm,
        out_shape=pltpu.VMEM((rows, model), BF16),
        scratch_shapes=[pltpu.VMEM(a.shape, a.dtype) for a in inputs] + [
            pltpu.VMEM((tokens, width), F32),
            pltpu.VMEM((width, 2 * HEAD), BF16),
            pltpu.VMEM((width, 2 * HEAD), BF16),
            pltpu.VMEM((width, 2 * HEAD), BF16),
            pltpu.VMEM((tokens, width), F32),
            pltpu.VMEM((tokens, width), F32),
            pltpu.VMEM((width, width), F32),
            pltpu.VMEM((width, width), F32),
            pltpu.VMEM((4, width, 2 * HEAD), BF16),
            pltpu.VMEM((tokens, width), BF16),
            pltpu.VMEM((rows, wo.shape[0]), BF16),
            pltpu.VMEM(wo.shape, BF16),
            pltpu.VMEM((rows, model), F32),
            pltpu.VMEM((4 * rows, model), BF16),
            pltpu.VMEM((n * depth, units), BF16),
            pltpu.VMEM((n * depth, units), BF16),
            pltpu.VMEM((units, n * depth), BF16),
            pltpu.VMEM((4 * rows, units), BF16),
            pltpu.VMEM((2 * rows, model), F32),
            pltpu.VMEM((2 * rows, model), F32),
            pltpu.VMEM((n, 2, rows, depth), BF16),
            pltpu.VMEM((n, 2, rows, depth), BF16),
            pltpu.VMEM((n, rows, depth), BF16),
            pltpu.VMEM((n, rows, depth), BF16),
            dma((11,)), dma, dma((4, 11)), dma((4, n)), dma((4,)), dma((4,)), dma((4,)), dma((4,)), dma((3,)), dma((3,)),
            dma((n, 2)), dma((n, 2)), dma((n,)), dma((n,)),
        ],
        compiler_params=pltpu.CompilerParams(collective_id=2, has_side_effects=True, vmem_limit_bytes=67043328 - 2 * rows * model),
    )(*inputs, wo, gate, up, down)


def per_device_pairs(
    resid, queries, keys, values, decay_input_part, decay_channel_offset, decay_head_extra,
    correction_rate_input, correction_rate_offset, head_norm_gain, mixer_output_weight,
    feedforward_norm_gain, gate_weight, up_weight, down_weight,
):
    return layer(
        queries, keys, values, decay_input_part, decay_channel_offset, decay_head_extra,
        correction_rate_input, correction_rate_offset, head_norm_gain, resid, feedforward_norm_gain, mixer_output_weight, gate_weight, up_weight, down_weight)


def solution(mesh):
    n_sp, n_tp = mesh.shape["sp"], mesh.shape["tp"]
    if (n_sp, n_tp) == (8, 4):
        inner = Mesh(mesh.devices.reshape(4, 2, 2, 2), ("z", "x", "y", "c"))
        sp, tp = ("z", "x"), ("y", "c")
        body = per_device_pairs
    else:
        nx = 2 if n_sp % 2 == 0 else 1
        nz = n_sp // nx
        inner = Mesh(mesh.devices.reshape(nz, nx, n_tp), ("z", "x", "tp"))
        sp, tp = ("z", "x"), ("tp",)
        body = functools.partial(per_device, nz, nx)
    rows = P((*sp, *tp), None)
    placed = (
        rows, P(sp, tp), P(sp, tp), P(sp, tp), P(sp, tp), P(tp), P(sp, tp), P(sp, tp), P(tp), P(tp), P(), P(),
        P(sp, tp), P(sp, tp), P(tp, sp),
    )
    return jax.shard_map(body, mesh=inner, in_specs=placed, out_specs=rows, check_vma=False)
```

```python
import functools
import math

import jax
import jax.numpy as jnp
from jax import lax
from jax.experimental import pallas as pl
from jax.experimental.pallas import tpu as pltpu
from jax.sharding import Mesh, PartitionSpec as P

HEAD = 64
F32 = jnp.float32
BF16 = jnp.bfloat16


def split2(a):
    high = a.astype(BF16)
    return high, (a - high.astype(F32)).astype(BF16)


def dot3(a, b, dims):
    (ah, al), (bh, bl) = a, b
    dn = (dims, ((), ()))
    d = functools.partial(lax.dot_general, dimension_numbers=dn, preferred_element_type=F32)
    return d(ah, bh) + (d(ah, bl) + d(al, bh))


NN = ((1,), (0,))
NT = ((1,), (1,))
TN = ((0,), (0,))


def chunk_kernel(heads, chunk, *refs):
    chunk_step(heads, chunk, pl.program_id(0), *refs)


def chunk_step(heads, chunk, step, q_ref, k_ref, v_ref, din_ref, doff_ref, extra_ref, rin_ref, roff_ref, reads_ref, total_ref, z_ref):
    rows = q_ref.shape[0]
    width = heads * HEAD
    wide = heads * chunk

    @pl.when(step == 0)
    def _():
        r = lax.broadcasted_iota(jnp.int32, (width, 2 * HEAD), 0) % HEAD
        c = lax.broadcasted_iota(jnp.int32, (width, 2 * HEAD), 1)
        z_ref[...] = jnp.where(r == c, 1.0, 0.0).astype(F32)

    def load(ref):
        return ref[...].astype(F32)

    def stack(a):
        return jnp.concatenate([a[:, h * HEAD:(h + 1) * HEAD] for h in range(heads)], axis=0)

    spread_r = lax.broadcasted_iota(jnp.int32, (heads, width), 0)
    spread_c = lax.broadcasted_iota(jnp.int32, (heads, width), 1) // HEAD
    spread = jnp.where(spread_r == spread_c, 1.0, 0.0).astype(F32)
    extra = extra_ref[...]
    if extra.shape[1] == heads:
        extra = lax.dot_general(extra, spread, ((((1,), (0,))), ((), ())), precision=lax.Precision.HIGHEST, preferred_element_type=F32)
    log_decay = -jax.nn.sigmoid(load(din_ref) + doff_ref[...]) * math.exp(-0.5) - extra
    tr = lax.broadcasted_iota(jnp.int32, (chunk, chunk), 0)
    tc = lax.broadcasted_iota(jnp.int32, (chunk, chunk), 1)
    lower = jnp.where(tr >= tc, 1.0, 0.0).astype(F32)
    cum = lax.dot_general(lower, log_decay, (((1,), (0,)), ((), ())), precision=lax.Precision.HIGHEST, preferred_element_type=F32)
    last = cum[chunk - 1:chunk, :]
    mid = cum[chunk // 2 - 1:chunk // 2, :]
    before = cum - log_decay
    rate = jax.nn.sigmoid(load(rin_ref) + roff_ref[...])

    key = stack(load(k_ref))
    unit = key * lax.rsqrt(jnp.sum(key * key, axis=-1, keepdims=True) + 1e-6)
    base = unit * stack(rate)
    query = stack(load(q_ref))
    value = split2(stack(load(v_ref)))
    to_mid = stack(jnp.exp(mid - cum))
    key_mid = split2(key * to_mid)
    base_mid = split2(base * to_mid)
    query_mid = split2(query * stack(jnp.exp(cum - mid)))
    unit_mid = split2(unit * stack(jnp.exp(before - mid)))
    to_last = stack(jnp.exp(last - cum))

    row = lax.broadcasted_iota(jnp.int32, (wide, wide), 0)
    col = lax.broadcasted_iota(jnp.int32, (wide, wide), 1)
    same = (row // chunk) == (col // chunk)
    strict = same & (row > col)
    upto = same & (row >= col)
    a_ub = jnp.where(strict, dot3(unit_mid, base_mid, NT), 0.0)
    a_uk = jnp.where(strict, dot3(unit_mid, key_mid, NT), 0.0)
    a_qb = jnp.where(upto, dot3(query_mid, base_mid, NT), 0.0)
    a_qk = jnp.where(upto, dot3(query_mid, key_mid, NT), 0.0)

    inverse = jnp.where(row == col, 1.0, 0.0).astype(F32)
    size = 1
    while size < chunk:
        pair = ((row // (2 * size)) == (col // (2 * size))) & ((row // size) > (col // size))
        part = jnp.where(pair, a_ub, 0.0)
        if size == 1:
            inverse = inverse - part
        else:
            inv = split2(inverse)
            inverse = inverse - dot3(split2(dot3(inv, split2(part), NN)), inv, NN)
        size *= 2
    inverse = split2(inverse)

    wr = lax.broadcasted_iota(jnp.int32, (wide, width), 0) // chunk
    wc = lax.broadcasted_iota(jnp.int32, (wide, width), 1) // HEAD

    def spread_wide(a):
        return jnp.where(wr == wc, jnp.concatenate([a] * heads, axis=1), 0.0)

    unit_wide = split2(spread_wide(unit * stack(jnp.exp(before))))
    query_wide = spread_wide(query * stack(jnp.exp(cum)))
    base_wide = split2(spread_wide(base * to_last))
    key_wide = split2(spread_wide(key * to_last))
    qb = split2(a_qb)
    trans = split2(dot3(inverse, unit_wide, NN))
    own = split2(dot3(inverse, split2(dot3(split2(a_uk), value, NN)), NN))
    read = split2(query_wide - dot3(qb, trans, NN))
    out_own = dot3(split2(a_qk), value, NN) - dot3(qb, own, NN)
    pr = lax.broadcasted_iota(jnp.int32, (width, width), 0)
    pc = lax.broadcasted_iota(jnp.int32, (width, width), 1)
    move = jnp.where(pr == pc, jnp.exp(last), 0.0) - dot3(base_wide, trans, TN)
    end = dot3(key_wide, value, TN) - dot3(base_wide, own, TN)

    z = split2(z_ref[...])
    x = dot3(read, z, NN) + jnp.concatenate([jnp.zeros_like(out_own), out_own], axis=1)
    for h in range(heads):
        reads_ref[h] = x[h * chunk:(h + 1) * chunk, :]
    z_new = dot3(split2(move), z, NN) + jnp.concatenate([jnp.zeros_like(end), end], axis=1)
    z_ref[...] = z_new
    total_ref[...] = z_new.astype(BF16)


def chunks(q, k, v, din, doff, extra, rin, roff):
    rows, width = q.shape
    heads = width // HEAD
    chunk = 64
    while rows % chunk:
        chunk //= 2
    tile = pl.BlockSpec((chunk, width), lambda i: (i, 0))
    vec = pl.BlockSpec((1, width), lambda i: (0, 0))
    n = rows // chunk
    return pl.pallas_call(
        functools.partial(chunk_kernel, heads, chunk),
        grid=(n,),
        in_specs=[tile, tile, tile, tile, vec, pl.BlockSpec((chunk, heads), lambda i: (i, 0)), tile, vec],
        out_specs=(
            pl.BlockSpec((heads, chunk, 2 * HEAD), lambda i: (0, i, 0)),
            pl.BlockSpec((width, 2 * HEAD), lambda i: (0, 0)),
        ),
        out_shape=(
            jax.ShapeDtypeStruct((heads, rows, 2 * HEAD), F32),
            jax.ShapeDtypeStruct((width, 2 * HEAD), BF16),
        ),
        scratch_shapes=[pltpu.VMEM((width, 2 * HEAD), F32)],
        compiler_params=pltpu.CompilerParams(dimension_semantics=("arbitrary",), vmem_limit_bytes=40 * 2**20),
    )(q, k, v, din, doff.reshape(1, width), extra, rin, roff.reshape(1, width))


def carry_kernel(nz, nx, total_ref, reads_ref, gain_ref, mixed_ref, held, send_sem, recv_sem):
    n = nz * nx
    me = lax.axis_index("z") * nx + lax.axis_index("x")
    heads = reads_ref.shape[0]

    def place(k):
        peer = lax.rem(me + k, n)
        return {"z": peer // nx, "x": lax.rem(peer, nx)}

    barrier = pltpu.get_barrier_semaphore()
    for k in range(1, n):
        pl.semaphore_signal(barrier, inc=1, device_id=place(k), device_id_type=pl.DeviceIdType.MESH)
    pl.semaphore_wait(barrier, n - 1)
    copies = []
    for k in range(1, n):
        c = pltpu.make_async_remote_copy(
            src_ref=total_ref, dst_ref=held.at[k], send_sem=send_sem.at[k], recv_sem=recv_sem.at[k],
            device_id=place(k), device_id_type=pl.DeviceIdType.MESH)
        c.start()
        copies.append(c)
    for c in copies:
        c.wait()
    state = [jnp.zeros((HEAD, HEAD), F32) for _ in range(heads)]
    for k in range(n - 1, 0, -1):
        there = k <= me
        for h in range(heads):
            block = held[k, h * HEAD:(h + 1) * HEAD, :].astype(F32)
            new = block[:, HEAD:] + jnp.dot(block[:, :HEAD], state[h], precision=lax.Precision.HIGHEST, preferred_element_type=F32)
            state[h] = jnp.where(there, new, state[h])
    outs = []
    for h in range(heads):
        x = reads_ref[h]
        o = x[:, HEAD:] + dot3(split2(x[:, :HEAD]), split2(state[h]), NN)
        center = o - jnp.mean(o, axis=-1, keepdims=True)
        var = jnp.mean(center * center, axis=-1, keepdims=True)
        outs.append(center * lax.rsqrt(var + 1e-5))
    mixed_ref[...] = (jnp.concatenate(outs, axis=1) * gain_ref[...]).astype(BF16)


def carry(total, reads, gain, nz, nx):
    heads, rows, _ = reads.shape
    width = heads * HEAD
    n = nz * nx
    vm = pl.BlockSpec(memory_space=pltpu.VMEM)
    return pl.pallas_call(
        functools.partial(carry_kernel, nz, nx),
        in_specs=[vm, vm, vm],
        out_specs=vm,
        out_shape=jax.ShapeDtypeStruct((rows, width), BF16),
        scratch_shapes=[
            pltpu.VMEM((n, width, 2 * HEAD), BF16),
            pltpu.SemaphoreType.DMA((n,)),
            pltpu.SemaphoreType.DMA((n,)),
        ],
        compiler_params=pltpu.CompilerParams(collective_id=1, has_side_effects=True, vmem_limit_bytes=24 * 2**20),
    )(total, reads, gain.reshape(1, width))


def send_z(block, nz):
    return [lax.ppermute(block, "z", [(s, (s + k) % nz) for s in range(nz)]) for k in range(1, nz)]


def in_order(block, came, nz, axis):
    z = lax.axis_index("z")
    size = block.shape[axis]
    shape = list(block.shape)
    shape[axis] = size * nz
    whole = jnp.zeros(shape, block.dtype)
    whole = lax.dynamic_update_slice_in_dim(whole, block, z * size, axis)
    for k in range(1, nz):
        whole = lax.dynamic_update_slice_in_dim(whole, came[k - 1], lax.rem(z - k + nz, nz) * size, axis)
    return whole


def per_device(
    nz, nx,
    resid, queries, keys, values, decay_input_part, decay_channel_offset, decay_head_extra,
    correction_rate_input, correction_rate_offset, head_norm_gain, mixer_output_weight,
    feedforward_norm_gain, gate_weight, up_weight, down_weight,
):
    ff = gate_weight.shape[1] // nx
    x = lax.axis_index("x")

    def exchange(weight, axis, join):
        pieces = weight.reshape(weight.shape[:axis] + (nx, ff) + weight.shape[axis + 1:])
        return lax.all_to_all(pieces, "x", split_axis=axis, concat_axis=join, tiled=False)

    def swap(weight, axis, join):
        if nx == 1:
            return weight
        if nx != 2:
            out = exchange(weight, axis, join)
            return out.reshape((-1, ff) if axis == 1 else (ff, -1))
        mine = lax.dynamic_slice_in_dim(weight, x * ff, ff, axis)
        other = lax.dynamic_slice_in_dim(weight, (1 - x) * ff, ff, axis)
        came = lax.ppermute(other, "x", [(0, 1), (1, 0)])
        first = jnp.where(x == 0, mine, came)
        second = jnp.where(x == 0, came, mine)
        return jnp.concatenate([first, second], axis=join)

    halves = (swap(gate_weight, 1, 0), swap(up_weight, 1, 0), swap(down_weight, 0, 1))
    halves, queries = lax.optimization_barrier((halves, queries))
    whole_gate = lax.all_gather(halves[0], "z", axis=0, tiled=True)
    up_came = send_z(halves[1], nz)
    down_came = send_z(halves[2], nz)

    reads, total = chunks(
        queries, keys, values, decay_input_part, decay_channel_offset, decay_head_extra,
        correction_rate_input, correction_rate_offset)
    total, up_came = lax.optimization_barrier((total, up_came))
    mixed = carry(total, reads, head_norm_gain, nz, nx)
    row_mixed = lax.all_to_all(mixed, "tp", split_axis=0, concat_axis=1, tiled=True)
    proj = jnp.dot(row_mixed, mixer_output_weight, preferred_element_type=F32)
    mid_f = (resid.astype(F32) + proj).astype(BF16).astype(F32)
    normed = (
        mid_f
        * lax.rsqrt(jnp.mean(mid_f * mid_f, axis=-1, keepdims=True) + 1e-06)
        * feedforward_norm_gain
    ).astype(BF16)
    normed, whole_gate = lax.optimization_barrier((normed, whole_gate))
    whole_up = in_order(halves[1], up_came, nz, 0)
    whole_down = in_order(halves[2], down_came, nz, 1)
    whole_rows = lax.all_gather(normed, ("x", "tp"), axis=0, tiled=True)
    gate = jnp.dot(whole_rows, whole_gate, preferred_element_type=F32)
    upper = jnp.dot(whole_rows, whole_up, preferred_element_type=F32)
    hidden = (jax.nn.silu(gate) * upper).astype(BF16)
    down_sum = lax.psum_scatter(
        jnp.dot(hidden, whole_down, preferred_element_type=F32).astype(BF16),
        ("x", "tp"), scatter_dimension=0, tiled=True,
    ).astype(F32)
    return (mid_f + 0.5 * down_sum).astype(BF16)


MESH = pl.DeviceIdType.MESH


def wide_step(heads, q_ref, k_ref, v_ref, din_ref, doff_ref, extra_ref, rin_ref, roff_ref, read_ref, own_ref, zm_ref, ze_ref):
    chunk = q_ref.shape[0]
    width = heads * HEAD

    def load(ref):
        return ref[...].astype(F32)

    def dot(a, b, dims=NN):
        return lax.dot_general(a, b, (dims, ((), ())), preferred_element_type=F32)

    big_r = lax.broadcasted_iota(jnp.int32, (width, width), 0)
    big_c = lax.broadcasted_iota(jnp.int32, (width, width), 1)
    same = (big_r // HEAD) == (big_c // HEAD)
    blocks = jnp.where(same, 1.0, 0.0).astype(BF16)

    def blocked(pair):
        return tuple(jnp.concatenate([a] * heads, axis=0) * blocks for a in pair)

    def exact(pair, b):
        return dot(pair[0], b) + dot(pair[1], b)

    key = load(k_ref)
    unit = key * lax.rsqrt(exact(split2(key * key), blocks) + 1e-6)
    base = unit * jax.nn.sigmoid(load(rin_ref) + roff_ref[...])
    query = load(q_ref)
    log_decay = -jax.nn.sigmoid(load(din_ref) + doff_ref[...]) * math.exp(-0.5) - extra_ref[...]
    tr = lax.broadcasted_iota(jnp.int32, (chunk, chunk), 0)
    tc = lax.broadcasted_iota(jnp.int32, (chunk, chunk), 1)
    lower = jnp.where(tr >= tc, 1.0, 0.0).astype(BF16)
    ld_high, ld_rest = split2(log_decay)
    ld_mid, ld_low = split2(log_decay - ld_high.astype(F32))
    cum = dot(lower, ld_high) + (dot(lower, ld_mid) + dot(lower, ld_low))
    last = cum[chunk - 1:chunk, :]
    mid = cum[chunk // 2 - 1:chunk // 2, :]
    before = cum - log_decay
    to_mid = jnp.exp(mid - cum)
    to_last = jnp.exp(last - cum)
    key_mid = blocked(split2(key * to_mid))
    base_mid = blocked(split2(base * to_mid))
    left = split2(jnp.concatenate([unit * jnp.exp(before - mid), query * jnp.exp(cum - mid)], axis=0))
    by_base = dot3(left, base_mid, NT)
    by_key = dot3(left, key_mid, NT)
    row = lax.broadcasted_iota(jnp.int32, (chunk, width), 0)
    col = lax.rem(lax.broadcasted_iota(jnp.int32, (chunk, width), 1), HEAD)
    a_ub = jnp.where(row > col, by_base[:chunk], 0.0)
    a_uk = split2(jnp.where(row > col, by_key[:chunk], 0.0))
    a_qb = split2(jnp.where(row >= col, by_base[chunk:], 0.0))
    a_qk = split2(jnp.where(row >= col, by_key[chunk:], 0.0))

    inverse = jnp.where(row == col, 1.0, 0.0).astype(F32)
    size = 1
    while size < chunk:
        joined = ((row // (2 * size)) == (col // (2 * size))) & ((row // size) > (col // size))
        part = jnp.where(joined, a_ub, 0.0)
        if size == 1:
            inverse = inverse - part
        else:
            inv = split2(inverse)
            inverse = inverse - dot3(split2(dot3(inv, blocked(split2(part)), NN)), blocked(inv), NN)
        size *= 2
    inverse = split2(inverse)

    value = v_ref[...]
    (values,) = blocked((value,))
    trans = split2(dot3(inverse, blocked(split2(unit * jnp.exp(before))), NN))
    own = split2(dot3(inverse, blocked(split2(exact(a_uk, values))), NN))
    read = split2(query * jnp.exp(cum) - dot3(a_qb, blocked(trans), NN))
    out_own = exact(a_qk, values) - dot3(a_qb, blocked(own), NN)
    base_last = split2(base * to_last)
    key_last = split2(key * to_last)
    move = jnp.where(big_r == big_c, jnp.exp(last), 0.0) - jnp.where(same, dot3(base_last, trans, TN), 0.0)
    end = dot(key_last[0], value, TN) + dot(key_last[1], value, TN) - dot3(base_last, own, TN)

    zm, ze = split2(zm_ref[...]), split2(ze_ref[...])
    read_ref[...] = dot3(read, zm, NN)
    own_ref[...] = out_own + dot3(read, ze, NN)
    move = split2(move)
    zm_ref[...] = dot3(move, zm, NN)
    ze_ref[...] = dot3(move, ze, NN) + jnp.where(same, end, 0.0)


def layer_kernel(
    chunk, q_hbm, k_hbm, v_hbm, din_hbm, doff_hbm, extra_hbm, rin_hbm,
    roff_hbm, gain_hbm, resid_hbm, fgain_hbm, wo_hbm, gate_hbm, up_hbm, down_hbm, out_ref,
    q_ref, k_ref, v_ref, din_ref, doff_ref, extra_ref, rin_ref, roff_ref, gain_ref, resid_ref, fgain_ref,
    extra_wide, total_ref, other_ref, pair_ref, read_ref, own_ref, zm_ref, ze_ref, held, mixed, mixrow, wo, mid, tok, gate, up, down, hidden, near_sum, far_sum, y_out, y_in, z_out, z_in,
    in_sem, wo_sem, w_send, w_recv, c_send, c_recv, a_send, a_recv, t_send, t_recv, y_send, y_recv, z_send, z_recv,
):
    whole = (q_hbm, k_hbm, v_hbm, din_hbm, doff_hbm, extra_hbm, rin_hbm, roff_hbm, gain_hbm, resid_hbm, fgain_hbm)
    local = (q_ref, k_ref, v_ref, din_ref, doff_ref, extra_ref, rin_ref, roff_ref, gain_ref, resid_ref, fgain_ref)
    loads = [pltpu.make_async_copy(src, dst, in_sem.at[i]) for i, (src, dst) in enumerate(zip(whole, local))]
    for load in loads:
        load.start()
    z, x, y, c = (lax.axis_index(name) for name in ("z", "x", "y", "c"))
    half, low = z // 2, lax.rem(z, 2)
    sib = z + 1 - 2 * low
    pair = lax.rem(z + 2, 4)
    near = 1 + half
    mine = c == half
    me = 2 * z + x
    n = 8
    depth = gate_hbm.shape[0]
    width = q_ref.shape[1]
    heads = width // HEAD
    rows = resid_ref.shape[0]
    model = resid_ref.shape[1]
    cut = down_hbm.shape[0] // 2
    sources = (gate_hbm, up_hbm, down_hbm.at[pl.ds(0, cut), :], down_hbm.at[pl.ds(cut, cut), :])

    def at(index, size):
        return pl.ds(pl.multiple_of(index * size, size), size)

    def remote(src, dst, send, recv, **where):
        return pltpu.make_async_remote_copy(
            src_ref=src, dst_ref=dst, send_sem=send, recv_sem=recv, device_id=where, device_id_type=MESH)

    def piece(m, s):
        if m < 2:
            return (gate, up)[m].at[at(s, depth), :]
        return down.at[pl.ds((m - 2) * cut, cut), at(s, depth)]

    def to(src, m, s, slot, **where):
        return remote(src, piece(m, s), w_send.at[m, slot], w_recv.at[m, s], **where)

    def landed(m, s):
        to(piece(m, s), m, s, 0, c=1 - c).wait_recv()

    def down_landed(s):
        landed(2, s)
        landed(3, s)

    def own(m):
        return pltpu.make_async_copy(sources[m], piece(m, me), w_recv.at[m, me])

    def side_sends(m):
        src = sources[m]
        return ((mine, (to(src, m, me, 1, x=1 - x), to(src, m, me, 2, c=1 - c))),)

    def line_sends(m):
        src = sources[m]
        return (
            (mine, (to(src, m, me, 0, z=sib, c=1 - half),)),
            (jnp.logical_not(mine), (to(src, m, me, 3, z=1 + c, c=low),)),
        )

    first = jnp.where(mine, z, sib)
    second = 2 * (1 - half) + c
    other_first = jnp.where(mine, sib, z)
    other_second = 2 * (1 - half) + 1 - c

    swapped = jnp.logical_and(z == near, c != half)
    early, late = jnp.where(swapped, second, first), jnp.where(swapped, first, second)
    other_swapped = jnp.logical_and(z == near, mine)
    other_early, other_late = jnp.where(other_swapped, other_second, other_first), jnp.where(other_swapped, other_first, other_second)

    def relay(m, step):
        s = 2 * (first, second, *((early, late) if m >= 2 else (first, second)))[step] + (x, x, 1 - x, 1 - x)[step]
        p = piece(m, s)
        if step == 0:
            return s, ((jnp.logical_not(mine), (to(p, m, s, 4, x=1 - x), to(p, m, s, 5, c=1 - c))),)
        if step == 1:
            return s, (
                (z == near, (to(p, m, s, 6, z=3 * half),)),
                (None, (to(p, m, s, 7, x=1 - x), to(p, m, s, 8, c=1 - c))),
            )
        return s, ((None, (to(p, m, s, 7 + step, c=1 - c),)),)

    def each(groups, act):
        for when, copies in groups:
            if when is None:
                for copy in copies:
                    act(copy)
            else:
                @pl.when(when)
                def _():
                    for copy in copies:
                        act(copy)

    def start(copy):
        copy.start()

    def begin(m):
        @pl.when(mine)
        def _():
            own(m).start()
        each(side_sends(m), start)

    def pump(m, step):
        s, groups = relay(m, step)
        landed(m, s)
        each(groups, start)

    def pump_far(m):
        s, groups = relay(m, 1)
        landed(m, s)
        each(groups[:1], start)

    def pump_side(m):
        each(relay(m, 1)[1][1:], start)

    def rest_of(m):
        for plane in (other_first, other_second):
            for column in (x, 1 - x):
                landed(m, 2 * plane + column)

    def drain(m):
        for groups in (side_sends(m), line_sends(m), *(relay(m, step)[1] for step in range(4))):
            each(groups, lambda copy: copy.wait_send())

    barrier = pltpu.get_barrier_semaphore()
    for dz in range(4):
        for dx in range(2):
            for dy in range(2):
                for dc in range(2):
                    if dz or dx or dy or dc:
                        peer = {"z": lax.rem(z + dz, 4), "x": lax.rem(x + dx, 2), "y": lax.rem(y + dy, 2), "c": lax.rem(c + dc, 2)}
                        pl.semaphore_signal(barrier, inc=1, device_id=peer, device_id_type=MESH)
    pl.semaphore_wait(barrier, 31)

    load_wo = pltpu.make_async_copy(wo_hbm, wo, wo_sem)
    load_wo.start()

    def carry_copy(k):
        return remote(pair_ref, held.at[k], c_send.at[k], c_recv.at[k], z=lax.rem(z + k, 4))

    leftward = jnp.logical_or(z == 3, jnp.logical_and(c == 0, z >= 1))
    rightward = jnp.logical_not(leftward)
    is_near = z == near
    is_far = jnp.logical_not(is_near)
    is_last = z == 3
    not_mine = jnp.logical_not(mine)
    for m in range(2):
        each(line_sends(m), start)
        begin(m)

    @pl.when(jnp.logical_and(leftward, not_mine))
    def _():
        each(line_sends(2), start)
        each(line_sends(3), start)
    tokens = q_ref.shape[0]
    for load in loads:
        load.wait()
    spread_r = lax.broadcasted_iota(jnp.int32, (heads, width), 0)
    spread_c = lax.broadcasted_iota(jnp.int32, (heads, width), 1) // HEAD
    spread = jnp.where(spread_r == spread_c, 1.0, 0.0).astype(F32)
    extra_wide[...] = lax.dot_general(
        extra_ref[...], spread, (TN, ((), ())), precision=lax.Precision.HIGHEST, preferred_element_type=F32)

    big_r = lax.broadcasted_iota(jnp.int32, (width, width), 0)
    big_c = lax.broadcasted_iota(jnp.int32, (width, width), 1)
    blocks = jnp.where((big_r // HEAD) == (big_c // HEAD), 1.0, 0.0).astype(BF16)
    zm_ref[...] = jnp.where(big_r == big_c, 1.0, 0.0).astype(F32)
    ze_ref[...] = jnp.zeros_like(ze_ref)

    def advance(i, _):
        span = at(i, chunk)
        wide_step(
            heads, q_ref.at[span, :], k_ref.at[span, :], v_ref.at[span, :], din_ref.at[span, :], doff_ref,
            extra_wide.at[span, :], rin_ref.at[span, :], roff_ref, read_ref.at[span, :], own_ref.at[span, :], zm_ref, ze_ref)

        @pl.when(jnp.logical_and(i == 2, is_far))
        def _():
            pump(0, 0)

        @pl.when(jnp.logical_and(i == 3, is_near))
        def _():
            pump(0, 0)
            pump_far(0)

        @pl.when(jnp.logical_and(i == 3, jnp.logical_and(is_last, mine)))
        def _():
            each(line_sends(2), start)
            each(line_sends(3), start)

        return 0

    lax.fori_loop(0, tokens // chunk, advance, 0)

    for h in range(heads):
        span = slice(h * HEAD, (h + 1) * HEAD)
        total_ref[span, :] = jnp.concatenate([zm_ref[span, span], ze_ref[span, span]], axis=1).astype(BF16)
    swap = remote(total_ref, other_ref, c_send.at[0], c_recv.at[0], x=1 - x)
    swap.start()

    @pl.when(is_near)
    def _():
        pump_side(0)

    @pl.when(is_far)
    def _():
        pump(1, 0)
        begin(2)
    swap.wait_recv()

    def tall(block):
        return jnp.concatenate([block[:, :HEAD]] * heads, axis=1) * blocks

    ours, theirs = total_ref[...].astype(F32), other_ref[...].astype(F32)
    older, newer = jnp.where(x == 0, ours, theirs).astype(BF16), jnp.where(x == 0, theirs, ours).astype(BF16)
    joint = jnp.dot(tall(newer), older, preferred_element_type=F32)
    pair_ref[...] = (joint + jnp.where(
        lax.broadcasted_iota(jnp.int32, joint.shape, 1) >= HEAD, newer.astype(F32), 0.0)).astype(BF16)
    for k in range(1, 4):
        @pl.when(z + k < 4)
        def _():
            carry_copy(k).start()

    @pl.when(jnp.logical_and(rightward, not_mine))
    def _():
        each(line_sends(2), start)
        each(line_sends(3), start)

    @pl.when(jnp.logical_and(rightward, jnp.logical_and(mine, is_far)))
    def _():
        each(line_sends(2), start)
        each(line_sends(3), start)

    @pl.when(is_near)
    def _():
        pump(1, 0)
        pump(1, 1)

    @pl.when(jnp.logical_and(mine, is_near))
    def _():
        each(line_sends(2), start)
        each(line_sends(3), start)

    @pl.when(is_last)
    def _():
        pump(0, 1)
        begin(3)
    for k in range(1, 4):
        @pl.when(z >= k)
        def _():
            carry_copy(k).wait_recv()
    state = jnp.zeros((width, HEAD), F32)
    for there, block in [(z >= k, held[k]) for k in (3, 2, 1)] + [(x == 1, older)]:
        move = tall(block)
        high, rest = split2(state)
        moved = jnp.dot(move, high, preferred_element_type=F32) + jnp.dot(move, rest, preferred_element_type=F32)
        state = jnp.where(there, block[:, HEAD:].astype(F32) + moved, state)

    def head_mean(a):
        high, low_part = split2(a)
        return (jnp.dot(high, blocks, preferred_element_type=F32) + jnp.dot(low_part, blocks, preferred_element_type=F32)) / HEAD

    carried = tuple(tall(a) for a in split2(state))
    o = own_ref[...] + dot3(split2(read_ref[...]), carried, NN)
    center = o - head_mean(o)
    mixed[...] = (center * lax.rsqrt(head_mean(center * center) + 1e-5) * gain_ref[...]).astype(BF16)

    t = 2 * y + c

    def exchange(dy, dc):
        ty, tc = lax.rem(y + dy, 2), lax.rem(c + dc, 2)
        slot = 2 * dy + dc
        return remote(
            mixed.at[at(2 * ty + tc, rows), :], mixrow.at[:, at(t, width)], a_send.at[slot], a_recv.at[slot], y=ty, c=tc)

    swaps = [exchange(1, 0), exchange(1, 1), exchange(0, 1)]
    for copy in swaps:
        copy.start()
    mixrow[:, at(t, width)] = mixed[at(t, rows), :]


    @pl.when(z == 0)
    def _():
        pump(0, 1)
    load_wo.wait()
    for copy in swaps:
        copy.wait()

    tile = 512
    square = jnp.zeros((rows, 1), F32)
    for j in range(0, model, tile):
        proj = jnp.dot(mixrow[...], wo[:, j:j + tile], preferred_element_type=F32)
        part = (resid_ref[:, j:j + tile].astype(F32) + proj).astype(BF16).astype(F32)
        mid[:, j:j + tile] = part
        square += jnp.sum(part * part, axis=-1, keepdims=True)
    g = 2 * half + y
    g_far = 2 * (1 - half) + y
    g_side = 2 * half + 1 - y
    g_diag = 2 * (1 - half) + 1 - y
    tok[at(g, rows), :] = (mid[...] * lax.rsqrt(square / model + 1e-06) * fgain_ref[...]).astype(BF16)

    def rows_to(block, slot, **where):
        r = tok.at[at(block, rows), :]
        return remote(r, r, t_send.at[slot], t_recv.at[slot], **where)

    def rows_from(block, slot):
        r = tok.at[at(block, rows), :]
        remote(r, r, t_send.at[slot], t_recv.at[slot], y=1 - y).wait_recv()

    ahead = rows_to(g, 0, z=pair)
    beside = rows_to(g, 1, y=1 - y)
    onward = rows_to(g_far, 2, y=1 - y)
    beside.start()

    @pl.when(is_far)
    def _():
        ahead.start()

    @pl.when(is_far)
    def _():
        pump(1, 1)

    @pl.when(z == 0)
    def _():
        begin(3)
    pump(0, 2)
    pump(0, 3)

    @pl.when(is_near)
    def _():
        ahead.start()

    @pl.when(z == 1)
    def _():
        pump_far(2)
        pump_far(3)
    rows_from(g_far, 0)
    onward.start()
    pump(1, 2)

    @pl.when(is_near)
    def _():
        begin(2)
        begin(3)

    @pl.when(z == 1)
    def _():
        pump_side(2)
        pump_side(3)

    @pl.when(z == 2)
    def _():
        pump(2, 1)
        pump(3, 1)

    @pl.when(is_near)
    def _():
        pump(2, 0)
        pump(3, 0)

    pump(1, 3)

    @pl.when(is_far)
    def _():
        pump(2, 0)

    @pl.when(is_last)
    def _():
        pump(3, 0)

    rest_of(0)
    rest_of(1)
    rows_from(g_side, 1)
    rows_from(g_diag, 2)

    units = gate.shape[1]
    for j in range(0, units, 256):
        cols = slice(j, min(j + 256, units))
        gated = jnp.dot(tok[...], gate[:, cols], preferred_element_type=F32)
        upper = jnp.dot(tok[...], up[:, cols], preferred_element_type=F32)
        hidden[:, cols] = (gated * jax.nn.sigmoid(gated) * upper).astype(BF16)

    def side_copy(i, b):
        return remote(y_out.at[i, b], y_in.at[i, b], y_send.at[i, b], y_recv.at[i, b], y=1 - y)

    def far_copy(i):
        return remote(z_out.at[i], z_in.at[i], z_send.at[i], z_recv.at[i], z=pair)

    def slices_of(column, plane, other):
        for b, block_half, sums in ((0, 1 - half, far_sum), (1, half, near_sum)):
            for k, source in enumerate((plane, other)):
                i = 2 * source + column
                if b == 0 and k == 1:
                    down_landed(i)
                sums[:, at(i, depth)] = jnp.dot(
                    hidden[at(block_half, 2 * rows), :], down[:, at(i, depth)], preferred_element_type=F32)
                y_out[i, b] = sums[at(1 - y, rows), at(i, depth)].astype(BF16)
                side_copy(i, b).start()

    def pass_on(plane, column):
        i = 2 * plane + column
        side_copy(i, 0).wait_recv()
        z_out[i] = (far_sum[at(y, rows), at(i, depth)] + y_in[i, 0].astype(F32)).astype(BF16)
        far_copy(i).start()

    next_first, next_other = jnp.where(is_last, first, second), jnp.where(is_last, other_first, other_second)
    next_column = jnp.where(is_last, 1 - x, x)
    then_first, then_other = jnp.where(is_last, second, early), jnp.where(is_last, other_second, other_early)
    then_column = jnp.where(is_last, x, 1 - x)

    @pl.when(z == 0)
    def _():
        pump(3, 0)

    @pl.when(is_far)
    def _():
        pump(2, 1)
    slices_of(x, first, other_first)

    @pl.when(z == 0)
    def _():
        pump(3, 1)

    @pl.when(is_last)
    def _():
        pump(2, 2)
        pump(3, 2)
    slices_of(next_column, next_first, next_other)
    pass_on(first, x)
    pass_on(other_first, x)

    @pl.when(is_last)
    def _():
        pump(3, 1)
    drain(0)
    drain(1)
    swap.wait_send()
    for k in range(1, 4):
        @pl.when(z + k < 4)
        def _():
            carry_copy(k).wait_send()

    @pl.when(jnp.logical_not(is_last))
    def _():
        pump(2, 2)
        pump(3, 2)
    slices_of(then_column, then_first, then_other)
    pass_on(next_first, next_column)
    pass_on(next_other, next_column)
    pass_on(then_first, then_column)
    pass_on(then_other, then_column)
    pump(2, 3)
    pump(3, 3)
    slices_of(1 - x, late, other_late)
    pass_on(late, 1 - x)
    pass_on(other_late, 1 - x)
    for i in range(n):
        cols = slice(i * depth, (i + 1) * depth)
        side_copy(i, 1).wait_recv()
        far_copy(i).wait_recv()
        total = near_sum[at(y, rows), cols] + y_in[i, 1].astype(F32) + z_in[i].astype(F32)
        out_ref[:, cols] = (mid[:, cols] + 0.5 * total).astype(BF16)

    drain(2)
    drain(3)
    for copy in (ahead, beside, onward):
        copy.wait_send()
    for i in range(n):
        side_copy(i, 0).wait_send()
        side_copy(i, 1).wait_send()
        far_copy(i).wait_send()


def layer(q, k, v, din, doff, extra, rin, roff, gain, resid, fgain, wo, gate, up, down):
    tokens, width = q.shape
    heads = width // HEAD
    chunk = 64
    while tokens % chunk:
        chunk //= 2
    rows, model = resid.shape
    depth, units = gate.shape
    n = 8
    vm = pl.BlockSpec(memory_space=pltpu.VMEM)
    hbm = pl.BlockSpec(memory_space=pl.ANY)
    dma = pltpu.SemaphoreType.DMA
    inputs = (
        q, k, v, din, doff.reshape(1, width), extra.T, rin, roff.reshape(1, width), gain.reshape(1, width), resid, fgain.reshape(1, model))
    return pl.pallas_call(
        functools.partial(layer_kernel, chunk),
        in_specs=[hbm] * 15,
        out_specs=vm,
        out_shape=pltpu.VMEM((rows, model), BF16),
        scratch_shapes=[pltpu.VMEM(a.shape, a.dtype) for a in inputs] + [
            pltpu.VMEM((tokens, width), F32),
            pltpu.VMEM((width, 2 * HEAD), BF16),
            pltpu.VMEM((width, 2 * HEAD), BF16),
            pltpu.VMEM((width, 2 * HEAD), BF16),
            pltpu.VMEM((tokens, width), F32),
            pltpu.VMEM((tokens, width), F32),
            pltpu.VMEM((width, width), F32),
            pltpu.VMEM((width, width), F32),
            pltpu.VMEM((4, width, 2 * HEAD), BF16),
            pltpu.VMEM((tokens, width), BF16),
            pltpu.VMEM((rows, wo.shape[0]), BF16),
            pltpu.VMEM(wo.shape, BF16),
            pltpu.VMEM((rows, model), F32),
            pltpu.VMEM((4 * rows, model), BF16),
            pltpu.VMEM((n * depth, units), BF16),
            pltpu.VMEM((n * depth, units), BF16),
            pltpu.VMEM((units, n * depth), BF16),
            pltpu.VMEM((4 * rows, units), BF16),
            pltpu.VMEM((2 * rows, model), F32),
            pltpu.VMEM((2 * rows, model), F32),
            pltpu.VMEM((n, 2, rows, depth), BF16),
            pltpu.VMEM((n, 2, rows, depth), BF16),
            pltpu.VMEM((n, rows, depth), BF16),
            pltpu.VMEM((n, rows, depth), BF16),
            dma((11,)), dma, dma((4, 11)), dma((4, n)), dma((4,)), dma((4,)), dma((4,)), dma((4,)), dma((3,)), dma((3,)),
            dma((n, 2)), dma((n, 2)), dma((n,)), dma((n,)),
        ],
        compiler_params=pltpu.CompilerParams(collective_id=2, has_side_effects=True, vmem_limit_bytes=67043328 - 2 * rows * model),
    )(*inputs, wo, gate, up, down)


def per_device_pairs(
    resid, queries, keys, values, decay_input_part, decay_channel_offset, decay_head_extra,
    correction_rate_input, correction_rate_offset, head_norm_gain, mixer_output_weight,
    feedforward_norm_gain, gate_weight, up_weight, down_weight,
):
    return layer(
        queries, keys, values, decay_input_part, decay_channel_offset, decay_head_extra,
        correction_rate_input, correction_rate_offset, head_norm_gain, resid, feedforward_norm_gain, mixer_output_weight, gate_weight, up_weight, down_weight)


def solution(mesh):
    n_sp, n_tp = mesh.shape["sp"], mesh.shape["tp"]
    if (n_sp, n_tp) == (8, 4):
        inner = Mesh(mesh.devices.reshape(4, 2, 2, 2), ("z", "x", "y", "c"))
        sp, tp = ("z", "x"), ("y", "c")
        body = per_device_pairs
    else:
        nx = 2 if n_sp % 2 == 0 else 1
        nz = n_sp // nx
        inner = Mesh(mesh.devices.reshape(nz, nx, n_tp), ("z", "x", "tp"))
        sp, tp = ("z", "x"), ("tp",)
        body = functools.partial(per_device, nz, nx)
    rows = P((*sp, *tp), None)
    placed = (
        rows, P(sp, tp), P(sp, tp), P(sp, tp), P(sp, tp), P(tp), P(sp, tp), P(sp, tp), P(tp), P(tp), P(), P(),
        P(sp, tp), P(sp, tp), P(tp, sp),
    )
    return jax.shard_map(body, mesh=inner, in_specs=placed, out_specs=rows, check_vma=False)
```
